32 devices in a mesh: ep: 8 (over z, x), tp: 4 (over y, core).
Axes of the slice: x: 2, y: 2, z: 4, core: 2. Of those that a mesh axis runs over, the one named last changes fastest.
Arguments:
- tokens: bfloat16 [128, 1024], P('ep'), may hold values from -6 to 6
- memory: float32 [128, 4, 128, 256], P('ep', 'tp'), may hold values from -6 to 6
- log_scale: float32 [128, 4], P('ep', 'tp'), may hold values from -1 to 130
- mix_gain_in: float32 [1024], replicated, may hold values from 0.1 to 1.9
- w_query: bfloat16 [1024, 512], P(None, 'tp'), may hold values from -0.1875 to 0.1875
- w_key: bfloat16 [1024, 512], P(None, 'tp'), may hold values from -0.1875 to 0.1875
- w_value: bfloat16 [1024, 1024], P(None, 'tp'), may hold values from -0.1875 to 0.1875
- w_igate: bfloat16 [1024, 4], P(None, 'tp'), may hold values from -0.1875 to 0.1875
- w_fgate: bfloat16 [1024, 4], P(None, 'tp'), may hold values from -0.1875 to 0.1875
- igate_bias: float32 [4], P('tp'), may hold values from -1 to 1
- fgate_bias: float32 [4], P('tp'), may hold values from 0 to 4
- head_gain: float32 [1024], P('tp'), may hold values from 0.1 to 1.9
- w_output: bfloat16 [1024, 1024], P('tp'), may hold values from -0.1875 to 0.1875
- mix_gain_out: float32 [1024], replicated, may hold values from 0.1 to 1.9
- ffn_gain_in: float32 [1024], replicated, may hold values from 0.1 to 1.9
- routes: int32 [128, 6], P('ep'), may hold values from 0 to 7, all different within a row; in each aligned block of 16 rows (0 to 15, 16 to 31, ...) at most 16 rows name the same one
- route_weights: float32 [128, 6], P('ep'), may hold values from 0.1 to 1
- expert_gate: bfloat16 [8, 1024, 1024], P('ep', None, 'tp'), may hold values from -0.1875 to 0.1875
- expert_up: bfloat16 [8, 1024, 1024], P('ep', None, 'tp'), may hold values from -0.1875 to 0.1875
- expert_down: bfloat16 [8, 1024, 1024], P('ep', 'tp'), may hold values from -0.9375 to 0.9375
- ffn_gain_out: float32 [1024], P('tp'), may hold values from 0.1 to 1.9
Outputs:
- output: bfloat16 [128, 1024], P('ep', 'tp')
The draws below stay inside these ranges and needn't reach their ends.
Inputs may be any that keep to these rules, and one draw needn't show every extreme that they name: `routes`: among the 16 tokens of one index of ep no expert is named by more than 16 tokens, and in every draw some expert is named by exactly 16 of them.
All inputs are finite; a program needn't handle non-finite values.
Results may differ from the reference program's by a relative error of at most 0.02.
Values may be sent and summed in bfloat16 or wider, within the bound.
No kernel may reach another device: no remote copies, remote signals or barrier semaphores. Data moves between devices by JAX's collectives and lax.ppermute only.
A program may use at most 64 MiB of HBM per device.

```python
import math
import jax
import jax.numpy as jnp
import numpy as np
from jax import lax

D = 1024
HEADS = 4
KEY_DIM = 128
VALUE_DIM = 256
EXPERT_WIDTH = 1024
TOP_K = 6
SEQ_G = 16
EXPERTS = 8
CAP = 16
BATCH = 128
N_EP = 8


def draw_log_scale(key, part):
    base_key = jax.random.fold_in(key, 11)
    values = jax.random.uniform(base_key, (BATCH, HEADS), jnp.float32, -1.0, 3.0)
    return values


def draw_expert_down(key, part):
    noise_key = jax.random.fold_in(key, 21)
    column_key = jax.random.fold_in(key, 22)
    raw = jnp.clip(jax.random.normal(noise_key, (EXPERTS, EXPERT_WIDTH, D), jnp.float32), -4.0, 4.0)
    spot = (jnp.arange(D, dtype=jnp.float32) + 0.5) / D
    jitter = jax.random.uniform(column_key, (D,), jnp.float32, -0.4, 0.4)
    ramp = 1.2 * (2.0 * spot - 1.0)
    scale = jnp.exp(ramp + jitter) * EXPERT_WIDTH ** (-0.5)
    return (raw * scale[None, None, :]).astype(jnp.bfloat16)


def block_scale(stream_key, dims, pieces, smallest, largest):
    loudness, own = 1.0, jax.random.fold_in(stream_key, 6)
    for dim, parts in pieces:
        heights = jnp.exp(jax.random.uniform(jax.random.fold_in(own, dim), (parts,), jnp.float32, smallest / len(pieces), largest / len(pieces)))
        loudness = loudness * jnp.repeat(heights, dims[dim] // parts).reshape([-1 if axis == dim else 1 for axis in range(len(dims))])
    return loudness


def assign_block(rng, own, number, rows, number_of, top, reach, lean):
    ranking = jax.random.permutation(rng, number_of)
    crowded, usual = portions_of(number_of, rows * top, reach, lean, True), portions_of(number_of, rows * top, reach, lean, False)
    places = jnp.arange(number_of)

    def named(sizes, turn):
        used = int((sizes > 0).sum())
        fixed = max(1, used // 4)
        moved = fixed + (places - fixed + turn * (used - fixed)) % max(1, number_of - fixed)
        return jnp.zeros((number_of,), jnp.int32).at[ranking[jnp.where(places < fixed, places, moved)]].set(jnp.asarray(sizes, jnp.int32))

    sizes = jnp.where(number % 4 == 0, named(crowded, number // 4), named(usual, number - number // 4 - 1))
    mixed = jax.random.permutation(jax.random.fold_in(own, 3), number_of)
    giver, taker = mixed[0:number_of // 2 * 2:2], mixed[1:number_of // 2 * 2:2]
    slack = jnp.minimum(sizes[giver] - 1, reach - sizes[taker]) // 2
    slack = jnp.where((giver == ranking[0]) | (taker == ranking[0]) | (sizes[taker] == 0), 0, jnp.maximum(slack, 0))
    moved = jax.random.randint(jax.random.fold_in(own, 4), (number_of // 2,), 0, 1 << 20) % (slack + 1)
    sizes = sizes.at[giver].add(-moved).at[taker].add(moved)
    members = jnp.searchsorted(jnp.cumsum(sizes), jnp.arange(rows * top), side="right").astype(jnp.int32)
    listing = members.reshape(top, rows).T
    listing = listing[jax.random.permutation(jax.random.fold_in(own, 1), rows)]
    turn = jax.random.randint(jax.random.fold_in(own, 2), (rows, 1), 0, top)
    return jnp.take_along_axis(listing, (jnp.arange(top)[None, :] + turn) % top, axis=1)


def portions_of(number_of, total, reach, lean, full):
    portions = [(1 << 20) // math.isqrt(rank ** lean) + 1 for rank in range(1, number_of + 1)]
    largest = reach if full else min(reach, max(-(-total // number_of), total * portions[0] // sum(portions)))
    least = 1 if total - largest >= number_of - 1 else 0
    counts, rest = [largest] + [least] * (number_of - 1), total - largest - least * (number_of - 1)
    while rest > 0:
        candidates = [i for i in range(1, number_of) if counts[i] < largest] or [i for i in range(1, number_of) if counts[i] < reach]
        pool, remaining = sum([portions[i] for i in candidates]), rest
        for i in candidates:
            addition = min(reach - counts[i], max(1, remaining * portions[i] // pool), rest)
            counts[i] = counts[i] + addition
            rest = rest - addition
    return np.array(counts)


def noise(key, shape, scale, bound, split=(), held_as=jnp.bfloat16):
    values = jax.random.normal(key, shape, jnp.float32) * scale
    if len(split) > 0:
        values = block_scale(key, shape, split, -0.22, 0.18) * values
    return jnp.clip(values, min=-bound, max=bound).astype(held_as)


def setup_inputs(seed: int = 0) -> dict:
    splits = jax.random.split(jax.random.key(seed), 22)
    tokens = noise(splits[0], (BATCH, D), 1.0, 6.0, ((0, 8),))
    memory = noise(splits[1], (BATCH, HEADS, KEY_DIM, VALUE_DIM), 1.0, 6.0, ((0, 8), (1, 4)), jnp.float32)
    log_scale = draw_log_scale(jax.random.fold_in(splits[21], 71), 0)
    mix_gain_in = jnp.clip(1.0 + 0.18 * jax.random.normal(splits[3], (D,), jnp.float32), 0.1, 1.9)
    w_query = noise(splits[4], (D, HEADS * KEY_DIM), D ** -0.5, 0.1875, ((1, 4),))
    w_key = noise(splits[5], (D, HEADS * KEY_DIM), D ** -0.5, 0.1875, ((1, 4),))
    w_value = noise(splits[6], (D, HEADS * VALUE_DIM), D ** -0.5, 0.1875, ((1, 4),))
    w_igate = noise(splits[7], (D, HEADS), D ** -0.5, 0.1875, ((1, 4),))
    w_fgate = noise(splits[8], (D, HEADS), D ** -0.5, 0.1875, ((1, 4),))
    igate_bias = jnp.clip(jax.random.uniform(splits[9], (HEADS,), jnp.float32, -1.0, 1.0) * block_scale(splits[9], (HEADS,), ((0, 4),), -0.4, 0.0), -1.0, 1.0)
    fgate_bias = jnp.clip(4.0 * jax.random.uniform(splits[10], (HEADS,), jnp.float32) ** block_scale(splits[10], (HEADS,), ((0, 4),), -0.2, 0.2), 0.0, 4.0)
    head_gain = jnp.clip(1.0 + 0.18 * jax.random.normal(splits[11], (HEADS * VALUE_DIM,), jnp.float32), 0.1, 1.9)
    w_output = noise(splits[12], (HEADS * VALUE_DIM, D), (HEADS * VALUE_DIM) ** -0.5, 0.1875, ((0, 4),))
    mix_gain_out = jnp.clip(1.0 + 0.18 * jax.random.normal(splits[13], (D,), jnp.float32), 0.1, 1.9)
    ffn_gain_in = jnp.clip(1.0 + 0.18 * jax.random.normal(splits[14], (D,), jnp.float32), 0.1, 1.9)
    routes_keys = jax.random.split(jax.random.fold_in(splits[15], 1), BATCH // SEQ_G)
    routes_turns = jax.random.permutation(jax.random.fold_in(splits[15], 3), BATCH // SEQ_G)
    routes = jax.vmap(lambda own, number: assign_block(jax.random.fold_in(splits[15], 2), own, number, SEQ_G, EXPERTS, TOP_K, CAP, 1))(routes_keys, routes_turns).reshape((BATCH, TOP_K))
    route_weights = jnp.clip(jnp.exp(math.log(1.0) - 2.3025851 * jax.random.uniform(splits[16], (BATCH, TOP_K), jnp.float32) ** block_scale(splits[16], (BATCH, TOP_K), ((0, 8),), -0.2, 0.2)), 0.1, 1.0)
    expert_gate = noise(splits[17], (EXPERTS, D, EXPERT_WIDTH), D ** -0.5, 0.1875, ((0, 8), (2, 4)))
    expert_up = noise(splits[18], (EXPERTS, D, EXPERT_WIDTH), D ** -0.5, 0.1875, ((0, 8), (2, 4)))
    expert_down = draw_expert_down(jax.random.fold_in(splits[21], 71), 0)
    ffn_gain_out = jnp.clip(1.0 + 0.18 * jax.random.normal(splits[20], (D,), jnp.float32), 0.1, 1.9)
    return dict(tokens=tokens, memory=memory, log_scale=log_scale, mix_gain_in=mix_gain_in, w_query=w_query, w_key=w_key, w_value=w_value, w_igate=w_igate, w_fgate=w_fgate, igate_bias=igate_bias, fgate_bias=fgate_bias, head_gain=head_gain, w_output=w_output, mix_gain_out=mix_gain_out, ffn_gain_in=ffn_gain_in, routes=routes, route_weights=route_weights, expert_gate=expert_gate, expert_up=expert_up, expert_down=expert_down, ffn_gain_out=ffn_gain_out)


EPS = 1e-06

def rms_scale(values):
    return lax.rsqrt(lax.optimization_barrier(jnp.mean(values * values, axis=-1, keepdims=True)) + EPS)

def reference(tokens, memory, log_scale, mix_gain_in, w_query, w_key, w_value, w_igate, w_fgate, igate_bias, fgate_bias, head_gain, w_output, mix_gain_out, ffn_gain_in, routes, route_weights, expert_gate, expert_up, expert_down, ffn_gain_out):
    f32 = jnp.float32
    bf16 = jnp.bfloat16
    xf = tokens.astype(f32)
    normed = (xf * rms_scale(xf) * mix_gain_in).astype(bf16)
    query = jnp.dot(normed, w_query, preferred_element_type=f32).reshape(BATCH, HEADS, KEY_DIM) * KEY_DIM ** (-0.5)
    keys = jnp.dot(normed, w_key, preferred_element_type=f32).reshape(BATCH, HEADS, KEY_DIM)
    values = jnp.dot(normed, w_value, preferred_element_type=f32).reshape(BATCH, HEADS, VALUE_DIM)
    in_pre = jnp.dot(normed, w_igate, preferred_element_type=f32) + igate_bias
    forget_log = jax.nn.log_sigmoid(jnp.dot(normed, w_fgate, preferred_element_type=f32) + fgate_bias)
    carried = forget_log + log_scale
    new_max = jnp.maximum(carried, in_pre)
    carry_weight = jnp.exp(carried - new_max)
    fresh_weight = jnp.exp(in_pre - new_max)
    recall = jnp.einsum('bhk,bhkv->bhv', query, memory, precision=lax.Precision.HIGHEST)
    match = lax.optimization_barrier(jnp.sum(query * keys, axis=-1))
    read = carry_weight[..., None] * recall + (fresh_weight * match)[..., None] * values
    headout = (read * rms_scale(read) * head_gain.reshape(HEADS, VALUE_DIM)).astype(bf16)
    per_head = jnp.einsum('bhv,hvd->bhd', headout.astype(f32), w_output.reshape(HEADS, VALUE_DIM, D).astype(f32)).astype(bf16)
    mixed = lax.optimization_barrier(jnp.sum(per_head.astype(f32), axis=1))
    resid = (xf + mixed * rms_scale(mixed) * mix_gain_out).astype(bf16)
    rf = resid.astype(f32)
    ffn_in = (rf * rms_scale(rf) * ffn_gain_in).astype(bf16)
    rows_total = BATCH * TOP_K
    limit = N_EP * CAP
    flat = routes.reshape(-1).astype(jnp.int32)

    def per_expert(done, expert):
        found = jnp.nonzero(flat == expert, size=limit, fill_value=rows_total)[0].astype(jnp.int32)
        token = jnp.minimum(found // TOP_K, BATCH - 1)
        picked = jnp.take(ffn_in, token, axis=0)
        gate = jnp.dot(picked, expert_gate[expert], preferred_element_type=f32)
        up = jnp.dot(picked, expert_up[expert], preferred_element_type=f32)
        act = (jax.nn.silu(gate) * up).astype(bf16)
        blocks = jnp.einsum('rtf,tfd->rtd', act.reshape(limit, HEADS, EXPERT_WIDTH // HEADS).astype(f32), expert_down[expert].reshape(HEADS, EXPERT_WIDTH // HEADS, D).astype(f32)).astype(bf16)
        result = lax.optimization_barrier(jnp.sum(blocks.astype(f32), axis=1)).astype(bf16)
        done = done.at[found].set(result, mode='drop')
        return (done, None)
    done, _ = lax.scan(per_expert, jnp.zeros((rows_total, D), bf16), jnp.arange(EXPERTS, dtype=jnp.int32))
    expert_rows = done.reshape(BATCH, TOP_K, D).astype(f32)
    routed = lax.optimization_barrier(jnp.sum(route_weights[..., None] * expert_rows, axis=1))
    return (rf + routed * rms_scale(routed) * ffn_gain_out).astype(bf16)
```

```python
import jax
import jax.numpy as jnp
from jax import lax
from jax.sharding import PartitionSpec as P

EPS = 1e-06


def rms_scale(values):
    return lax.rsqrt(jnp.mean(values * values, axis=-1, keepdims=True) + EPS)


def per_device(
    tokens,
    memory,
    log_scale,
    mix_gain_in,
    w_query,
    w_key,
    w_value,
    w_igate,
    w_fgate,
    igate_bias,
    fgate_bias,
    head_gain,
    w_output,
    mix_gain_out,
    ffn_gain_in,
    routes,
    route_weights,
    expert_gate,
    expert_up,
    expert_down,
    ffn_gain_out,
):
    f32 = jnp.float32
    bf16 = jnp.bfloat16
    seqs, width = tokens.shape
    heads = log_scale.shape[1]
    key_dim = memory.shape[2]
    value_dim = memory.shape[3]
    xf = tokens.astype(f32)
    normed = (xf * rms_scale(xf) * mix_gain_in).astype(bf16)
    query = jnp.dot(normed, w_query, preferred_element_type=f32).reshape(
        seqs, heads, key_dim
    ) * key_dim ** (-0.5)
    keys = jnp.dot(normed, w_key, preferred_element_type=f32).reshape(seqs, heads, key_dim)
    values = jnp.dot(normed, w_value, preferred_element_type=f32).reshape(seqs, heads, value_dim)
    in_pre = jnp.dot(normed, w_igate, preferred_element_type=f32) + igate_bias
    forget_log = jax.nn.log_sigmoid(
        jnp.dot(normed, w_fgate, preferred_element_type=f32) + fgate_bias
    )
    carried = forget_log + log_scale
    new_max = jnp.maximum(carried, in_pre)
    carry_weight = jnp.exp(carried - new_max)
    fresh_weight = jnp.exp(in_pre - new_max)
    recall = jnp.einsum("shk,shkv->shv", query, memory, precision=lax.Precision.HIGHEST)
    match = jnp.sum(query * keys, axis=-1)
    read = carry_weight[..., None] * recall + (fresh_weight * match)[..., None] * values
    headout = (
        (read * rms_scale(read) * head_gain.reshape(heads, value_dim))
        .astype(bf16)
        .reshape(seqs, heads * value_dim)
    )
    partial_value = jnp.dot(headout, w_output, preferred_element_type=f32)
    mixed = sum_over(partial_value.astype(bf16), "tp")
    resid = (xf + mixed * rms_scale(mixed) * mix_gain_out).astype(bf16)
    rf = resid.astype(f32)
    ffn_in = (rf * rms_scale(rf) * ffn_gain_in).astype(bf16)
    lanes = lax.axis_size("tp")
    groups = lax.axis_size("ep")
    quarter = width // lanes
    own = lax.axis_index("tp") * quarter
    local_experts = expert_gate.shape[0]
    experts_all = local_experts * groups
    top = routes.shape[1]
    cap = min(seqs, max(2, 3 * seqs * top // (2 * experts_all)))
    if cap == seqs and local_experts == 1:
        routed = every_token(ffn_in, routes, route_weights, expert_gate, expert_up, expert_down)
    else:
        routed = slotted(ffn_in, routes, route_weights, expert_gate, expert_up, expert_down, cap)
    resid_part = lax.dynamic_slice_in_dim(rf, own, quarter, 1)
    total = sum_over(jnp.sum(routed * routed, axis=1), "tp")
    scaled = routed * lax.rsqrt(total / width + EPS)[:, None]
    return (resid_part + scaled * ffn_gain_out).astype(bf16)


def sum_over(value, axis):
    size = lax.axis_size(axis)
    total = value.astype(jnp.float32)
    for step in range(1, size):
        if size & (size - 1) == 0:
            pairs = [(i, i ^ step) for i in range(size)]
        else:
            pairs = [(i, (i + step) % size) for i in range(size)]
        total = total + lax.ppermute(value, axis, pairs).astype(jnp.float32)
    return total


def every_token(ffn_in, routes, route_weights, expert_gate, expert_up, expert_down):
    f32 = jnp.float32
    bf16 = jnp.bfloat16
    seqs, width = ffn_in.shape
    lanes = lax.axis_size("tp")
    groups = lax.axis_size("ep")
    quarter = width // lanes
    spread = jnp.broadcast_to(ffn_in[None], (groups, seqs, width))
    rows = lax.all_to_all(spread, "ep", split_axis=0, concat_axis=0, tiled=True)
    rows = rows.reshape(groups * seqs, width)
    gate = jnp.dot(rows, expert_gate[0], preferred_element_type=f32)
    up = jnp.dot(rows, expert_up[0], preferred_element_type=f32)
    act = (jax.nn.silu(gate) * up).astype(bf16)
    part = jnp.dot(act, expert_down[0], preferred_element_type=f32).astype(bf16)
    blocks = part.reshape(groups, seqs, lanes, quarter).transpose(0, 2, 1, 3)
    blocks = blocks.reshape(groups * lanes, seqs, quarter)
    back = lax.all_to_all(blocks, ("ep", "tp"), split_axis=0, concat_axis=0, tiled=True)
    back = back.reshape(groups, lanes, seqs, quarter).astype(f32)
    done = jnp.sum(back, axis=1).astype(bf16).astype(f32)
    named = routes[:, :, None] == jnp.arange(groups, dtype=jnp.int32)[None, None, :]
    weights = jnp.sum(jnp.where(named, route_weights[:, :, None], 0.0), axis=1)
    return jnp.sum(weights.T[:, :, None] * done, axis=0)


def slotted(ffn_in, routes, route_weights, expert_gate, expert_up, expert_down, cap):
    f32 = jnp.float32
    bf16 = jnp.bfloat16
    seqs, width = ffn_in.shape
    top = routes.shape[1]
    local_experts = expert_gate.shape[0]
    experts_all = local_experts * lax.axis_size("ep")
    flat = routes.reshape(-1)
    hits = (flat[:, None] == jnp.arange(experts_all, dtype=jnp.int32)[None, :]).astype(jnp.int32)
    earlier = jnp.cumsum(hits, axis=0) - hits
    slot = jnp.sum(earlier * hits, axis=1)
    place = (flat * cap + slot).reshape(seqs, top)
    picker = jnp.any(
        jnp.arange(experts_all * cap, dtype=jnp.int32)[:, None, None] == place[None, :, :], axis=2
    ).astype(bf16)
    outbound = (
        jnp.dot(picker, ffn_in, preferred_element_type=f32)
        .astype(bf16)
        .reshape(experts_all, cap, width)
    )
    arrived = lax.all_to_all(outbound, "ep", split_axis=0, concat_axis=0, tiled=True)
    items = arrived.shape[1]
    rows = arrived.reshape(-1, local_experts, items, width)
    gate = jnp.einsum("secd,edf->secf", rows, expert_gate, preferred_element_type=f32)
    up = jnp.einsum("secd,edf->secf", rows, expert_up, preferred_element_type=f32)
    act = (jax.nn.silu(gate) * up).astype(bf16)
    part = jnp.einsum("secf,efd->secd", act, expert_down, preferred_element_type=f32).reshape(
        -1, items, width
    )
    summed = lax.psum_scatter(
        part.astype(jnp.bfloat16), "tp", scatter_dimension=2, tiled=True
    ).astype(jnp.float32)
    done = summed.astype(bf16)
    returned = lax.all_to_all(done, "ep", split_axis=0, concat_axis=0, tiled=True)
    columns = returned.shape[2]
    chosen = jnp.take(returned.reshape(-1, columns), place.reshape(-1), axis=0).reshape(
        seqs, top, columns
    )
    return jnp.sum(route_weights[:, :, None] * chosen.astype(f32), axis=1)


def solution(mesh):
    return jax.shard_map(
        per_device,
        mesh=mesh,
        in_specs=(
            P("ep", None),
            P("ep", "tp", None, None),
            P("ep", "tp"),
            P(),
            P(None, "tp"),
            P(None, "tp"),
            P(None, "tp"),
            P(None, "tp"),
            P(None, "tp"),
            P("tp"),
            P("tp"),
            P("tp"),
            P("tp", None),
            P(),
            P(),
            P("ep", None),
            P("ep", None),
            P("ep", None, "tp"),
            P("ep", None, "tp"),
            P("ep", "tp", None),
            P("tp"),
        ),
        out_specs=P("ep", "tp"),
        check_vma=False,
    )
```

```python
import jax
import jax.numpy as jnp
from jax import lax
from jax.experimental import pallas as pl
from jax.experimental.pallas import tpu as pltpu
from jax.sharding import PartitionSpec as P

EPS = 1e-06


def rms_scale(values):
    return lax.rsqrt(jnp.mean(values * values, axis=-1, keepdims=True) + EPS)


def per_device(
    tokens,
    memory,
    log_scale,
    mix_gain_in,
    w_query,
    w_key,
    w_value,
    w_igate,
    w_fgate,
    igate_bias,
    fgate_bias,
    head_gain,
    w_output,
    mix_gain_out,
    ffn_gain_in,
    routes,
    route_weights,
    expert_gate,
    expert_up,
    expert_down,
    ffn_gain_out,
):
    f32 = jnp.float32
    bf16 = jnp.bfloat16
    seqs, width = tokens.shape
    partial_value = cell(
        tokens,
        memory,
        log_scale,
        mix_gain_in,
        w_query,
        w_key,
        w_value,
        w_igate,
        w_fgate,
        igate_bias,
        fgate_bias,
        head_gain,
        w_output,
    )
    others = from_others(partial_value, "tp")
    resid, ffn_in = after_mix([partial_value] + others, tokens, mix_gain_out, ffn_gain_in)
    rf = resid.astype(f32)
    lanes = lax.axis_size("tp")
    groups = lax.axis_size("ep")
    quarter = width // lanes
    own = lax.axis_index("tp") * quarter
    local_experts = expert_gate.shape[0]
    experts_all = local_experts * groups
    top = routes.shape[1]
    cap = min(seqs, max(2, 3 * seqs * top // (2 * experts_all)))
    if cap == seqs and local_experts == 1:
        routed = every_token(ffn_in, routes, route_weights, expert_gate, expert_up, expert_down)
    else:
        routed = slotted(ffn_in, routes, route_weights, expert_gate, expert_up, expert_down, cap)
    resid_part = lax.dynamic_slice_in_dim(rf, own, quarter, 1)
    total = sum_over(jnp.sum(routed * routed, axis=1), "tp")
    scaled = routed * lax.rsqrt(total / width + EPS)[:, None]
    return (resid_part + scaled * ffn_gain_out).astype(bf16)


def from_others(value, axis):
    size = lax.axis_size(axis)
    received = []
    for step in range(1, size):
        if size & (size - 1) == 0:
            pairs = [(i, i ^ step) for i in range(size)]
        else:
            pairs = [(i, (i + step) % size) for i in range(size)]
        received.append(lax.ppermute(value, axis, pairs))
    return received


def sum_over(value, axis):
    return sum(from_others(value, axis), value)


def whole():
    return pl.BlockSpec(memory_space=pltpu.VMEM)


def cell_body(heads, key_dim, value_dim, chunk, *refs):
    f32 = jnp.float32
    bf16 = jnp.bfloat16
    (tokens_h, gain_h, wi_h, wf_h, scale_h, wq_h, wk_h, wv_h, mem_h, hg_h, wo_h, ib, fb) = refs[:13]
    out = refs[13]
    (tokens, gain, wi, wf, scale, wq, wk, wv, mem, hg, wo, recall, sems) = refs[14:]
    seqs = tokens.shape[0]
    count = seqs // chunk
    pieces = [
        (tokens_h, tokens),
        (gain_h, gain),
        (wq_h, wq),
        (wi_h, wi),
        (wf_h, wf),
        (scale_h, scale),
        (wk_h, wk),
    ]
    for c in range(count):
        rows = pl.ds(c * chunk, chunk)
        pieces.append((mem_h.at[rows], mem.at[rows]))
    pieces += [(wv_h, wv), (hg_h, hg), (wo_h, wo)]
    copies = [pltpu.make_async_copy(src, dst, sems.at[i]) for i, (src, dst) in enumerate(pieces)]
    for copy in copies:
        copy.start()
    copies[0].wait()
    copies[1].wait()
    xf = tokens[...].astype(f32)
    inv = lax.rsqrt(jnp.mean(xf * xf, axis=1, keepdims=True) + EPS)
    normed = (xf * inv * gain[...]).astype(bf16)
    copies[2].wait()
    query = jnp.dot(normed, wq[...], preferred_element_type=f32) * key_dim ** (-0.5)
    for i in (3, 4, 5):
        copies[i].wait()
    wide = normed.astype(f32)
    diagonal = lax.broadcasted_iota(jnp.int32, (seqs, seqs), 0) == lax.broadcasted_iota(
        jnp.int32, (seqs, seqs), 1
    )
    carries, fresh = [], []
    for h in range(heads):
        in_pre = jnp.sum(wide * wi[h : h + 1, :].astype(f32), axis=1, keepdims=True) + ib[h]
        forget = jnp.sum(wide * wf[h : h + 1, :].astype(f32), axis=1, keepdims=True) + fb[h]
        forget_log = jnp.minimum(forget, 0.0) - jnp.log1p(jnp.exp(-jnp.abs(forget)))
        column = jnp.sum(jnp.where(diagonal, scale[h : h + 1, :], 0.0), axis=1, keepdims=True)
        carried = forget_log + column
        new_max = jnp.maximum(carried, in_pre)
        carries.append(jnp.exp(carried - new_max))
        fresh.append(jnp.exp(in_pre - new_max))
    copies[6].wait()
    keys = jnp.dot(normed, wk[...], preferred_element_type=f32)
    turned = [query[:, h * key_dim : (h + 1) * key_dim].T for h in range(heads)]
    for c in range(count):
        copies[7 + c].wait()
        for b in range(c * chunk, (c + 1) * chunk):
            for h in range(heads):
                product = turned[h][:, b : b + 1] * mem[b, h]
                recall[h, b : b + 1, :] = jnp.sum(product, axis=0, keepdims=True)
    copies[7 + count].wait()
    values = jnp.dot(normed, wv[...], preferred_element_type=f32)
    copies[8 + count].wait()
    parts = []
    for h in range(heads):
        ks = slice(h * key_dim, (h + 1) * key_dim)
        vs = slice(h * value_dim, (h + 1) * value_dim)
        match = jnp.sum(query[:, ks] * keys[:, ks], axis=1, keepdims=True)
        read = carries[h] * recall[h] + (fresh[h] * match) * values[:, vs]
        inv = lax.rsqrt(jnp.mean(read * read, axis=1, keepdims=True) + EPS)
        parts.append((read * inv * hg[:, vs]).astype(bf16))
    copies[9 + count].wait()
    headout = parts[0] if heads == 1 else jnp.concatenate(parts, axis=1)
    out[...] = jnp.dot(headout, wo[...], preferred_element_type=f32).astype(bf16)


def cell(
    tokens,
    memory,
    log_scale,
    mix_gain_in,
    w_query,
    w_key,
    w_value,
    w_igate,
    w_fgate,
    igate_bias,
    fgate_bias,
    head_gain,
    w_output,
):
    f32 = jnp.float32
    bf16 = jnp.bfloat16
    seqs, width = tokens.shape
    heads, key_dim, value_dim = memory.shape[1:]
    chunk = 4 if seqs % 4 == 0 else 1
    body = lambda *refs: cell_body(heads, key_dim, value_dim, chunk, *refs)
    operands = [
        tokens,
        mix_gain_in.reshape(1, width),
        w_igate.T,
        w_fgate.T,
        log_scale.T,
        w_query,
        w_key,
        w_value,
        memory,
        head_gain.reshape(1, heads * value_dim),
        w_output,
    ]
    return pl.pallas_call(
        body,
        out_shape=jax.ShapeDtypeStruct((seqs, w_output.shape[1]), bf16),
        in_specs=[pl.BlockSpec(memory_space=pltpu.HBM)] * len(operands)
        + [pl.BlockSpec(memory_space=pltpu.SMEM)] * 2,
        out_specs=whole(),
        scratch_shapes=[pltpu.VMEM(o.shape, o.dtype) for o in operands]
        + [
            pltpu.VMEM((heads, seqs, value_dim), f32),
            pltpu.SemaphoreType.DMA((10 + seqs // chunk,)),
        ],
        name="cell",
    )(*operands, igate_bias, fgate_bias)


def after_mix_body(count, *refs):
    f32 = jnp.float32
    bf16 = jnp.bfloat16
    parts = refs[:count]
    tokens, gain_out, gain_in, resid, ffn_in = refs[count:]
    mixed = parts[0][...].astype(f32)
    for part in parts[1:]:
        mixed = mixed + part[...].astype(f32)
    kept = (tokens[...].astype(f32) + mixed * rms_scale(mixed) * gain_out[...]).astype(bf16)
    resid[...] = kept
    rf = kept.astype(f32)
    ffn_in[...] = (rf * rms_scale(rf) * gain_in[...]).astype(bf16)


def after_mix(parts, tokens, gain_out, gain_in):
    width = tokens.shape[1]
    shape = jax.ShapeDtypeStruct(tokens.shape, jnp.bfloat16)
    return pl.pallas_call(
        lambda *refs: after_mix_body(len(parts), *refs),
        out_shape=(shape, shape),
        in_specs=[whole()] * (len(parts) + 3),
        out_specs=(whole(), whole()),
        name="after_mix",
    )(*parts, tokens, gain_out.reshape(1, width), gain_in.reshape(1, width))


def expert_body(groups, seqs, lanes, quarter, rows, gate_w, up_w, down_w, out):
    f32 = jnp.float32
    bf16 = jnp.bfloat16
    gate = jnp.dot(rows[...], gate_w[...], preferred_element_type=f32)
    up = jnp.dot(rows[...], up_w[...], preferred_element_type=f32)
    act = (gate * jax.nn.sigmoid(gate) * up).astype(bf16)
    for q in range(lanes):
        columns = slice(q * quarter, (q + 1) * quarter)
        part = jnp.dot(act, down_w[:, columns], preferred_element_type=f32).astype(bf16)
        for g in range(groups):
            out[g * lanes + q] = part[g * seqs : (g + 1) * seqs]


def expert(rows, gate_w, up_w, down_w, groups, lanes):
    seqs = rows.shape[0] // groups
    quarter = rows.shape[1] // lanes
    return pl.pallas_call(
        lambda *refs: expert_body(groups, seqs, lanes, quarter, *refs),
        out_shape=jax.ShapeDtypeStruct((groups * lanes, seqs, quarter), jnp.bfloat16),
        in_specs=[whole()] * 4,
        out_specs=whole(),
        name="expert",
    )(rows, gate_w, up_w, down_w)


def every_token(ffn_in, routes, route_weights, expert_gate, expert_up, expert_down):
    f32 = jnp.float32
    bf16 = jnp.bfloat16
    seqs, width = ffn_in.shape
    lanes = lax.axis_size("tp")
    groups = lax.axis_size("ep")
    quarter = width // lanes
    spread = jnp.broadcast_to(ffn_in[None], (groups, seqs, width))
    rows = lax.all_to_all(spread, "ep", split_axis=0, concat_axis=0, tiled=True)
    rows = rows.reshape(groups * seqs, width)
    blocks = expert(rows, expert_gate[0], expert_up[0], expert_down[0], groups, lanes)
    back = lax.all_to_all(blocks, ("ep", "tp"), split_axis=0, concat_axis=0, tiled=True)
    back = back.reshape(groups, lanes, seqs, quarter).astype(f32)
    done = jnp.sum(back, axis=1).astype(bf16).astype(f32)
    named = routes[:, :, None] == jnp.arange(groups, dtype=jnp.int32)[None, None, :]
    weights = jnp.sum(jnp.where(named, route_weights[:, :, None], 0.0), axis=1)
    return jnp.sum(weights.T[:, :, None] * done, axis=0)


def slotted(ffn_in, routes, route_weights, expert_gate, expert_up, expert_down, cap):
    f32 = jnp.float32
    bf16 = jnp.bfloat16
    seqs, width = ffn_in.shape
    top = routes.shape[1]
    local_experts = expert_gate.shape[0]
    experts_all = local_experts * lax.axis_size("ep")
    flat = routes.reshape(-1)
    hits = (flat[:, None] == jnp.arange(experts_all, dtype=jnp.int32)[None, :]).astype(jnp.int32)
    earlier = jnp.cumsum(hits, axis=0) - hits
    slot = jnp.sum(earlier * hits, axis=1)
    place = (flat * cap + slot).reshape(seqs, top)
    picker = jnp.any(
        jnp.arange(experts_all * cap, dtype=jnp.int32)[:, None, None] == place[None, :, :], axis=2
    ).astype(bf16)
    outbound = (
        jnp.dot(picker, ffn_in, preferred_element_type=f32)
        .astype(bf16)
        .reshape(experts_all, cap, width)
    )
    arrived = lax.all_to_all(outbound, "ep", split_axis=0, concat_axis=0, tiled=True)
    items = arrived.shape[1]
    rows = arrived.reshape(-1, local_experts, items, width)
    gate = jnp.einsum("secd,edf->secf", rows, expert_gate, preferred_element_type=f32)
    up = jnp.einsum("secd,edf->secf", rows, expert_up, preferred_element_type=f32)
    act = (jax.nn.silu(gate) * up).astype(bf16)
    part = jnp.einsum("secf,efd->secd", act, expert_down, preferred_element_type=f32).reshape(
        -1, items, width
    )
    summed = lax.psum_scatter(
        part.astype(jnp.bfloat16), "tp", scatter_dimension=2, tiled=True
    ).astype(jnp.float32)
    done = summed.astype(bf16)
    returned = lax.all_to_all(done, "ep", split_axis=0, concat_axis=0, tiled=True)
    columns = returned.shape[2]
    chosen = jnp.take(returned.reshape(-1, columns), place.reshape(-1), axis=0).reshape(
        seqs, top, columns
    )
    return jnp.sum(route_weights[:, :, None] * chosen.astype(f32), axis=1)


def solution(mesh):
    return jax.shard_map(
        per_device,
        mesh=mesh,
        in_specs=(
            P("ep", None),
            P("ep", "tp", None, None),
            P("ep", "tp"),
            P(),
            P(None, "tp"),
            P(None, "tp"),
            P(None, "tp"),
            P(None, "tp"),
            P(None, "tp"),
            P("tp"),
            P("tp"),
            P("tp"),
            P("tp", None),
            P(),
            P(),
            P("ep", None),
            P("ep", None),
            P("ep", None, "tp"),
            P("ep", None, "tp"),
            P("ep", "tp", None),
            P("tp"),
        ),
        out_specs=P("ep", "tp"),
        check_vma=False,
    )
```

```python
import jax
import jax.numpy as jnp
from jax import lax
from jax.experimental import pallas as pl
from jax.experimental.pallas import tpu as pltpu
from jax.sharding import PartitionSpec as P

EPS = 1e-06


def rms_scale(values):
    return lax.rsqrt(jnp.mean(values * values, axis=-1, keepdims=True) + EPS)


def per_device(
    tokens,
    memory,
    log_scale,
    mix_gain_in,
    w_query,
    w_key,
    w_value,
    w_igate,
    w_fgate,
    igate_bias,
    fgate_bias,
    head_gain,
    w_output,
    mix_gain_out,
    ffn_gain_in,
    routes,
    route_weights,
    expert_gate,
    expert_up,
    expert_down,
    ffn_gain_out,
):
    f32 = jnp.float32
    bf16 = jnp.bfloat16
    seqs, width = tokens.shape
    partial_value = cell(
        tokens,
        memory,
        log_scale,
        mix_gain_in,
        w_query,
        w_key,
        w_value,
        w_igate,
        w_fgate,
        igate_bias,
        fgate_bias,
        head_gain,
        w_output,
    )
    others = from_others(partial_value, "tp")
    lanes = lax.axis_size("tp")
    groups = lax.axis_size("ep")
    own = lax.axis_index("tp").astype(jnp.int32).reshape(1)
    resid_part, ffn_in = after_mix(
        own, [partial_value] + others, tokens, mix_gain_out, ffn_gain_in, lanes
    )
    local_experts = expert_gate.shape[0]
    experts_all = local_experts * groups
    top = routes.shape[1]
    cap = min(seqs, max(2, 3 * seqs * top // (2 * experts_all)))
    if cap == seqs and local_experts == 1:
        routed = every_token(ffn_in, routes, route_weights, expert_gate, expert_up, expert_down)
    else:
        routed = slotted(ffn_in, routes, route_weights, expert_gate, expert_up, expert_down, cap)
    total = sum_over(jnp.sum(routed * routed, axis=1), "tp")
    scaled = routed * lax.rsqrt(total / width + EPS)[:, None]
    return (resid_part.astype(f32) + scaled * ffn_gain_out).astype(bf16)


def from_others(value, axis):
    size = lax.axis_size(axis)
    received = []
    for step in range(1, size):
        if size & (size - 1) == 0:
            pairs = [(i, i ^ step) for i in range(size)]
        else:
            pairs = [(i, (i + step) % size) for i in range(size)]
        received.append(lax.ppermute(value, axis, pairs))
    return received


def sum_over(value, axis):
    return sum(from_others(value, axis), value)


def whole():
    return pl.BlockSpec(memory_space=pltpu.VMEM)


def cell_body(heads, key_dim, value_dim, chunk, *refs):
    f32 = jnp.float32
    bf16 = jnp.bfloat16
    (tokens_h, gain_h, wi_h, wf_h, scale_h, wq_h, wk_h, wv_h, mem_h, hg_h, wo_h, ib, fb) = refs[:13]
    out = refs[13]
    (tokens, gain, wi, wf, scale, wq, wk, wv, mem, hg, wo, recall, sems) = refs[14:]
    seqs = tokens.shape[0]
    count = seqs // chunk
    pieces = [
        (tokens_h, tokens),
        (gain_h, gain),
        (wq_h, wq),
        (wi_h, wi),
        (wf_h, wf),
        (scale_h, scale),
        (wk_h, wk),
    ]
    for c in range(count):
        rows = pl.ds(c * chunk, chunk)
        pieces.append((mem_h.at[rows], mem.at[rows]))
    pieces += [(wv_h, wv), (hg_h, hg), (wo_h, wo)]
    copies = [pltpu.make_async_copy(src, dst, sems.at[i]) for i, (src, dst) in enumerate(pieces)]
    for copy in copies:
        copy.start()
    copies[0].wait()
    copies[1].wait()
    xf = tokens[...].astype(f32)
    inv = lax.rsqrt(jnp.mean(xf * xf, axis=1, keepdims=True) + EPS)
    normed = (xf * inv * gain[...]).astype(bf16)
    copies[2].wait()
    query = jnp.dot(normed, wq[...], preferred_element_type=f32) * key_dim ** (-0.5)
    for i in (3, 4, 5):
        copies[i].wait()
    wide = normed.astype(f32)
    diagonal = lax.broadcasted_iota(jnp.int32, (seqs, seqs), 0) == lax.broadcasted_iota(
        jnp.int32, (seqs, seqs), 1
    )
    carries, fresh = [], []
    for h in range(heads):
        in_pre = jnp.sum(wide * wi[h : h + 1, :].astype(f32), axis=1, keepdims=True) + ib[h]
        forget = jnp.sum(wide * wf[h : h + 1, :].astype(f32), axis=1, keepdims=True) + fb[h]
        forget_log = jnp.minimum(forget, 0.0) - jnp.log1p(jnp.exp(-jnp.abs(forget)))
        column = jnp.sum(jnp.where(diagonal, scale[h : h + 1, :], 0.0), axis=1, keepdims=True)
        carried = forget_log + column
        new_max = jnp.maximum(carried, in_pre)
        carries.append(jnp.exp(carried - new_max))
        fresh.append(jnp.exp(in_pre - new_max))
    copies[6].wait()
    keys = jnp.dot(normed, wk[...], preferred_element_type=f32)
    turned = [query[:, h * key_dim : (h + 1) * key_dim].T for h in range(heads)]
    for c in range(count):
        copies[7 + c].wait()
        for b in range(c * chunk, (c + 1) * chunk):
            for h in range(heads):
                product = turned[h][:, b : b + 1] * mem[b, h]
                recall[h, b : b + 1, :] = jnp.sum(product, axis=0, keepdims=True)
    copies[7 + count].wait()
    values = jnp.dot(normed, wv[...], preferred_element_type=f32)
    copies[8 + count].wait()
    parts = []
    for h in range(heads):
        ks = slice(h * key_dim, (h + 1) * key_dim)
        vs = slice(h * value_dim, (h + 1) * value_dim)
        match = jnp.sum(query[:, ks] * keys[:, ks], axis=1, keepdims=True)
        read = carries[h] * recall[h] + (fresh[h] * match) * values[:, vs]
        inv = lax.rsqrt(jnp.mean(read * read, axis=1, keepdims=True) + EPS)
        parts.append((read * inv * hg[:, vs]).astype(bf16))
    copies[9 + count].wait()
    headout = parts[0] if heads == 1 else jnp.concatenate(parts, axis=1)
    out[...] = jnp.dot(headout, wo[...], preferred_element_type=f32).astype(bf16)


def cell(
    tokens,
    memory,
    log_scale,
    mix_gain_in,
    w_query,
    w_key,
    w_value,
    w_igate,
    w_fgate,
    igate_bias,
    fgate_bias,
    head_gain,
    w_output,
):
    f32 = jnp.float32
    bf16 = jnp.bfloat16
    seqs, width = tokens.shape
    heads, key_dim, value_dim = memory.shape[1:]
    chunk = 4 if seqs % 4 == 0 else 1
    body = lambda *refs: cell_body(heads, key_dim, value_dim, chunk, *refs)
    operands = [
        tokens,
        mix_gain_in.reshape(1, width),
        w_igate.T,
        w_fgate.T,
        log_scale.T,
        w_query,
        w_key,
        w_value,
        memory,
        head_gain.reshape(1, heads * value_dim),
        w_output,
    ]
    return pl.pallas_call(
        body,
        out_shape=jax.ShapeDtypeStruct((seqs, w_output.shape[1]), bf16),
        in_specs=[pl.BlockSpec(memory_space=pltpu.HBM)] * len(operands)
        + [pl.BlockSpec(memory_space=pltpu.SMEM)] * 2,
        out_specs=whole(),
        scratch_shapes=[pltpu.VMEM(o.shape, o.dtype) for o in operands]
        + [
            pltpu.VMEM((heads, seqs, value_dim), f32),
            pltpu.SemaphoreType.DMA((10 + seqs // chunk,)),
        ],
        compiler_params=pltpu.CompilerParams(vmem_limit_bytes=12 << 20),
        name="cell",
    )(*[pltpu.with_memory_space_constraint(o, pltpu.HBM) for o in operands], igate_bias, fgate_bias)


def after_mix_body(count, quarter, own, *refs):
    f32 = jnp.float32
    bf16 = jnp.bfloat16
    parts = refs[:count]
    tokens, gain_out, gain_in, resid_part, ffn_in, resid = refs[count:]
    mixed = parts[0][...].astype(f32)
    for part in parts[1:]:
        mixed = mixed + part[...].astype(f32)
    kept = (tokens[...].astype(f32) + mixed * rms_scale(mixed) * gain_out[...]).astype(bf16)
    resid[...] = kept
    rf = kept.astype(f32)
    ffn_in[...] = (rf * rms_scale(rf) * gain_in[...]).astype(bf16)
    resid_part[...] = resid[:, pl.ds(pl.multiple_of(own[0] * quarter, quarter), quarter)]


def after_mix(own, parts, tokens, gain_out, gain_in, lanes):
    bf16 = jnp.bfloat16
    seqs, width = tokens.shape
    quarter = width // lanes
    return pl.pallas_call(
        lambda *refs: after_mix_body(len(parts), quarter, *refs),
        out_shape=(
            jax.ShapeDtypeStruct((seqs, quarter), bf16),
            jax.ShapeDtypeStruct((seqs, width), bf16),
        ),
        in_specs=[pl.BlockSpec(memory_space=pltpu.SMEM)] + [whole()] * (len(parts) + 3),
        out_specs=(whole(), whole()),
        scratch_shapes=[pltpu.VMEM((seqs, width), bf16)],
        compiler_params=pltpu.CompilerParams(vmem_limit_bytes=8 << 20),
        name="after_mix",
    )(own, *parts, tokens, gain_out.reshape(1, width), gain_in.reshape(1, width))


def expert_body(groups, seqs, lanes, quarter, rows, gate_w, up_w, down_w, out):
    f32 = jnp.float32
    bf16 = jnp.bfloat16
    gate = jnp.dot(rows[...], gate_w[...], preferred_element_type=f32)
    up = jnp.dot(rows[...], up_w[...], preferred_element_type=f32)
    act = (gate * jax.nn.sigmoid(gate) * up).astype(bf16)
    for q in range(lanes):
        columns = slice(q * quarter, (q + 1) * quarter)
        part = jnp.dot(act, down_w[:, columns], preferred_element_type=f32).astype(bf16)
        for g in range(groups):
            out[g * lanes + q] = part[g * seqs : (g + 1) * seqs]


def expert(rows, gate_w, up_w, down_w, groups, lanes):
    seqs = rows.shape[0] // groups
    quarter = rows.shape[1] // lanes
    return pl.pallas_call(
        lambda *refs: expert_body(groups, seqs, lanes, quarter, *refs),
        out_shape=jax.ShapeDtypeStruct((groups * lanes, seqs, quarter), jnp.bfloat16),
        in_specs=[whole()] * 4,
        out_specs=whole(),
        compiler_params=pltpu.CompilerParams(vmem_limit_bytes=12 << 20),
        name="expert",
    )(rows, gate_w, up_w, down_w)


def every_token(ffn_in, routes, route_weights, expert_gate, expert_up, expert_down):
    f32 = jnp.float32
    bf16 = jnp.bfloat16
    seqs, width = ffn_in.shape
    lanes = lax.axis_size("tp")
    groups = lax.axis_size("ep")
    quarter = width // lanes
    named = routes[:, :, None] == jnp.arange(groups, dtype=jnp.int32)[None, None, :]
    weights = jnp.sum(jnp.where(named, route_weights[:, :, None], 0.0), axis=1)
    spread = jnp.broadcast_to(ffn_in[None], (groups, seqs, width))
    spread, weights, gate_w, up_w, down_w = lax.optimization_barrier(
        (spread, weights.T, expert_gate[0], expert_up[0], expert_down[0])
    )
    rows = lax.all_to_all(spread, "ep", split_axis=0, concat_axis=0, tiled=True)
    rows = rows.reshape(groups * seqs, width)
    blocks = expert(rows, gate_w, up_w, down_w, groups, lanes)
    back = lax.all_to_all(blocks, ("ep", "tp"), split_axis=0, concat_axis=0, tiled=True)
    back = back.reshape(groups, lanes, seqs, quarter).astype(f32)
    done = jnp.sum(back, axis=1).astype(bf16).astype(f32)
    return jnp.sum(weights[:, :, None] * done, axis=0)


def slotted(ffn_in, routes, route_weights, expert_gate, expert_up, expert_down, cap):
    f32 = jnp.float32
    bf16 = jnp.bfloat16
    seqs, width = ffn_in.shape
    top = routes.shape[1]
    local_experts = expert_gate.shape[0]
    experts_all = local_experts * lax.axis_size("ep")
    flat = routes.reshape(-1)
    hits = (flat[:, None] == jnp.arange(experts_all, dtype=jnp.int32)[None, :]).astype(jnp.int32)
    earlier = jnp.cumsum(hits, axis=0) - hits
    slot = jnp.sum(earlier * hits, axis=1)
    place = (flat * cap + slot).reshape(seqs, top)
    picker = jnp.any(
        jnp.arange(experts_all * cap, dtype=jnp.int32)[:, None, None] == place[None, :, :], axis=2
    ).astype(bf16)
    outbound = (
        jnp.dot(picker, ffn_in, preferred_element_type=f32)
        .astype(bf16)
        .reshape(experts_all, cap, width)
    )
    arrived = lax.all_to_all(outbound, "ep", split_axis=0, concat_axis=0, tiled=True)
    items = arrived.shape[1]
    rows = arrived.reshape(-1, local_experts, items, width)
    gate = jnp.einsum("secd,edf->secf", rows, expert_gate, preferred_element_type=f32)
    up = jnp.einsum("secd,edf->secf", rows, expert_up, preferred_element_type=f32)
    act = (jax.nn.silu(gate) * up).astype(bf16)
    part = jnp.einsum("secf,efd->secd", act, expert_down, preferred_element_type=f32).reshape(
        -1, items, width
    )
    summed = lax.psum_scatter(
        part.astype(jnp.bfloat16), "tp", scatter_dimension=2, tiled=True
    ).astype(jnp.float32)
    done = summed.astype(bf16)
    returned = lax.all_to_all(done, "ep", split_axis=0, concat_axis=0, tiled=True)
    columns = returned.shape[2]
    chosen = jnp.take(returned.reshape(-1, columns), place.reshape(-1), axis=0).reshape(
        seqs, top, columns
    )
    return jnp.sum(route_weights[:, :, None] * chosen.astype(f32), axis=1)


def solution(mesh):
    return jax.shard_map(
        per_device,
        mesh=mesh,
        in_specs=(
            P("ep", None),
            P("ep", "tp", None, None),
            P("ep", "tp"),
            P(),
            P(None, "tp"),
            P(None, "tp"),
            P(None, "tp"),
            P(None, "tp"),
            P(None, "tp"),
            P("tp"),
            P("tp"),
            P("tp"),
            P("tp", None),
            P(),
            P(),
            P("ep", None),
            P("ep", None),
            P("ep", None, "tp"),
            P("ep", None, "tp"),
            P("ep", "tp", None),
            P("tp"),
        ),
        out_specs=P("ep", "tp"),
        check_vma=False,
    )
```

```python
import jax
import jax.numpy as jnp
from jax import lax
from jax.experimental import pallas as pl
from jax.experimental.pallas import tpu as pltpu
from jax.sharding import PartitionSpec as P

EPS = 1e-06


def rms_scale(values):
    return lax.rsqrt(jnp.mean(values * values, axis=-1, keepdims=True) + EPS)


def per_device(
    tokens,
    memory,
    log_scale,
    mix_gain_in,
    w_query,
    w_key,
    w_value,
    w_igate,
    w_fgate,
    igate_bias,
    fgate_bias,
    head_gain,
    w_output,
    mix_gain_out,
    ffn_gain_in,
    routes,
    route_weights,
    expert_gate,
    expert_up,
    expert_down,
    ffn_gain_out,
):
    f32 = jnp.float32
    bf16 = jnp.bfloat16
    seqs, width = tokens.shape
    lanes = lax.axis_size("tp")
    groups = lax.axis_size("ep")
    local_experts = expert_gate.shape[0]
    experts_all = local_experts * groups
    top = routes.shape[1]
    cap = min(seqs, max(2, 3 * seqs * top // (2 * experts_all)))
    dense = cap == seqs and local_experts == 1 and lanes == 4 and seqs % 16 == 0
    partial_value = cell(
        tokens,
        memory,
        log_scale,
        mix_gain_in,
        w_query,
        w_key,
        w_value,
        w_igate,
        w_fgate,
        igate_bias,
        fgate_bias,
        head_gain,
        w_output,
        dense,
    )
    if dense:
        return every_token(
            partial_value,
            tokens,
            mix_gain_out,
            ffn_gain_in,
            routes,
            route_weights,
            expert_gate,
            expert_up,
            expert_down,
            ffn_gain_out,
        )
    quarter = width // lanes
    own = lax.axis_index("tp") * quarter
    mixed = sum_over(partial_value, "tp")
    resid = (tokens.astype(f32) + mixed * rms_scale(mixed) * mix_gain_out).astype(bf16)
    rf = resid.astype(f32)
    ffn_in = (rf * rms_scale(rf) * ffn_gain_in).astype(bf16)
    routed = slotted(ffn_in, routes, route_weights, expert_gate, expert_up, expert_down, cap)
    resid_part = lax.dynamic_slice_in_dim(rf, own, quarter, 1)
    total = sum_over(jnp.sum(routed * routed, axis=1), "tp")
    scaled = routed * lax.rsqrt(total / width + EPS)[:, None]
    return (resid_part + scaled * ffn_gain_out).astype(bf16)


def exchange(value, axis, step):
    size = lax.axis_size(axis)
    if size & (size - 1) == 0:
        pairs = [(i, i ^ step) for i in range(size)]
    else:
        pairs = [(i, (i + step) % size) for i in range(size)]
    return lax.ppermute(value, axis, pairs)


def sum_over(value, axis):
    total = value.astype(jnp.float32)
    for step in range(1, lax.axis_size(axis)):
        total = total + exchange(value, axis, step).astype(jnp.float32)
    return total


def whole():
    return pl.BlockSpec(memory_space=pltpu.VMEM)


def cell_body(heads, key_dim, value_dim, chunk, halves, *refs):
    f32 = jnp.float32
    bf16 = jnp.bfloat16
    sources, outs, rest = refs[:13], refs[13 : 14 + halves], refs[14 + halves :]
    targets, (recall, sems) = rest[:13], rest[13:]
    (tokens, gain, wi, wf, ib, fb, scale, wq, wk, wv, mem, hg, wo) = targets
    seqs = tokens.shape[0]
    count = seqs // chunk
    pairs = list(zip(sources, targets))
    pieces = [pairs[i] for i in (0, 1, 7, 2, 3, 4, 5, 6, 8)]
    for c in range(count):
        rows = pl.ds(c * chunk, chunk)
        pieces.append((pairs[10][0].at[rows], mem.at[rows]))
    pieces += [pairs[9], pairs[11], pairs[12]]
    copies = [pltpu.make_async_copy(src, dst, sems.at[i]) for i, (src, dst) in enumerate(pieces)]
    for copy in copies:
        copy.start()
    copies[0].wait()
    copies[1].wait()
    xf = tokens[...].astype(f32)
    inv = lax.rsqrt(jnp.mean(xf * xf, axis=1, keepdims=True) + EPS)
    normed = (xf * inv * gain[...]).astype(bf16)
    copies[2].wait()
    query = jnp.dot(normed, wq[...], preferred_element_type=f32) * key_dim ** (-0.5)
    for i in range(3, 8):
        copies[i].wait()
    wide = normed.astype(f32)
    diagonal = lax.broadcasted_iota(jnp.int32, (seqs, seqs), 0) == lax.broadcasted_iota(
        jnp.int32, (seqs, seqs), 1
    )
    carries, fresh = [], []
    for h in range(heads):
        in_pre = jnp.sum(wide * wi[h : h + 1, :].astype(f32), axis=1, keepdims=True) + ib[:, h : h + 1]
        forget = jnp.sum(wide * wf[h : h + 1, :].astype(f32), axis=1, keepdims=True) + fb[:, h : h + 1]
        forget_log = jnp.minimum(forget, 0.0) - jnp.log1p(jnp.exp(-jnp.abs(forget)))
        column = jnp.sum(jnp.where(diagonal, scale[h : h + 1, :], 0.0), axis=1, keepdims=True)
        carried = forget_log + column
        new_max = jnp.maximum(carried, in_pre)
        carries.append(jnp.exp(carried - new_max))
        fresh.append(jnp.exp(in_pre - new_max))
    copies[8].wait()
    keys = jnp.dot(normed, wk[...], preferred_element_type=f32)
    turned = [query[:, h * key_dim : (h + 1) * key_dim].T for h in range(heads)]
    for c in range(count):
        copies[9 + c].wait()
        for b in range(c * chunk, (c + 1) * chunk):
            for h in range(heads):
                product = turned[h][:, b : b + 1] * mem[b, h]
                recall[h, b : b + 1, :] = jnp.sum(product, axis=0, keepdims=True)
    copies[9 + count].wait()
    copies[10 + count].wait()
    values = jnp.dot(normed, wv[...], preferred_element_type=f32)
    parts = []
    for h in range(heads):
        ks = slice(h * key_dim, (h + 1) * key_dim)
        vs = slice(h * value_dim, (h + 1) * value_dim)
        match = jnp.sum(query[:, ks] * keys[:, ks], axis=1, keepdims=True)
        read = carries[h] * recall[h] + (fresh[h] * match) * values[:, vs]
        inv = lax.rsqrt(jnp.mean(read * read, axis=1, keepdims=True) + EPS)
        parts.append((read * inv * hg[:, vs]).astype(bf16))
    copies[11 + count].wait()
    headout = parts[0] if heads == 1 else jnp.concatenate(parts, axis=1)
    product = jnp.dot(headout, wo[...], preferred_element_type=f32)
    if halves:
        low, high = product[: seqs // 2], product[seqs // 2 :]
        odd = lax.axis_index("tp") % 2 == 1
        outs[0][...] = jnp.where(odd, high, low).astype(bf16)
        outs[1][...] = jnp.where(odd, low, high).astype(bf16)
    else:
        outs[0][...] = product.astype(bf16)


def cell(
    tokens,
    memory,
    log_scale,
    mix_gain_in,
    w_query,
    w_key,
    w_value,
    w_igate,
    w_fgate,
    igate_bias,
    fgate_bias,
    head_gain,
    w_output,
    halves,
):
    f32 = jnp.float32
    bf16 = jnp.bfloat16
    seqs, width = tokens.shape
    heads, key_dim, value_dim = memory.shape[1:]
    chunk = 4 if seqs % 4 == 0 else 1
    body = lambda *refs: cell_body(heads, key_dim, value_dim, chunk, halves, *refs)
    operands = [
        tokens,
        mix_gain_in.reshape(1, width),
        w_igate.T,
        w_fgate.T,
        igate_bias.reshape(1, heads),
        fgate_bias.reshape(1, heads),
        log_scale.T,
        w_query,
        w_key,
        w_value,
        memory,
        head_gain.reshape(1, heads * value_dim),
        w_output,
    ]
    shape = jax.ShapeDtypeStruct((seqs // 2 if halves else seqs, w_output.shape[1]), bf16)
    result = pl.pallas_call(
        body,
        out_shape=[shape] * (2 if halves else 1),
        in_specs=[pl.BlockSpec(memory_space=pltpu.HBM)] * len(operands),
        out_specs=[whole()] * (2 if halves else 1),
        scratch_shapes=[pltpu.VMEM(o.shape, o.dtype) for o in operands]
        + [
            pltpu.VMEM((heads, seqs, value_dim), f32),
            pltpu.SemaphoreType.DMA((12 + seqs // chunk,)),
        ],
        compiler_params=pltpu.CompilerParams(vmem_limit_bytes=12 << 20),
        name="cell",
    )(*[o if o.size == heads else pltpu.with_memory_space_constraint(o, pltpu.HBM) for o in operands])
    return result if halves else result[0]


def after_mix_body(parts, tokens, gain_out, spread):
    f32 = jnp.float32
    half = tokens.shape[0] // 2
    mixed = parts[0][...].astype(f32)
    for part in parts[1:]:
        mixed = mixed + part[...].astype(f32)
    odd = lax.axis_index("tp") % 2 == 1
    xf = tokens[...].astype(f32)
    xf = jnp.where(odd, xf[half:], xf[:half])
    resid = (xf + mixed * rms_scale(mixed) * gain_out[...]).astype(jnp.bfloat16)
    for g in range(spread.shape[0]):
        spread[g] = resid


def after_mix(parts, tokens, gain_out, groups):
    seqs, width = tokens.shape
    count = len(parts)
    return pl.pallas_call(
        lambda *refs: after_mix_body(refs[:count], *refs[count:]),
        out_shape=jax.ShapeDtypeStruct((groups, seqs // 2, width), jnp.bfloat16),
        in_specs=[whole()] * (count + 2),
        out_specs=whole(),
        compiler_params=pltpu.CompilerParams(vmem_limit_bytes=8 << 20),
        name="after_mix",
    )(*parts, tokens, gain_out.reshape(1, width))


def expert_body(near, far, gain, gate_w, up_w, down_w, keep, send, resid_part, rows):
    f32 = jnp.float32
    bf16 = jnp.bfloat16
    groups, half, width = near.shape
    seqs = 2 * half
    quarter = resid_part.shape[1]
    lane = lax.axis_index("tp")
    odd = lane % 2 == 1
    mine, theirs = near[...].astype(f32), far[...].astype(f32)
    rows[:, :half] = jnp.where(odd, theirs, mine)
    rows[:, half:] = jnp.where(odd, mine, theirs)
    columns = pl.ds(pl.multiple_of(lane * quarter, quarter), quarter)
    resid_part[...] = rows[lax.axis_index("ep"), :, columns]
    rf = rows[...].reshape(groups * seqs, width)
    ffn_in = (rf * rms_scale(rf) * gain[...]).astype(bf16)
    gate = jnp.dot(ffn_in, gate_w[...], preferred_element_type=f32)
    up = jnp.dot(ffn_in, up_w[...], preferred_element_type=f32)
    act = (gate * jax.nn.sigmoid(gate) * up).astype(bf16)
    for s in range(width // quarter // 2):
        places = slice(2 * s * quarter, (2 * s + 1) * quarter)
        even_part = jnp.dot(act, down_w[:, places], preferred_element_type=f32)
        places = slice((2 * s + 1) * quarter, (2 * s + 2) * quarter)
        odd_part = jnp.dot(act, down_w[:, places], preferred_element_type=f32)
        kept = jnp.where(odd, odd_part, even_part).astype(bf16).reshape(groups, seqs, quarter)
        sent = jnp.where(odd, even_part, odd_part).astype(bf16).reshape(groups, seqs, quarter)
        places = slice(s * quarter, (s + 1) * quarter)
        keep[:, :, places] = kept
        send[:, :, places] = sent


def expert(near, far, gain, gate_w, up_w, down_w, lanes):
    groups, half, width = near.shape
    quarter = width // lanes
    shape = jax.ShapeDtypeStruct((groups, 2 * half, width // 2), jnp.bfloat16)
    return pl.pallas_call(
        expert_body,
        out_shape=(shape, shape, jax.ShapeDtypeStruct((2 * half, quarter), jnp.float32)),
        in_specs=[whole()] * 6,
        out_specs=(whole(), whole(), whole()),
        scratch_shapes=[pltpu.VMEM((groups, 2 * half, width), jnp.float32)],
        compiler_params=pltpu.CompilerParams(vmem_limit_bytes=16 << 20),
        name="expert",
    )(near, far, gain.reshape(1, width), gate_w, up_w, down_w)


def last_body(r0, r1, r2, r3, resid_part, gain, out, same):
    f32 = jnp.float32
    quarter = out.shape[1]
    width = 2 * r0.shape[1]
    kept = r0[...].astype(f32) + r2[...].astype(f32)
    other = r1[...].astype(f32) + r3[...].astype(f32)
    same[...] = kept
    total = jnp.sum(kept * kept, axis=1, keepdims=True) + jnp.sum(
        other * other, axis=1, keepdims=True
    )
    place = lax.axis_index("tp") // 2
    routed = same[:, pl.ds(pl.multiple_of(place * quarter, quarter), quarter)]
    scaled = routed * lax.rsqrt(total / width + EPS)
    out[...] = (resid_part[...] + scaled * gain[...]).astype(jnp.bfloat16)


def last(parts, resid_part, gain):
    seqs, quarter = resid_part.shape
    return pl.pallas_call(
        last_body,
        out_shape=jax.ShapeDtypeStruct((seqs, quarter), jnp.bfloat16),
        in_specs=[whole()] * 6,
        out_specs=whole(),
        scratch_shapes=[pltpu.VMEM(parts[0].shape, jnp.float32)],
        compiler_params=pltpu.CompilerParams(vmem_limit_bytes=8 << 20),
        name="last",
    )(*parts, resid_part, gain.reshape(1, quarter))


def every_token(
    halves,
    tokens,
    mix_gain_out,
    ffn_gain_in,
    routes,
    route_weights,
    expert_gate,
    expert_up,
    expert_down,
    ffn_gain_out,
):
    f32 = jnp.float32
    bf16 = jnp.bfloat16
    lanes = lax.axis_size("tp")
    groups = lax.axis_size("ep")
    mine, theirs = halves
    parts = [mine] + [exchange(theirs if step % 2 else mine, "tp", step) for step in (1, 2, 3)]
    spread = after_mix(parts, tokens, mix_gain_out, groups)
    named = routes[:, :, None] == jnp.arange(groups, dtype=jnp.int32)[None, None, :]
    weights = jnp.sum(jnp.where(named, route_weights[:, :, None], 0.0), axis=1).T
    spread, weights, gate_w, up_w, down_w, gain_in = lax.optimization_barrier(
        (spread, weights, expert_gate[0], expert_up[0], expert_down[0], ffn_gain_in)
    )
    near = lax.all_to_all(spread, "ep", split_axis=0, concat_axis=0, tiled=True)
    far = exchange(near, "tp", 1)
    keep, send, resid_part = expert(near, far, gain_in, gate_w, up_w, down_w, lanes)
    got = exchange(send, "tp", 1)
    blocks = (keep.astype(f32) + got.astype(f32)).astype(bf16)
    blocks, resid_part, ffn_gain_out = lax.optimization_barrier((blocks, resid_part, ffn_gain_out))
    back = lax.all_to_all(blocks, "ep", split_axis=0, concat_axis=0, tiled=True)
    share = jnp.sum(weights[:, :, None] * back.astype(f32), axis=0).astype(bf16)
    parts = [share] + [exchange(share, "tp", step) for step in (1, 2, 3)]
    return last(parts, resid_part, ffn_gain_out)


def slotted(ffn_in, routes, route_weights, expert_gate, expert_up, expert_down, cap):
    f32 = jnp.float32
    bf16 = jnp.bfloat16
    seqs, width = ffn_in.shape
    top = routes.shape[1]
    local_experts = expert_gate.shape[0]
    experts_all = local_experts * lax.axis_size("ep")
    flat = routes.reshape(-1)
    hits = (flat[:, None] == jnp.arange(experts_all, dtype=jnp.int32)[None, :]).astype(jnp.int32)
    earlier = jnp.cumsum(hits, axis=0) - hits
    slot = jnp.sum(earlier * hits, axis=1)
    place = (flat * cap + slot).reshape(seqs, top)
    picker = jnp.any(
        jnp.arange(experts_all * cap, dtype=jnp.int32)[:, None, None] == place[None, :, :], axis=2
    ).astype(bf16)
    outbound = (
        jnp.dot(picker, ffn_in, preferred_element_type=f32)
        .astype(bf16)
        .reshape(experts_all, cap, width)
    )
    arrived = lax.all_to_all(outbound, "ep", split_axis=0, concat_axis=0, tiled=True)
    items = arrived.shape[1]
    rows = arrived.reshape(-1, local_experts, items, width)
    gate = jnp.einsum("secd,edf->secf", rows, expert_gate, preferred_element_type=f32)
    up = jnp.einsum("secd,edf->secf", rows, expert_up, preferred_element_type=f32)
    act = (jax.nn.silu(gate) * up).astype(bf16)
    part = jnp.einsum("secf,efd->secd", act, expert_down, preferred_element_type=f32).reshape(
        -1, items, width
    )
    summed = lax.psum_scatter(
        part.astype(jnp.bfloat16), "tp", scatter_dimension=2, tiled=True
    ).astype(jnp.float32)
    done = summed.astype(bf16)
    returned = lax.all_to_all(done, "ep", split_axis=0, concat_axis=0, tiled=True)
    columns = returned.shape[2]
    chosen = jnp.take(returned.reshape(-1, columns), place.reshape(-1), axis=0).reshape(
        seqs, top, columns
    )
    return jnp.sum(route_weights[:, :, None] * chosen.astype(f32), axis=1)


def solution(mesh):
    return jax.shard_map(
        per_device,
        mesh=mesh,
        in_specs=(
            P("ep", None),
            P("ep", "tp", None, None),
            P("ep", "tp"),
            P(),
            P(None, "tp"),
            P(None, "tp"),
            P(None, "tp"),
            P(None, "tp"),
            P(None, "tp"),
            P("tp"),
            P("tp"),
            P("tp"),
            P("tp", None),
            P(),
            P(),
            P("ep", None),
            P("ep", None),
            P("ep", None, "tp"),
            P("ep", None, "tp"),
            P("ep", "tp", None),
            P("tp"),
        ),
        out_specs=P("ep", "tp"),
        check_vma=False,
    )
```

```python
import jax
import jax.numpy as jnp
from jax import lax
from jax.experimental import pallas as pl
from jax.experimental.pallas import tpu as pltpu
from jax.sharding import PartitionSpec as P


EPS = 1e-06


def rms_scale(values):
    return lax.rsqrt(jnp.mean(values * values, axis=-1, keepdims=True) + EPS)


def per_device(
    tokens,
    memory,
    log_scale,
    mix_gain_in,
    w_query,
    w_key,
    w_value,
    w_igate,
    w_fgate,
    igate_bias,
    fgate_bias,
    head_gain,
    w_output,
    mix_gain_out,
    ffn_gain_in,
    routes,
    route_weights,
    expert_gate,
    expert_up,
    expert_down,
    ffn_gain_out,
):
    f32 = jnp.float32
    bf16 = jnp.bfloat16
    seqs, width = tokens.shape
    lanes = lax.axis_size("tp")
    groups = lax.axis_size("ep")
    local_experts = expert_gate.shape[0]
    experts_all = local_experts * groups
    top = routes.shape[1]
    cap = min(seqs, max(2, 3 * seqs * top // (2 * experts_all)))
    dense = cap == seqs and local_experts == 1 and lanes == 4 and seqs % 16 == 0
    partial_value = cell(
        tokens,
        memory,
        log_scale,
        mix_gain_in,
        w_query,
        w_key,
        w_value,
        w_igate,
        w_fgate,
        igate_bias,
        fgate_bias,
        head_gain,
        w_output,
        dense,
    )
    if dense:
        return every_token(
            partial_value,
            tokens,
            mix_gain_out,
            ffn_gain_in,
            routes,
            route_weights,
            expert_gate,
            expert_up,
            expert_down,
            ffn_gain_out,
        )
    quarter = width // lanes
    own = lax.axis_index("tp") * quarter
    mixed = sum_over(partial_value, "tp")
    resid = (tokens.astype(f32) + mixed * rms_scale(mixed) * mix_gain_out).astype(bf16)
    rf = resid.astype(f32)
    ffn_in = (rf * rms_scale(rf) * ffn_gain_in).astype(bf16)
    routed = slotted(ffn_in, routes, route_weights, expert_gate, expert_up, expert_down, cap)
    resid_part = lax.dynamic_slice_in_dim(rf, own, quarter, 1)
    total = sum_over(jnp.sum(routed * routed, axis=1), "tp")
    scaled = routed * lax.rsqrt(total / width + EPS)[:, None]
    return (resid_part + scaled * ffn_gain_out).astype(bf16)


def exchange(value, axis, step):
    size = lax.axis_size(axis)
    if size & (size - 1) == 0:
        pairs = [(i, i ^ step) for i in range(size)]
    else:
        pairs = [(i, (i + step) % size) for i in range(size)]
    return lax.ppermute(value, axis, pairs)


def sum_over(value, axis):
    total = value.astype(jnp.float32)
    for step in range(1, lax.axis_size(axis)):
        total = total + exchange(value, axis, step).astype(jnp.float32)
    return total


def whole():
    return pl.BlockSpec(memory_space=pltpu.VMEM)


def cell_body(heads, key_dim, value_dim, chunk, halves, *refs):
    f32 = jnp.float32
    bf16 = jnp.bfloat16
    sources, outs, rest = refs[:13], refs[13 : 14 + halves], refs[14 + halves :]
    targets, (recall, sems) = rest[:13], rest[13:]
    (tokens, gain, wi, wf, ib, fb, scale, wq, wk, wv, mem, hg, wo) = targets
    seqs = tokens.shape[0]
    count = seqs // chunk
    pairs = list(zip(sources, targets))
    pieces = [pairs[i] for i in (0, 1, 7, 2, 3, 4, 5, 6, 8)]
    for c in range(count):
        rows = pl.ds(c * chunk, chunk)
        pieces.append((pairs[10][0].at[rows], mem.at[rows]))
    pieces += [pairs[9], pairs[11], pairs[12]]
    copies = [pltpu.make_async_copy(src, dst, sems.at[i]) for i, (src, dst) in enumerate(pieces)]
    for copy in copies:
        copy.start()
    copies[0].wait()
    copies[1].wait()
    xf = tokens[...].astype(f32)
    inv = lax.rsqrt(jnp.mean(xf * xf, axis=1, keepdims=True) + EPS)
    normed = (xf * inv * gain[...]).astype(bf16)
    copies[2].wait()
    query = jnp.dot(normed, wq[...], preferred_element_type=f32) * key_dim ** (-0.5)
    for i in range(3, 8):
        copies[i].wait()
    wide = normed.astype(f32)
    diagonal = lax.broadcasted_iota(jnp.int32, (seqs, seqs), 0) == lax.broadcasted_iota(
        jnp.int32, (seqs, seqs), 1
    )
    carries, fresh = [], []
    for h in range(heads):
        in_pre = jnp.sum(wide * wi[h : h + 1, :].astype(f32), axis=1, keepdims=True) + ib[:, h : h + 1]
        forget = jnp.sum(wide * wf[h : h + 1, :].astype(f32), axis=1, keepdims=True) + fb[:, h : h + 1]
        forget_log = jnp.minimum(forget, 0.0) - jnp.log1p(jnp.exp(-jnp.abs(forget)))
        column = jnp.sum(jnp.where(diagonal, scale[h : h + 1, :], 0.0), axis=1, keepdims=True)
        carried = forget_log + column
        new_max = jnp.maximum(carried, in_pre)
        carries.append(jnp.exp(carried - new_max))
        fresh.append(jnp.exp(in_pre - new_max))
    copies[8].wait()
    keys = jnp.dot(normed, wk[...], preferred_element_type=f32)
    turned = [query[:, h * key_dim : (h + 1) * key_dim].T for h in range(heads)]
    for c in range(count):
        copies[9 + c].wait()
        for b in range(c * chunk, (c + 1) * chunk):
            for h in range(heads):
                product = turned[h][:, b : b + 1] * mem[b, h]
                recall[h, b : b + 1, :] = jnp.sum(product, axis=0, keepdims=True)
    copies[9 + count].wait()
    copies[10 + count].wait()
    values = jnp.dot(normed, wv[...], preferred_element_type=f32)
    parts = []
    for h in range(heads):
        ks = slice(h * key_dim, (h + 1) * key_dim)
        vs = slice(h * value_dim, (h + 1) * value_dim)
        match = jnp.sum(query[:, ks] * keys[:, ks], axis=1, keepdims=True)
        read = carries[h] * recall[h] + (fresh[h] * match) * values[:, vs]
        inv = lax.rsqrt(jnp.mean(read * read, axis=1, keepdims=True) + EPS)
        parts.append((read * inv * hg[:, vs]).astype(bf16))
    copies[11 + count].wait()
    headout = parts[0] if heads == 1 else jnp.concatenate(parts, axis=1)
    product = jnp.dot(headout, wo[...], preferred_element_type=f32)
    if halves:
        low, high = product[: seqs // 2], product[seqs // 2 :]
        odd = lax.axis_index("tp") % 2 == 1
        outs[0][...] = jnp.where(odd, high, low).astype(bf16)
        outs[1][...] = jnp.where(odd, low, high).astype(bf16)
    else:
        outs[0][...] = product.astype(bf16)


def cell(
    tokens,
    memory,
    log_scale,
    mix_gain_in,
    w_query,
    w_key,
    w_value,
    w_igate,
    w_fgate,
    igate_bias,
    fgate_bias,
    head_gain,
    w_output,
    halves,
):
    f32 = jnp.float32
    bf16 = jnp.bfloat16
    seqs, width = tokens.shape
    heads, key_dim, value_dim = memory.shape[1:]
    chunk = 4 if seqs % 4 == 0 else 1
    body = lambda *refs: cell_body(heads, key_dim, value_dim, chunk, halves, *refs)
    operands = [
        tokens,
        mix_gain_in.reshape(1, width),
        w_igate.T,
        w_fgate.T,
        igate_bias.reshape(1, heads),
        fgate_bias.reshape(1, heads),
        log_scale.T,
        w_query,
        w_key,
        w_value,
        memory,
        head_gain.reshape(1, heads * value_dim),
        w_output,
    ]
    shape = jax.ShapeDtypeStruct((seqs // 2 if halves else seqs, w_output.shape[1]), bf16)
    result = pl.pallas_call(
        body,
        out_shape=[shape] * (2 if halves else 1),
        in_specs=[pl.BlockSpec(memory_space=pltpu.HBM)] * len(operands),
        out_specs=[whole()] * (2 if halves else 1),
        scratch_shapes=[pltpu.VMEM(o.shape, o.dtype) for o in operands]
        + [
            pltpu.VMEM((heads, seqs, value_dim), f32),
            pltpu.SemaphoreType.DMA((12 + seqs // chunk,)),
        ],
        compiler_params=pltpu.CompilerParams(vmem_limit_bytes=12 << 20),
        name="cell",
    )(*[o if o.size == heads else pltpu.with_memory_space_constraint(o, pltpu.HBM) for o in operands])
    return result if halves else result[0]


def after_mix_body(parts, tokens, gain_out, gain_in, resid, spread):
    f32 = jnp.float32
    half = tokens.shape[0] // 2
    mixed = parts[0][...].astype(f32)
    for part in parts[1:]:
        mixed = mixed + part[...].astype(f32)
    odd = lax.axis_index("tp") % 2 == 1
    xf = tokens[...].astype(f32)
    xf = jnp.where(odd, xf[half:], xf[:half])
    kept = (xf + mixed * rms_scale(mixed) * gain_out[...]).astype(jnp.bfloat16)
    resid[...] = kept
    rf = kept.astype(f32)
    ffn_in = (rf * rms_scale(rf) * gain_in[...]).astype(jnp.bfloat16)
    for g in range(spread.shape[0]):
        spread[g] = ffn_in


def after_mix(parts, tokens, gain_out, gain_in, groups):
    seqs, width = tokens.shape
    count = len(parts)
    return pl.pallas_call(
        lambda *refs: after_mix_body(refs[:count], *refs[count:]),
        out_shape=(
            jax.ShapeDtypeStruct((seqs // 2, width), jnp.bfloat16),
            jax.ShapeDtypeStruct((groups, seqs // 2, width), jnp.bfloat16),
        ),
        in_specs=[whole()] * (count + 3),
        out_specs=(whole(), whole()),
        compiler_params=pltpu.CompilerParams(vmem_limit_bytes=8 << 20),
        name="after_mix",
    )(*parts, tokens, gain_out.reshape(1, width), gain_in.reshape(1, width))


def expert_body(rows, gate_w, up_w, down_w, gate_n, up_n, down_n, out):
    f32 = jnp.float32
    groups, half, width = rows.shape
    ffn_in = rows[...].reshape(groups * half, width)
    total = None
    for gates, ups, downs in ((gate_w, up_w, down_w), (gate_n, up_n, down_n)):
        gate = jnp.dot(ffn_in, gates[...], preferred_element_type=f32)
        up = jnp.dot(ffn_in, ups[...], preferred_element_type=f32)
        act = (gate * jax.nn.sigmoid(gate) * up).astype(jnp.bfloat16)
        part = jnp.dot(act, downs[...], preferred_element_type=f32)
        total = part if total is None else total + part
    out[...] = total.astype(jnp.bfloat16).reshape(groups, half, width)


def expert(rows, own, neighbour):
    return pl.pallas_call(
        expert_body,
        out_shape=jax.ShapeDtypeStruct(rows.shape, jnp.bfloat16),
        in_specs=[whole()] * 7,
        out_specs=whole(),
        compiler_params=pltpu.CompilerParams(vmem_limit_bytes=16 << 20),
        name="expert",
    )(rows, *own, *neighbour)


def share_body(back, weights, resid, share, both):
    f32 = jnp.float32
    groups, half, _ = back.shape
    odd = lax.axis_index("tp") % 2 == 1
    turned = weights[...].T
    mine = jnp.where(odd, turned[half:], turned[:half])
    total = mine[:, 0:1] * back[0].astype(f32)
    for e in range(1, groups):
        total = total + mine[:, e : e + 1] * back[e].astype(f32)
    rounded = total.astype(jnp.bfloat16)
    share[...] = rounded
    both[0] = rounded
    both[1] = resid[...]


def combine(back, weights, resid):
    _, half, width = back.shape
    return pl.pallas_call(
        share_body,
        out_shape=(
            jax.ShapeDtypeStruct((half, width), jnp.bfloat16),
            jax.ShapeDtypeStruct((2, half, width), jnp.bfloat16),
        ),
        in_specs=[whole()] * 3,
        out_specs=(whole(), whole()),
        compiler_params=pltpu.CompilerParams(vmem_limit_bytes=8 << 20),
        name="share",
    )(back, weights, resid)


def last_body(share, both, other_y, other_far, resid, gain, out, picks):
    f32 = jnp.float32
    quarter = out.shape[1]
    kept = share[...].astype(f32) + other_y[...].astype(f32)
    other = both[0].astype(f32) + other_far[...].astype(f32)
    picks[0] = kept * rms_scale(kept)
    picks[1] = other * rms_scale(other)
    picks[2] = resid[...].astype(f32)
    picks[3] = both[1].astype(f32)
    lane = lax.axis_index("tp")
    odd = lane % 2 == 1
    places = pl.ds(pl.multiple_of(lane * quarter, quarter), quarter)
    mine = picks[2, :, places] + picks[0, :, places] * gain[...]
    theirs = picks[3, :, places] + picks[1, :, places] * gain[...]
    low, high = jnp.where(odd, theirs, mine), jnp.where(odd, mine, theirs)
    out[...] = jnp.concatenate([low, high], axis=0).astype(jnp.bfloat16)


def last(share, both, other_y, other_far, resid, gain):
    half, width = share.shape
    quarter = gain.shape[0]
    return pl.pallas_call(
        last_body,
        out_shape=jax.ShapeDtypeStruct((2 * half, quarter), jnp.bfloat16),
        in_specs=[whole()] * 6,
        out_specs=whole(),
        scratch_shapes=[pltpu.VMEM((4, half, width), jnp.float32)],
        compiler_params=pltpu.CompilerParams(vmem_limit_bytes=8 << 20),
        name="last",
    )(share, both, other_y, other_far, resid, gain.reshape(1, quarter))


def every_token(
    halves,
    tokens,
    mix_gain_out,
    ffn_gain_in,
    routes,
    route_weights,
    expert_gate,
    expert_up,
    expert_down,
    ffn_gain_out,
):
    groups = lax.axis_size("ep")
    mine, theirs = halves
    parts = [exchange(theirs if step % 2 else mine, "tp", step) for step in (1, 2, 3)]
    parts = [mine] + parts
    shards = (expert_gate[0], expert_up[0], expert_down[0])
    *waited, _ = lax.optimization_barrier((*shards, mine))
    neighbour = [exchange(shard, "tp", 1) for shard in waited]
    resid, spread = after_mix(parts, tokens, mix_gain_out, ffn_gain_in, groups)
    named = routes[:, :, None] == jnp.arange(groups, dtype=jnp.int32)[None, None, :]
    weights = jnp.sum(jnp.where(named, route_weights[:, :, None], 0.0), axis=1).T
    spread, weights, gain_out = lax.optimization_barrier((spread, weights, ffn_gain_out))
    rows = lax.all_to_all(spread, "ep", split_axis=0, concat_axis=0, tiled=True)
    blocks = expert(rows, shards, neighbour)
    blocks, weights, resid, gain_out = lax.optimization_barrier((blocks, weights, resid, gain_out))
    back = lax.all_to_all(blocks, "ep", split_axis=0, concat_axis=0, tiled=True)
    share, both = combine(back, weights, resid)
    return last(
        share,
        exchange(both, "tp", 1),
        exchange(share, "tp", 2),
        exchange(share, "tp", 3),
        resid,
        gain_out,
    )


def slotted(ffn_in, routes, route_weights, expert_gate, expert_up, expert_down, cap):
    f32 = jnp.float32
    bf16 = jnp.bfloat16
    seqs, width = ffn_in.shape
    top = routes.shape[1]
    local_experts = expert_gate.shape[0]
    experts_all = local_experts * lax.axis_size("ep")
    flat = routes.reshape(-1)
    hits = (flat[:, None] == jnp.arange(experts_all, dtype=jnp.int32)[None, :]).astype(jnp.int32)
    earlier = jnp.cumsum(hits, axis=0) - hits
    slot = jnp.sum(earlier * hits, axis=1)
    place = (flat * cap + slot).reshape(seqs, top)
    picker = jnp.any(
        jnp.arange(experts_all * cap, dtype=jnp.int32)[:, None, None] == place[None, :, :], axis=2
    ).astype(bf16)
    outbound = (
        jnp.dot(picker, ffn_in, preferred_element_type=f32)
        .astype(bf16)
        .reshape(experts_all, cap, width)
    )
    arrived = lax.all_to_all(outbound, "ep", split_axis=0, concat_axis=0, tiled=True)
    items = arrived.shape[1]
    rows = arrived.reshape(-1, local_experts, items, width)
    gate = jnp.einsum("secd,edf->secf", rows, expert_gate, preferred_element_type=f32)
    up = jnp.einsum("secd,edf->secf", rows, expert_up, preferred_element_type=f32)
    act = (jax.nn.silu(gate) * up).astype(bf16)
    part = jnp.einsum("secf,efd->secd", act, expert_down, preferred_element_type=f32).reshape(
        -1, items, width
    )
    summed = lax.psum_scatter(
        part.astype(jnp.bfloat16), "tp", scatter_dimension=2, tiled=True
    ).astype(jnp.float32)
    done = summed.astype(bf16)
    returned = lax.all_to_all(done, "ep", split_axis=0, concat_axis=0, tiled=True)
    columns = returned.shape[2]
    chosen = jnp.take(returned.reshape(-1, columns), place.reshape(-1), axis=0).reshape(
        seqs, top, columns
    )
    return jnp.sum(route_weights[:, :, None] * chosen.astype(f32), axis=1)


def solution(mesh):
    return jax.shard_map(
        per_device,
        mesh=mesh,
        in_specs=(
            P("ep", None),
            P("ep", "tp", None, None),
            P("ep", "tp"),
            P(),
            P(None, "tp"),
            P(None, "tp"),
            P(None, "tp"),
            P(None, "tp"),
            P(None, "tp"),
            P("tp"),
            P("tp"),
            P("tp"),
            P("tp", None),
            P(),
            P(),
            P("ep", None),
            P("ep", None),
            P("ep", None, "tp"),
            P("ep", None, "tp"),
            P("ep", "tp", None),
            P("tp"),
        ),
        out_specs=P("ep", "tp"),
        check_vma=False,
    )
```

```python
import jax
import jax.numpy as jnp
from jax import lax
from jax.experimental import pallas as pl
from jax.experimental.pallas import tpu as pltpu
from jax.sharding import PartitionSpec as P


EPS = 1e-06


def rms_scale(values):
    return lax.rsqrt(jnp.mean(values * values, axis=-1, keepdims=True) + EPS)


def per_device(
    tokens,
    memory,
    log_scale,
    mix_gain_in,
    w_query,
    w_key,
    w_value,
    w_igate,
    w_fgate,
    igate_bias,
    fgate_bias,
    head_gain,
    w_output,
    mix_gain_out,
    ffn_gain_in,
    routes,
    route_weights,
    expert_gate,
    expert_up,
    expert_down,
    ffn_gain_out,
):
    f32 = jnp.float32
    bf16 = jnp.bfloat16
    seqs, width = tokens.shape
    lanes = lax.axis_size("tp")
    groups = lax.axis_size("ep")
    local_experts = expert_gate.shape[0]
    experts_all = local_experts * groups
    top = routes.shape[1]
    cap = min(seqs, max(2, 3 * seqs * top // (2 * experts_all)))
    dense = cap == seqs and local_experts == 1 and lanes == 4 and seqs % 16 == 0
    partial_value = cell(
        tokens,
        memory,
        log_scale,
        mix_gain_in,
        w_query,
        w_key,
        w_value,
        w_igate,
        w_fgate,
        igate_bias,
        fgate_bias,
        head_gain,
        w_output,
        dense,
    )
    if dense:
        return every_token(
            partial_value,
            tokens,
            mix_gain_out,
            ffn_gain_in,
            routes,
            route_weights,
            expert_gate,
            expert_up,
            expert_down,
            ffn_gain_out,
        )
    quarter = width // lanes
    own = lax.axis_index("tp") * quarter
    mixed = sum_over(partial_value, "tp")
    resid = (tokens.astype(f32) + mixed * rms_scale(mixed) * mix_gain_out).astype(bf16)
    rf = resid.astype(f32)
    ffn_in = (rf * rms_scale(rf) * ffn_gain_in).astype(bf16)
    routed = slotted(ffn_in, routes, route_weights, expert_gate, expert_up, expert_down, cap)
    resid_part = lax.dynamic_slice_in_dim(rf, own, quarter, 1)
    total = sum_over(jnp.sum(routed * routed, axis=1), "tp")
    scaled = routed * lax.rsqrt(total / width + EPS)[:, None]
    return (resid_part + scaled * ffn_gain_out).astype(bf16)


def exchange(value, axis, step):
    size = lax.axis_size(axis)
    if size & (size - 1) == 0:
        pairs = [(i, i ^ step) for i in range(size)]
    else:
        pairs = [(i, (i + step) % size) for i in range(size)]
    return lax.ppermute(value, axis, pairs)


def sum_over(value, axis):
    total = value.astype(jnp.float32)
    for step in range(1, lax.axis_size(axis)):
        total = total + exchange(value, axis, step).astype(jnp.float32)
    return total


def whole():
    return pl.BlockSpec(memory_space=pltpu.VMEM)


def scan_body(heads, key_dim, chunk, *refs):
    f32 = jnp.float32
    bf16 = jnp.bfloat16
    sources, outs, targets = refs[:11], refs[11:18], refs[18:27]
    sems = refs[27]
    recall, values, match, in_dot, forget_dot, hg, wo = outs
    tokens, gain, wi, wf, scale, wq, wk, wv, mem = targets
    seqs = tokens.shape[0]
    count = seqs // chunk
    pairs = list(zip(sources, (*targets, hg, wo)))
    pieces = [pairs[i] for i in (0, 1, 5, 2, 3, 4, 6)]
    for c in range(count):
        rows = pl.ds(c * chunk, chunk)
        pieces.append((pairs[8][0].at[rows], mem.at[rows]))
    pieces += [pairs[7], pairs[9], pairs[10]]
    copies = [pltpu.make_async_copy(src, dst, sems.at[i]) for i, (src, dst) in enumerate(pieces)]
    for copy in copies:
        copy.start()
    copies[0].wait()
    copies[1].wait()
    xf = tokens[...].astype(f32)
    normed = (xf * rms_scale(xf) * gain[...]).astype(bf16)
    copies[2].wait()
    query = jnp.dot(normed, wq[...], preferred_element_type=f32) * key_dim ** (-0.5)
    for i in range(3, 6):
        copies[i].wait()
    wide = normed.astype(f32)
    diagonal = lax.broadcasted_iota(jnp.int32, (seqs, seqs), 0) == lax.broadcasted_iota(
        jnp.int32, (seqs, seqs), 1
    )
    for h in range(heads):
        row = slice(h, h + 1)
        in_dot[:, row] = jnp.sum(wide * wi[row, :].astype(f32), axis=1, keepdims=True)
        forget_dot[0, :, row] = jnp.sum(wide * wf[row, :].astype(f32), axis=1, keepdims=True)
        column = jnp.sum(jnp.where(diagonal, scale[row, :], 0.0), axis=1, keepdims=True)
        forget_dot[1, :, row] = column
    copies[6].wait()
    keys = jnp.dot(normed, wk[...], preferred_element_type=f32)
    for h in range(heads):
        ks = slice(h * key_dim, (h + 1) * key_dim)
        match[:, h : h + 1] = jnp.sum(query[:, ks] * keys[:, ks], axis=1, keepdims=True)
    turned = [query[:, h * key_dim : (h + 1) * key_dim].T for h in range(heads)]
    for c in range(count):
        copies[7 + c].wait()
        for b in range(c * chunk, (c + 1) * chunk):
            for h in range(heads):
                product = turned[h][:, b : b + 1] * mem[b, h]
                recall[h, b : b + 1, :] = jnp.sum(product, axis=0, keepdims=True)
    copies[7 + count].wait()
    values[...] = jnp.dot(normed, wv[...], preferred_element_type=f32)
    copies[8 + count].wait()
    copies[9 + count].wait()


def close_body(heads, halves, recall, values, match, in_dot, forget_dot, hg, wo, ib, fb, *outs):
    f32 = jnp.float32
    bf16 = jnp.bfloat16
    value_dim = recall.shape[2]
    seqs = values.shape[0]
    parts = []
    for h in range(heads):
        one = slice(h, h + 1)
        vs = slice(h * value_dim, (h + 1) * value_dim)
        in_pre = in_dot[:, one] + ib[:, one]
        forget = forget_dot[0, :, one] + fb[:, one]
        forget_log = jnp.minimum(forget, 0.0) - jnp.log1p(jnp.exp(-jnp.abs(forget)))
        carried = forget_log + forget_dot[1, :, one]
        new_max = jnp.maximum(carried, in_pre)
        carry = jnp.exp(carried - new_max)
        fresh = jnp.exp(in_pre - new_max)
        read = carry * recall[h] + (fresh * match[:, one]) * values[:, vs]
        parts.append((read * rms_scale(read) * hg[:, vs]).astype(bf16))
    headout = parts[0] if heads == 1 else jnp.concatenate(parts, axis=1)
    product = jnp.dot(headout, wo[...], preferred_element_type=f32)
    if halves:
        low, high = product[: seqs // 2], product[seqs // 2 :]
        odd = lax.axis_index("tp") % 2 == 1
        outs[0][...] = jnp.where(odd, high, low).astype(bf16)
        outs[1][...] = jnp.where(odd, low, high).astype(bf16)
    else:
        outs[0][...] = product.astype(bf16)


def cell(
    tokens,
    memory,
    log_scale,
    mix_gain_in,
    w_query,
    w_key,
    w_value,
    w_igate,
    w_fgate,
    igate_bias,
    fgate_bias,
    head_gain,
    w_output,
    halves,
):
    f32 = jnp.float32
    bf16 = jnp.bfloat16
    seqs, width = tokens.shape
    heads, key_dim, value_dim = memory.shape[1:]
    chunk = 4 if seqs % 4 == 0 else 1
    stay = [(i, i) for i in range(lax.axis_size("tp"))]
    biases = [lax.ppermute(b, "tp", stay).reshape(1, heads) for b in (igate_bias, fgate_bias)]
    operands = [
        tokens,
        mix_gain_in.reshape(1, width),
        w_igate.T,
        w_fgate.T,
        log_scale.T,
        w_query,
        w_key,
        w_value,
        memory,
        head_gain.reshape(1, heads * value_dim),
        w_output,
    ]
    found = pl.pallas_call(
        lambda *refs: scan_body(heads, key_dim, chunk, *refs),
        out_shape=[
            jax.ShapeDtypeStruct((heads, seqs, value_dim), f32),
            jax.ShapeDtypeStruct((seqs, heads * value_dim), f32),
            jax.ShapeDtypeStruct((seqs, heads), f32),
            jax.ShapeDtypeStruct((seqs, heads), f32),
            jax.ShapeDtypeStruct((2, seqs, heads), f32),
            jax.ShapeDtypeStruct((1, heads * value_dim), f32),
            jax.ShapeDtypeStruct(w_output.shape, bf16),
        ],
        in_specs=[pl.BlockSpec(memory_space=pltpu.HBM)] * len(operands),
        out_specs=[whole()] * 7,
        scratch_shapes=[pltpu.VMEM(o.shape, o.dtype) for o in operands[:9]]
        + [pltpu.SemaphoreType.DMA((10 + seqs // chunk,))],
        compiler_params=pltpu.CompilerParams(vmem_limit_bytes=12 << 20),
        name="scan",
    )(*[pltpu.with_memory_space_constraint(o, pltpu.HBM) for o in operands])
    shape = jax.ShapeDtypeStruct((seqs // 2 if halves else seqs, w_output.shape[1]), bf16)
    result = pl.pallas_call(
        lambda *refs: close_body(heads, halves, *refs),
        out_shape=[shape] * (2 if halves else 1),
        in_specs=[whole()] * 9,
        out_specs=[whole()] * (2 if halves else 1),
        compiler_params=pltpu.CompilerParams(vmem_limit_bytes=8 << 20),
        name="close",
    )(*found, *biases)
    return result if halves else result[0]


def after_mix_body(parts, tokens, gain_out, gain_in, resid, spread):
    f32 = jnp.float32
    half = tokens.shape[0] // 2
    mixed = parts[0][...].astype(f32)
    for part in parts[1:]:
        mixed = mixed + part[...].astype(f32)
    odd = lax.axis_index("tp") % 2 == 1
    xf = tokens[...].astype(f32)
    xf = jnp.where(odd, xf[half:], xf[:half])
    kept = (xf + mixed * rms_scale(mixed) * gain_out[...]).astype(jnp.bfloat16)
    resid[...] = kept
    rf = kept.astype(f32)
    ffn_in = (rf * rms_scale(rf) * gain_in[...]).astype(jnp.bfloat16)
    for g in range(spread.shape[0]):
        spread[g] = ffn_in


def after_mix(parts, tokens, gain_out, gain_in, groups):
    seqs, width = tokens.shape
    count = len(parts)
    return pl.pallas_call(
        lambda *refs: after_mix_body(refs[:count], *refs[count:]),
        out_shape=(
            jax.ShapeDtypeStruct((seqs // 2, width), jnp.bfloat16),
            jax.ShapeDtypeStruct((groups, seqs // 2, width), jnp.bfloat16),
        ),
        in_specs=[whole()] * (count + 3),
        out_specs=(whole(), whole()),
        compiler_params=pltpu.CompilerParams(vmem_limit_bytes=8 << 20),
        name="after_mix",
    )(*parts, tokens, gain_out.reshape(1, width), gain_in.reshape(1, width))


def expert_body(rows, gate_w, up_w, down_w, gate_n, up_n, down_n, out):
    f32 = jnp.float32
    groups, half, width = rows.shape
    ffn_in = rows[...].reshape(groups * half, width)
    total = None
    for gates, ups, downs in ((gate_w, up_w, down_w), (gate_n, up_n, down_n)):
        gate = jnp.dot(ffn_in, gates[...], preferred_element_type=f32)
        up = jnp.dot(ffn_in, ups[...], preferred_element_type=f32)
        act = (gate * jax.nn.sigmoid(gate) * up).astype(jnp.bfloat16)
        part = jnp.dot(act, downs[...], preferred_element_type=f32)
        total = part if total is None else total + part
    out[...] = total.astype(jnp.bfloat16).reshape(groups, half, width)


def expert(rows, own, neighbour):
    return pl.pallas_call(
        expert_body,
        out_shape=jax.ShapeDtypeStruct(rows.shape, jnp.bfloat16),
        in_specs=[whole()] * 7,
        out_specs=whole(),
        compiler_params=pltpu.CompilerParams(vmem_limit_bytes=16 << 20),
        name="expert",
    )(rows, *own, *neighbour)


def share_body(back, weights, resid, share, both):
    f32 = jnp.float32
    groups, half, _ = back.shape
    odd = lax.axis_index("tp") % 2 == 1
    turned = weights[...].T
    mine = jnp.where(odd, turned[half:], turned[:half])
    total = mine[:, 0:1] * back[0].astype(f32)
    for e in range(1, groups):
        total = total + mine[:, e : e + 1] * back[e].astype(f32)
    rounded = total.astype(jnp.bfloat16)
    share[...] = rounded
    both[0] = rounded
    both[1] = resid[...]


def combine(back, weights, resid):
    _, half, width = back.shape
    return pl.pallas_call(
        share_body,
        out_shape=(
            jax.ShapeDtypeStruct((half, width), jnp.bfloat16),
            jax.ShapeDtypeStruct((2, half, width), jnp.bfloat16),
        ),
        in_specs=[whole()] * 3,
        out_specs=(whole(), whole()),
        compiler_params=pltpu.CompilerParams(vmem_limit_bytes=8 << 20),
        name="share",
    )(back, weights, resid)


def last_body(share, both, other_y, other_far, resid, gain, out, picks):
    f32 = jnp.float32
    quarter = out.shape[1]
    kept = share[...].astype(f32) + other_y[...].astype(f32)
    other = both[0].astype(f32) + other_far[...].astype(f32)
    picks[0] = kept * rms_scale(kept)
    picks[1] = other * rms_scale(other)
    picks[2] = resid[...].astype(f32)
    picks[3] = both[1].astype(f32)
    lane = lax.axis_index("tp")
    odd = lane % 2 == 1
    places = pl.ds(pl.multiple_of(lane * quarter, quarter), quarter)
    mine = picks[2, :, places] + picks[0, :, places] * gain[...]
    theirs = picks[3, :, places] + picks[1, :, places] * gain[...]
    low, high = jnp.where(odd, theirs, mine), jnp.where(odd, mine, theirs)
    out[...] = jnp.concatenate([low, high], axis=0).astype(jnp.bfloat16)


def last(share, both, other_y, other_far, resid, gain):
    half, width = share.shape
    quarter = gain.shape[0]
    return pl.pallas_call(
        last_body,
        out_shape=jax.ShapeDtypeStruct((2 * half, quarter), jnp.bfloat16),
        in_specs=[whole()] * 6,
        out_specs=whole(),
        scratch_shapes=[pltpu.VMEM((4, half, width), jnp.float32)],
        compiler_params=pltpu.CompilerParams(vmem_limit_bytes=8 << 20),
        name="last",
    )(share, both, other_y, other_far, resid, gain.reshape(1, quarter))


def every_token(
    halves,
    tokens,
    mix_gain_out,
    ffn_gain_in,
    routes,
    route_weights,
    expert_gate,
    expert_up,
    expert_down,
    ffn_gain_out,
):
    groups = lax.axis_size("ep")
    mine, theirs = halves
    parts = [mine]
    for step in (2, 3, 1):
        parts.append(exchange(theirs if step % 2 else mine, "tp", step))
    shards = (expert_gate[0], expert_up[0], expert_down[0])
    *waited, _ = lax.optimization_barrier((*shards, mine))
    neighbour = [exchange(shard, "tp", 1) for shard in waited]
    resid, spread = after_mix(parts, tokens, mix_gain_out, ffn_gain_in, groups)
    named = routes[:, :, None] == jnp.arange(groups, dtype=jnp.int32)[None, None, :]
    weights = jnp.sum(jnp.where(named, route_weights[:, :, None], 0.0), axis=1).T
    spread, weights, gain_out = lax.optimization_barrier((spread, weights, ffn_gain_out))
    rows = lax.all_to_all(spread, "ep", split_axis=0, concat_axis=0, tiled=True)
    blocks = expert(rows, shards, neighbour)
    blocks, weights, resid, gain_out = lax.optimization_barrier((blocks, weights, resid, gain_out))
    back = lax.all_to_all(blocks, "ep", split_axis=0, concat_axis=0, tiled=True)
    share, both = combine(back, weights, resid)
    sums = {}
    for step in (2, 3, 1):
        sums[step] = exchange(both if step == 1 else share, "tp", step)
    return last(share, sums[1], sums[2], sums[3], resid, gain_out)


def slotted(ffn_in, routes, route_weights, expert_gate, expert_up, expert_down, cap):
    f32 = jnp.float32
    bf16 = jnp.bfloat16
    seqs, width = ffn_in.shape
    top = routes.shape[1]
    local_experts = expert_gate.shape[0]
    experts_all = local_experts * lax.axis_size("ep")
    flat = routes.reshape(-1)
    hits = (flat[:, None] == jnp.arange(experts_all, dtype=jnp.int32)[None, :]).astype(jnp.int32)
    earlier = jnp.cumsum(hits, axis=0) - hits
    slot = jnp.sum(earlier * hits, axis=1)
    place = (flat * cap + slot).reshape(seqs, top)
    picker = jnp.any(
        jnp.arange(experts_all * cap, dtype=jnp.int32)[:, None, None] == place[None, :, :], axis=2
    ).astype(bf16)
    outbound = (
        jnp.dot(picker, ffn_in, preferred_element_type=f32)
        .astype(bf16)
        .reshape(experts_all, cap, width)
    )
    arrived = lax.all_to_all(outbound, "ep", split_axis=0, concat_axis=0, tiled=True)
    items = arrived.shape[1]
    rows = arrived.reshape(-1, local_experts, items, width)
    gate = jnp.einsum("secd,edf->secf", rows, expert_gate, preferred_element_type=f32)
    up = jnp.einsum("secd,edf->secf", rows, expert_up, preferred_element_type=f32)
    act = (jax.nn.silu(gate) * up).astype(bf16)
    part = jnp.einsum("secf,efd->secd", act, expert_down, preferred_element_type=f32).reshape(
        -1, items, width
    )
    summed = lax.psum_scatter(
        part.astype(jnp.bfloat16), "tp", scatter_dimension=2, tiled=True
    ).astype(jnp.float32)
    done = summed.astype(bf16)
    returned = lax.all_to_all(done, "ep", split_axis=0, concat_axis=0, tiled=True)
    columns = returned.shape[2]
    chosen = jnp.take(returned.reshape(-1, columns), place.reshape(-1), axis=0).reshape(
        seqs, top, columns
    )
    return jnp.sum(route_weights[:, :, None] * chosen.astype(f32), axis=1)


def solution(mesh):
    return jax.shard_map(
        per_device,
        mesh=mesh,
        in_specs=(
            P("ep", None),
            P("ep", "tp", None, None),
            P("ep", "tp"),
            P(),
            P(None, "tp"),
            P(None, "tp"),
            P(None, "tp"),
            P(None, "tp"),
            P(None, "tp"),
            P("tp"),
            P("tp"),
            P("tp"),
            P("tp", None),
            P(),
            P(),
            P("ep", None),
            P("ep", None),
            P("ep", None, "tp"),
            P("ep", None, "tp"),
            P("ep", "tp", None),
            P("tp"),
        ),
        out_specs=P("ep", "tp"),
        check_vma=False,
    )
```

```python
import jax
import jax.numpy as jnp
from jax import lax
from jax.experimental import pallas as pl
from jax.experimental.pallas import tpu as pltpu
from jax.sharding import PartitionSpec as P


EPS = 1e-06


def rms_scale(values):
    return lax.rsqrt(jnp.mean(values * values, axis=-1, keepdims=True) + EPS)


def per_device(
    tokens,
    memory,
    log_scale,
    mix_gain_in,
    w_query,
    w_key,
    w_value,
    w_igate,
    w_fgate,
    igate_bias,
    fgate_bias,
    head_gain,
    w_output,
    mix_gain_out,
    ffn_gain_in,
    routes,
    route_weights,
    expert_gate,
    expert_up,
    expert_down,
    ffn_gain_out,
):
    f32 = jnp.float32
    bf16 = jnp.bfloat16
    seqs, width = tokens.shape
    lanes = lax.axis_size("tp")
    groups = lax.axis_size("ep")
    local_experts = expert_gate.shape[0]
    experts_all = local_experts * groups
    top = routes.shape[1]
    cap = min(seqs, max(2, 3 * seqs * top // (2 * experts_all)))
    dense = cap == seqs and local_experts == 1 and lanes == 4 and seqs % 16 == 0
    partial_value = cell(
        tokens,
        memory,
        log_scale,
        mix_gain_in,
        w_query,
        w_key,
        w_value,
        w_igate,
        w_fgate,
        igate_bias,
        fgate_bias,
        head_gain,
        w_output,
        dense,
    )
    if dense:
        return every_token(
            partial_value,
            tokens,
            mix_gain_out,
            ffn_gain_in,
            routes,
            route_weights,
            expert_gate,
            expert_up,
            expert_down,
            ffn_gain_out,
        )
    quarter = width // lanes
    own = lax.axis_index("tp") * quarter
    mixed = sum_over(partial_value, "tp")
    resid = (tokens.astype(f32) + mixed * rms_scale(mixed) * mix_gain_out).astype(bf16)
    rf = resid.astype(f32)
    ffn_in = (rf * rms_scale(rf) * ffn_gain_in).astype(bf16)
    routed = slotted(ffn_in, routes, route_weights, expert_gate, expert_up, expert_down, cap)
    resid_part = lax.dynamic_slice_in_dim(rf, own, quarter, 1)
    total = sum_over(jnp.sum(routed * routed, axis=1), "tp")
    scaled = routed * lax.rsqrt(total / width + EPS)[:, None]
    return (resid_part + scaled * ffn_gain_out).astype(bf16)


def exchange(value, axis, step):
    size = lax.axis_size(axis)
    if size & (size - 1) == 0:
        pairs = [(i, i ^ step) for i in range(size)]
    else:
        pairs = [(i, (i + step) % size) for i in range(size)]
    return lax.ppermute(value, axis, pairs)


def sum_over(value, axis):
    total = value.astype(jnp.float32)
    for step in range(1, lax.axis_size(axis)):
        total = total + exchange(value, axis, step).astype(jnp.float32)
    return total


def whole():
    return pl.BlockSpec(memory_space=pltpu.VMEM)


def cell_body(heads, key_dim, value_dim, chunk, halves, *refs):
    f32 = jnp.float32
    bf16 = jnp.bfloat16
    sources, outs, rest = refs[:13], refs[13 : 14 + halves], refs[14 + halves :]
    targets, (recall, sems) = rest[:13], rest[13:]
    (tokens, gain, wi, wf, ib, fb, scale, wq, wk, wv, mem, hg, wo) = targets
    seqs = tokens.shape[0]
    count = seqs // chunk
    pairs = list(zip(sources, targets))
    pieces = [pairs[i] for i in (0, 1, 7, 2, 3, 4, 5, 6, 8)]
    for c in range(count):
        rows = pl.ds(c * chunk, chunk)
        pieces.append((pairs[10][0].at[rows], mem.at[rows]))
    pieces += [pairs[9], pairs[11], pairs[12]]
    copies = [pltpu.make_async_copy(src, dst, sems.at[i]) for i, (src, dst) in enumerate(pieces)]
    for copy in copies:
        copy.start()
    copies[0].wait()
    copies[1].wait()
    xf = tokens[...].astype(f32)
    inv = lax.rsqrt(jnp.mean(xf * xf, axis=1, keepdims=True) + EPS)
    normed = (xf * inv * gain[...]).astype(bf16)
    copies[2].wait()
    query = jnp.dot(normed, wq[...], preferred_element_type=f32) * key_dim ** (-0.5)
    for i in range(3, 8):
        copies[i].wait()
    wide = normed.astype(f32)
    diagonal = lax.broadcasted_iota(jnp.int32, (seqs, seqs), 0) == lax.broadcasted_iota(
        jnp.int32, (seqs, seqs), 1
    )
    carries, fresh = [], []
    for h in range(heads):
        in_pre = jnp.sum(wide * wi[h : h + 1, :].astype(f32), axis=1, keepdims=True) + ib[:, h : h + 1]
        forget = jnp.sum(wide * wf[h : h + 1, :].astype(f32), axis=1, keepdims=True) + fb[:, h : h + 1]
        forget_log = jnp.minimum(forget, 0.0) - jnp.log1p(jnp.exp(-jnp.abs(forget)))
        column = jnp.sum(jnp.where(diagonal, scale[h : h + 1, :], 0.0), axis=1, keepdims=True)
        carried = forget_log + column
        new_max = jnp.maximum(carried, in_pre)
        carries.append(jnp.exp(carried - new_max))
        fresh.append(jnp.exp(in_pre - new_max))
    copies[8].wait()
    keys = jnp.dot(normed, wk[...], preferred_element_type=f32)
    turned = [query[:, h * key_dim : (h + 1) * key_dim].T for h in range(heads)]
    for c in range(count):
        copies[9 + c].wait()
        for b in range(c * chunk, (c + 1) * chunk):
            for h in range(heads):
                product = turned[h][:, b : b + 1] * mem[b, h]
                recall[h, b : b + 1, :] = jnp.sum(product, axis=0, keepdims=True)
    copies[9 + count].wait()
    copies[10 + count].wait()
    values = jnp.dot(normed, wv[...], preferred_element_type=f32)
    parts = []
    for h in range(heads):
        ks = slice(h * key_dim, (h + 1) * key_dim)
        vs = slice(h * value_dim, (h + 1) * value_dim)
        match = jnp.sum(query[:, ks] * keys[:, ks], axis=1, keepdims=True)
        read = carries[h] * recall[h] + (fresh[h] * match) * values[:, vs]
        inv = lax.rsqrt(jnp.mean(read * read, axis=1, keepdims=True) + EPS)
        parts.append((read * inv * hg[:, vs]).astype(bf16))
    copies[11 + count].wait()
    headout = parts[0] if heads == 1 else jnp.concatenate(parts, axis=1)
    product = jnp.dot(headout, wo[...], preferred_element_type=f32)
    if halves:
        low, high = product[: seqs // 2], product[seqs // 2 :]
        odd = lax.axis_index("tp") % 2 == 1
        outs[0][...] = jnp.where(odd, high, low).astype(bf16)
        outs[1][...] = jnp.where(odd, low, high).astype(bf16)
    else:
        outs[0][...] = product.astype(bf16)


def cell(
    tokens,
    memory,
    log_scale,
    mix_gain_in,
    w_query,
    w_key,
    w_value,
    w_igate,
    w_fgate,
    igate_bias,
    fgate_bias,
    head_gain,
    w_output,
    halves,
):
    f32 = jnp.float32
    bf16 = jnp.bfloat16
    seqs, width = tokens.shape
    heads, key_dim, value_dim = memory.shape[1:]
    chunk = 4 if seqs % 4 == 0 else 1
    body = lambda *refs: cell_body(heads, key_dim, value_dim, chunk, halves, *refs)
    operands = [
        tokens,
        mix_gain_in.reshape(1, width),
        w_igate.T,
        w_fgate.T,
        igate_bias.reshape(1, heads),
        fgate_bias.reshape(1, heads),
        log_scale.T,
        w_query,
        w_key,
        w_value,
        memory,
        head_gain.reshape(1, heads * value_dim),
        w_output,
    ]
    shape = jax.ShapeDtypeStruct((seqs // 2 if halves else seqs, w_output.shape[1]), bf16)
    result = pl.pallas_call(
        body,
        out_shape=[shape] * (2 if halves else 1),
        in_specs=[pl.BlockSpec(memory_space=pltpu.HBM)] * len(operands),
        out_specs=[whole()] * (2 if halves else 1),
        scratch_shapes=[pltpu.VMEM(o.shape, o.dtype) for o in operands]
        + [
            pltpu.VMEM((heads, seqs, value_dim), f32),
            pltpu.SemaphoreType.DMA((12 + seqs // chunk,)),
        ],
        compiler_params=pltpu.CompilerParams(vmem_limit_bytes=12 << 20),
        name="cell",
    )(*[o if o.size == heads else pltpu.with_memory_space_constraint(o, pltpu.HBM) for o in operands])
    return result if halves else result[0]


def after_mix_body(parts, tokens, gain_out, gain_in, resid, spread):
    f32 = jnp.float32
    half = tokens.shape[0] // 2
    mixed = parts[0][...].astype(f32)
    for part in parts[1:]:
        mixed = mixed + part[...].astype(f32)
    odd = lax.axis_index("tp") % 2 == 1
    xf = tokens[...].astype(f32)
    xf = jnp.where(odd, xf[half:], xf[:half])
    kept = (xf + mixed * rms_scale(mixed) * gain_out[...]).astype(jnp.bfloat16)
    resid[...] = kept
    rf = kept.astype(f32)
    ffn_in = (rf * rms_scale(rf) * gain_in[...]).astype(jnp.bfloat16)
    for g in range(spread.shape[0]):
        spread[g] = ffn_in


def after_mix(parts, tokens, gain_out, gain_in, groups):
    seqs, width = tokens.shape
    count = len(parts)
    return pl.pallas_call(
        lambda *refs: after_mix_body(refs[:count], *refs[count:]),
        out_shape=(
            jax.ShapeDtypeStruct((seqs // 2, width), jnp.bfloat16),
            jax.ShapeDtypeStruct((groups, seqs // 2, width), jnp.bfloat16),
        ),
        in_specs=[whole()] * (count + 3),
        out_specs=(whole(), whole()),
        compiler_params=pltpu.CompilerParams(vmem_limit_bytes=8 << 20),
        name="after_mix",
    )(*parts, tokens, gain_out.reshape(1, width), gain_in.reshape(1, width))


def expert_body(rows, gate_w, up_w, down_w, gate_n, up_n, down_n, out):
    f32 = jnp.float32
    groups, half, width = rows.shape
    ffn_in = rows[...].reshape(groups * half, width)
    total = None
    for gates, ups, downs in ((gate_w, up_w, down_w), (gate_n, up_n, down_n)):
        gate = jnp.dot(ffn_in, gates[...], preferred_element_type=f32)
        up = jnp.dot(ffn_in, ups[...], preferred_element_type=f32)
        act = (gate * jax.nn.sigmoid(gate) * up).astype(jnp.bfloat16)
        part = jnp.dot(act, downs[...], preferred_element_type=f32)
        total = part if total is None else total + part
    out[...] = total.astype(jnp.bfloat16).reshape(groups, half, width)


def expert(rows, own, neighbour):
    return pl.pallas_call(
        expert_body,
        out_shape=jax.ShapeDtypeStruct(rows.shape, jnp.bfloat16),
        in_specs=[whole()] * 7,
        out_specs=whole(),
        compiler_params=pltpu.CompilerParams(vmem_limit_bytes=16 << 20),
        name="expert",
    )(rows, *own, *neighbour)


def share_body(back, weights, resid, share, both):
    f32 = jnp.float32
    groups, half, _ = back.shape
    odd = lax.axis_index("tp") % 2 == 1
    turned = weights[...].T
    mine = jnp.where(odd, turned[half:], turned[:half])
    total = mine[:, 0:1] * back[0].astype(f32)
    for e in range(1, groups):
        total = total + mine[:, e : e + 1] * back[e].astype(f32)
    rounded = total.astype(jnp.bfloat16)
    share[...] = rounded
    both[0] = rounded
    both[1] = resid[...]


def combine(back, weights, resid):
    _, half, width = back.shape
    return pl.pallas_call(
        share_body,
        out_shape=(
            jax.ShapeDtypeStruct((half, width), jnp.bfloat16),
            jax.ShapeDtypeStruct((2, half, width), jnp.bfloat16),
        ),
        in_specs=[whole()] * 3,
        out_specs=(whole(), whole()),
        compiler_params=pltpu.CompilerParams(vmem_limit_bytes=8 << 20),
        name="share",
    )(back, weights, resid)


def last_body(share, both, other_y, other_far, resid, gain, out, picks):
    f32 = jnp.float32
    quarter = out.shape[1]
    kept = share[...].astype(f32) + other_y[...].astype(f32)
    other = both[0].astype(f32) + other_far[...].astype(f32)
    picks[0] = kept * rms_scale(kept)
    picks[1] = other * rms_scale(other)
    picks[2] = resid[...].astype(f32)
    picks[3] = both[1].astype(f32)
    lane = lax.axis_index("tp")
    odd = lane % 2 == 1
    places = pl.ds(pl.multiple_of(lane * quarter, quarter), quarter)
    mine = picks[2, :, places] + picks[0, :, places] * gain[...]
    theirs = picks[3, :, places] + picks[1, :, places] * gain[...]
    low, high = jnp.where(odd, theirs, mine), jnp.where(odd, mine, theirs)
    out[...] = jnp.concatenate([low, high], axis=0).astype(jnp.bfloat16)


def last(share, both, other_y, other_far, resid, gain):
    half, width = share.shape
    quarter = gain.shape[0]
    return pl.pallas_call(
        last_body,
        out_shape=jax.ShapeDtypeStruct((2 * half, quarter), jnp.bfloat16),
        in_specs=[whole()] * 6,
        out_specs=whole(),
        scratch_shapes=[pltpu.VMEM((4, half, width), jnp.float32)],
        compiler_params=pltpu.CompilerParams(vmem_limit_bytes=8 << 20),
        name="last",
    )(share, both, other_y, other_far, resid, gain.reshape(1, quarter))


def every_token(
    halves,
    tokens,
    mix_gain_out,
    ffn_gain_in,
    routes,
    route_weights,
    expert_gate,
    expert_up,
    expert_down,
    ffn_gain_out,
):
    groups = lax.axis_size("ep")
    mine, theirs = halves
    parts = [mine]
    for step in (2, 3, 1):
        parts.append(exchange(theirs if step % 2 else mine, "tp", step))
    shards = (expert_gate[0], expert_up[0], expert_down[0])
    *waited, _ = lax.optimization_barrier((*shards, mine))
    neighbour = [exchange(shard, "tp", 1) for shard in waited]
    resid, spread = after_mix(parts, tokens, mix_gain_out, ffn_gain_in, groups)
    named = routes[:, :, None] == jnp.arange(groups, dtype=jnp.int32)[None, None, :]
    weights = jnp.sum(jnp.where(named, route_weights[:, :, None], 0.0), axis=1).T
    spread, weights, gain_out = lax.optimization_barrier((spread, weights, ffn_gain_out))
    rows = lax.all_to_all(spread, "ep", split_axis=0, concat_axis=0, tiled=True)
    blocks = expert(rows, shards, neighbour)
    blocks, weights, resid, gain_out = lax.optimization_barrier((blocks, weights, resid, gain_out))
    back = lax.all_to_all(blocks, "ep", split_axis=0, concat_axis=0, tiled=True)
    share, both = combine(back, weights, resid)
    sums = {}
    for step in (3, 2, 1):
        sums[step] = exchange(both if step == 1 else share, "tp", step)
    return last(share, sums[1], sums[2], sums[3], resid, gain_out)


def slotted(ffn_in, routes, route_weights, expert_gate, expert_up, expert_down, cap):
    f32 = jnp.float32
    bf16 = jnp.bfloat16
    seqs, width = ffn_in.shape
    top = routes.shape[1]
    local_experts = expert_gate.shape[0]
    experts_all = local_experts * lax.axis_size("ep")
    flat = routes.reshape(-1)
    hits = (flat[:, None] == jnp.arange(experts_all, dtype=jnp.int32)[None, :]).astype(jnp.int32)
    earlier = jnp.cumsum(hits, axis=0) - hits
    slot = jnp.sum(earlier * hits, axis=1)
    place = (flat * cap + slot).reshape(seqs, top)
    picker = jnp.any(
        jnp.arange(experts_all * cap, dtype=jnp.int32)[:, None, None] == place[None, :, :], axis=2
    ).astype(bf16)
    outbound = (
        jnp.dot(picker, ffn_in, preferred_element_type=f32)
        .astype(bf16)
        .reshape(experts_all, cap, width)
    )
    arrived = lax.all_to_all(outbound, "ep", split_axis=0, concat_axis=0, tiled=True)
    items = arrived.shape[1]
    rows = arrived.reshape(-1, local_experts, items, width)
    gate = jnp.einsum("secd,edf->secf", rows, expert_gate, preferred_element_type=f32)
    up = jnp.einsum("secd,edf->secf", rows, expert_up, preferred_element_type=f32)
    act = (jax.nn.silu(gate) * up).astype(bf16)
    part = jnp.einsum("secf,efd->secd", act, expert_down, preferred_element_type=f32).reshape(
        -1, items, width
    )
    summed = lax.psum_scatter(
        part.astype(jnp.bfloat16), "tp", scatter_dimension=2, tiled=True
    ).astype(jnp.float32)
    done = summed.astype(bf16)
    returned = lax.all_to_all(done, "ep", split_axis=0, concat_axis=0, tiled=True)
    columns = returned.shape[2]
    chosen = jnp.take(returned.reshape(-1, columns), place.reshape(-1), axis=0).reshape(
        seqs, top, columns
    )
    return jnp.sum(route_weights[:, :, None] * chosen.astype(f32), axis=1)


def solution(mesh):
    return jax.shard_map(
        per_device,
        mesh=mesh,
        in_specs=(
            P("ep", None),
            P("ep", "tp", None, None),
            P("ep", "tp"),
            P(),
            P(None, "tp"),
            P(None, "tp"),
            P(None, "tp"),
            P(None, "tp"),
            P(None, "tp"),
            P("tp"),
            P("tp"),
            P("tp"),
            P("tp", None),
            P(),
            P(),
            P("ep", None),
            P("ep", None),
            P("ep", None, "tp"),
            P("ep", None, "tp"),
            P("ep", "tp", None),
            P("tp"),
        ),
        out_specs=P("ep", "tp"),
        check_vma=False,
    )
```

```python
import jax
import jax.numpy as jnp
from jax import lax
from jax.experimental import pallas as pl
from jax.experimental.pallas import tpu as pltpu
from jax.sharding import PartitionSpec as P


EPS = 1e-06


def rms_scale(values):
    return lax.rsqrt(jnp.mean(values * values, axis=-1, keepdims=True) + EPS)


def per_device(
    tokens,
    memory,
    log_scale,
    mix_gain_in,
    w_query,
    w_key,
    w_value,
    w_igate,
    w_fgate,
    igate_bias,
    fgate_bias,
    head_gain,
    w_output,
    mix_gain_out,
    ffn_gain_in,
    routes,
    route_weights,
    expert_gate,
    expert_up,
    expert_down,
    ffn_gain_out,
):
    f32 = jnp.float32
    bf16 = jnp.bfloat16
    seqs, width = tokens.shape
    lanes = lax.axis_size("tp")
    groups = lax.axis_size("ep")
    local_experts = expert_gate.shape[0]
    experts_all = local_experts * groups
    top = routes.shape[1]
    cap = min(seqs, max(2, 3 * seqs * top // (2 * experts_all)))
    dense = cap == seqs and local_experts == 1 and lanes == 4 and seqs % 16 == 0
    partial_value = cell(
        tokens,
        memory,
        log_scale,
        mix_gain_in,
        w_query,
        w_key,
        w_value,
        w_igate,
        w_fgate,
        igate_bias,
        fgate_bias,
        head_gain,
        w_output,
        dense,
    )
    if dense:
        return every_token(
            partial_value,
            tokens,
            mix_gain_out,
            ffn_gain_in,
            routes,
            route_weights,
            expert_gate,
            expert_up,
            expert_down,
            ffn_gain_out,
        )
    quarter = width // lanes
    own = lax.axis_index("tp") * quarter
    mixed = sum_over(partial_value, "tp")
    resid = (tokens.astype(f32) + mixed * rms_scale(mixed) * mix_gain_out).astype(bf16)
    rf = resid.astype(f32)
    ffn_in = (rf * rms_scale(rf) * ffn_gain_in).astype(bf16)
    routed = slotted(ffn_in, routes, route_weights, expert_gate, expert_up, expert_down, cap)
    resid_part = lax.dynamic_slice_in_dim(rf, own, quarter, 1)
    total = sum_over(jnp.sum(routed * routed, axis=1), "tp")
    scaled = routed * lax.rsqrt(total / width + EPS)[:, None]
    return (resid_part + scaled * ffn_gain_out).astype(bf16)


def exchange(value, axis, step):
    size = lax.axis_size(axis)
    if size & (size - 1) == 0:
        pairs = [(i, i ^ step) for i in range(size)]
    else:
        pairs = [(i, (i + step) % size) for i in range(size)]
    return lax.ppermute(value, axis, pairs)


def sum_over(value, axis):
    total = value.astype(jnp.float32)
    for step in range(1, lax.axis_size(axis)):
        total = total + exchange(value, axis, step).astype(jnp.float32)
    return total


def whole():
    return pl.BlockSpec(memory_space=pltpu.VMEM)


def norm_body(tokens_h, gain_h, normed, tokens, gain, sems):
    copies = [
        pltpu.make_async_copy(tokens_h, tokens, sems.at[0]),
        pltpu.make_async_copy(gain_h, gain, sems.at[1]),
    ]
    for copy in copies:
        copy.start()
    for copy in copies:
        copy.wait()
    xf = tokens[...].astype(jnp.float32)
    normed[...] = (xf * rms_scale(xf) * gain[...]).astype(jnp.bfloat16)


def norm(tokens, gain):
    operands = [tokens, gain.reshape(1, tokens.shape[1])]
    return pl.pallas_call(
        norm_body,
        out_shape=jax.ShapeDtypeStruct(tokens.shape, jnp.bfloat16),
        in_specs=[pl.BlockSpec(memory_space=pltpu.HBM)] * 2,
        out_specs=whole(),
        scratch_shapes=[pltpu.VMEM(o.shape, o.dtype) for o in operands]
        + [pltpu.SemaphoreType.DMA((2,))],
        compiler_params=pltpu.CompilerParams(vmem_limit_bytes=4 << 20),
        cost_estimate=pl.CostEstimate(flops=11 * 10**8, transcendentals=0, bytes_accessed=65536),
        name="norm",
    )(*[pltpu.with_memory_space_constraint(o, pltpu.HBM) for o in operands])


def cell_body(heads, key_dim, value_dim, halves, *refs):
    f32 = jnp.float32
    bf16 = jnp.bfloat16
    (normed_ref, wi, wf, ib, fb, scale, wq, wk, wv, mem, hg, wo) = refs[:12]
    outs, recall = refs[12:-1], refs[-1]
    normed = normed_ref[...]
    seqs = normed.shape[0]
    query = jnp.dot(normed, wq[...], preferred_element_type=f32) * key_dim ** (-0.5)
    wide = normed.astype(f32)
    diagonal = lax.broadcasted_iota(jnp.int32, (seqs, seqs), 0) == lax.broadcasted_iota(
        jnp.int32, (seqs, seqs), 1
    )
    carries, fresh = [], []
    for h in range(heads):
        in_pre = jnp.sum(wide * wi[h : h + 1, :].astype(f32), axis=1, keepdims=True) + ib[:, h : h + 1]
        forget = jnp.sum(wide * wf[h : h + 1, :].astype(f32), axis=1, keepdims=True) + fb[:, h : h + 1]
        forget_log = jnp.minimum(forget, 0.0) - jnp.log1p(jnp.exp(-jnp.abs(forget)))
        column = jnp.sum(jnp.where(diagonal, scale[h : h + 1, :], 0.0), axis=1, keepdims=True)
        carried = forget_log + column
        new_max = jnp.maximum(carried, in_pre)
        carries.append(jnp.exp(carried - new_max))
        fresh.append(jnp.exp(in_pre - new_max))
    keys = jnp.dot(normed, wk[...], preferred_element_type=f32)
    turned = [query[:, h * key_dim : (h + 1) * key_dim].T for h in range(heads)]
    for b in range(seqs):
        for h in range(heads):
            product = turned[h][:, b : b + 1] * mem[b, h]
            recall[h, b : b + 1, :] = jnp.sum(product, axis=0, keepdims=True)
    values = jnp.dot(normed, wv[...], preferred_element_type=f32)
    parts = []
    for h in range(heads):
        ks = slice(h * key_dim, (h + 1) * key_dim)
        vs = slice(h * value_dim, (h + 1) * value_dim)
        match = jnp.sum(query[:, ks] * keys[:, ks], axis=1, keepdims=True)
        read = carries[h] * recall[h] + (fresh[h] * match) * values[:, vs]
        inv = lax.rsqrt(jnp.mean(read * read, axis=1, keepdims=True) + EPS)
        parts.append((read * inv * hg[:, vs]).astype(bf16))
    headout = parts[0] if heads == 1 else jnp.concatenate(parts, axis=1)
    product = jnp.dot(headout, wo[...], preferred_element_type=f32)
    if halves:
        low, high = product[: seqs // 2], product[seqs // 2 :]
        odd = lax.axis_index("tp") % 2 == 1
        outs[0][...] = jnp.where(odd, high, low).astype(bf16)
        outs[1][...] = jnp.where(odd, low, high).astype(bf16)
    else:
        outs[0][...] = product.astype(bf16)


def cell(
    tokens,
    memory,
    log_scale,
    mix_gain_in,
    w_query,
    w_key,
    w_value,
    w_igate,
    w_fgate,
    igate_bias,
    fgate_bias,
    head_gain,
    w_output,
    halves,
):
    f32 = jnp.float32
    bf16 = jnp.bfloat16
    seqs, _ = tokens.shape
    heads, key_dim, value_dim = memory.shape[1:]
    body = lambda *refs: cell_body(heads, key_dim, value_dim, halves, *refs)
    normed = norm(tokens, mix_gain_in)
    normed, igate_bias, fgate_bias = lax.optimization_barrier((normed, igate_bias, fgate_bias))
    operands = [
        normed,
        w_igate.T,
        w_fgate.T,
        igate_bias.reshape(1, heads),
        fgate_bias.reshape(1, heads),
        log_scale.T,
        w_query,
        w_key,
        w_value,
        memory,
        head_gain.reshape(1, heads * value_dim),
        w_output,
    ]
    shape = jax.ShapeDtypeStruct((seqs // 2 if halves else seqs, w_output.shape[1]), bf16)
    result = pl.pallas_call(
        body,
        out_shape=[shape] * (2 if halves else 1),
        in_specs=[whole()] * len(operands),
        out_specs=[whole()] * (2 if halves else 1),
        scratch_shapes=[pltpu.VMEM((heads, seqs, value_dim), f32)],
        compiler_params=pltpu.CompilerParams(vmem_limit_bytes=12 << 20),
        name="cell",
    )(*operands)
    return result if halves else result[0]


def after_mix_body(parts, tokens, gain_out, gain_in, resid, spread):
    f32 = jnp.float32
    half = tokens.shape[0] // 2
    mixed = parts[0][...].astype(f32)
    for part in parts[1:]:
        mixed = mixed + part[...].astype(f32)
    odd = lax.axis_index("tp") % 2 == 1
    xf = tokens[...].astype(f32)
    xf = jnp.where(odd, xf[half:], xf[:half])
    kept = (xf + mixed * rms_scale(mixed) * gain_out[...]).astype(jnp.bfloat16)
    resid[...] = kept
    rf = kept.astype(f32)
    ffn_in = (rf * rms_scale(rf) * gain_in[...]).astype(jnp.bfloat16)
    for g in range(spread.shape[0]):
        spread[g] = ffn_in


def after_mix(parts, tokens, gain_out, gain_in, groups):
    seqs, width = tokens.shape
    count = len(parts)
    return pl.pallas_call(
        lambda *refs: after_mix_body(refs[:count], *refs[count:]),
        out_shape=(
            jax.ShapeDtypeStruct((seqs // 2, width), jnp.bfloat16),
            jax.ShapeDtypeStruct((groups, seqs // 2, width), jnp.bfloat16),
        ),
        in_specs=[whole()] * (count + 3),
        out_specs=(whole(), whole()),
        compiler_params=pltpu.CompilerParams(vmem_limit_bytes=8 << 20),
        name="after_mix",
    )(*parts, tokens, gain_out.reshape(1, width), gain_in.reshape(1, width))


def expert_body(rows, gate_w, up_w, down_w, gate_n, up_n, down_n, out):
    f32 = jnp.float32
    groups, half, width = rows.shape
    ffn_in = rows[...].reshape(groups * half, width)
    total = None
    for gates, ups, downs in ((gate_w, up_w, down_w), (gate_n, up_n, down_n)):
        gate = jnp.dot(ffn_in, gates[...], preferred_element_type=f32)
        up = jnp.dot(ffn_in, ups[...], preferred_element_type=f32)
        act = (gate * jax.nn.sigmoid(gate) * up).astype(jnp.bfloat16)
        part = jnp.dot(act, downs[...], preferred_element_type=f32)
        total = part if total is None else total + part
    out[...] = total.astype(jnp.bfloat16).reshape(groups, half, width)


def expert(rows, own, neighbour):
    return pl.pallas_call(
        expert_body,
        out_shape=jax.ShapeDtypeStruct(rows.shape, jnp.bfloat16),
        in_specs=[whole()] * 7,
        out_specs=whole(),
        compiler_params=pltpu.CompilerParams(vmem_limit_bytes=16 << 20),
        name="expert",
    )(rows, *own, *neighbour)


def share_body(back, weights, resid, share, both):
    f32 = jnp.float32
    groups, half, _ = back.shape
    odd = lax.axis_index("tp") % 2 == 1
    turned = weights[...].T
    mine = jnp.where(odd, turned[half:], turned[:half])
    total = mine[:, 0:1] * back[0].astype(f32)
    for e in range(1, groups):
        total = total + mine[:, e : e + 1] * back[e].astype(f32)
    rounded = total.astype(jnp.bfloat16)
    share[...] = rounded
    both[0] = rounded
    both[1] = resid[...]


def combine(back, weights, resid):
    _, half, width = back.shape
    return pl.pallas_call(
        share_body,
        out_shape=(
            jax.ShapeDtypeStruct((half, width), jnp.bfloat16),
            jax.ShapeDtypeStruct((2, half, width), jnp.bfloat16),
        ),
        in_specs=[whole()] * 3,
        out_specs=(whole(), whole()),
        compiler_params=pltpu.CompilerParams(vmem_limit_bytes=8 << 20),
        name="share",
    )(back, weights, resid)


def last_body(share, both, other_y, other_far, resid, gain, out, picks):
    f32 = jnp.float32
    quarter = out.shape[1]
    kept = share[...].astype(f32) + other_y[...].astype(f32)
    other = both[0].astype(f32) + other_far[...].astype(f32)
    picks[0] = kept * rms_scale(kept)
    picks[1] = other * rms_scale(other)
    picks[2] = resid[...].astype(f32)
    picks[3] = both[1].astype(f32)
    lane = lax.axis_index("tp")
    odd = lane % 2 == 1
    places = pl.ds(pl.multiple_of(lane * quarter, quarter), quarter)
    mine = picks[2, :, places] + picks[0, :, places] * gain[...]
    theirs = picks[3, :, places] + picks[1, :, places] * gain[...]
    low, high = jnp.where(odd, theirs, mine), jnp.where(odd, mine, theirs)
    out[...] = jnp.concatenate([low, high], axis=0).astype(jnp.bfloat16)


def last(share, both, other_y, other_far, resid, gain):
    half, width = share.shape
    quarter = gain.shape[0]
    return pl.pallas_call(
        last_body,
        out_shape=jax.ShapeDtypeStruct((2 * half, quarter), jnp.bfloat16),
        in_specs=[whole()] * 6,
        out_specs=whole(),
        scratch_shapes=[pltpu.VMEM((4, half, width), jnp.float32)],
        compiler_params=pltpu.CompilerParams(vmem_limit_bytes=8 << 20),
        name="last",
    )(share, both, other_y, other_far, resid, gain.reshape(1, quarter))


def every_token(
    halves,
    tokens,
    mix_gain_out,
    ffn_gain_in,
    routes,
    route_weights,
    expert_gate,
    expert_up,
    expert_down,
    ffn_gain_out,
):
    groups = lax.axis_size("ep")
    mine, theirs = halves
    parts = [mine]
    for step in (2, 3, 1):
        parts.append(exchange(theirs if step % 2 else mine, "tp", step))
    shards = (expert_gate[0], expert_up[0], expert_down[0])
    *waited, _ = lax.optimization_barrier((*shards, mine))
    neighbour = [exchange(shard, "tp", 1) for shard in waited]
    resid, spread = after_mix(parts, tokens, mix_gain_out, ffn_gain_in, groups)
    named = routes[:, :, None] == jnp.arange(groups, dtype=jnp.int32)[None, None, :]
    weights = jnp.sum(jnp.where(named, route_weights[:, :, None], 0.0), axis=1).T
    spread, weights, gain_out = lax.optimization_barrier((spread, weights, ffn_gain_out))
    rows = lax.all_to_all(spread, "ep", split_axis=0, concat_axis=0, tiled=True)
    blocks = expert(rows, shards, neighbour)
    blocks, weights, resid, gain_out = lax.optimization_barrier((blocks, weights, resid, gain_out))
    back = lax.all_to_all(blocks, "ep", split_axis=0, concat_axis=0, tiled=True)
    share, both = combine(back, weights, resid)
    sums = {}
    for step in (3, 2, 1):
        sums[step] = exchange(both if step == 1 else share, "tp", step)
    return last(share, sums[1], sums[2], sums[3], resid, gain_out)


def slotted(ffn_in, routes, route_weights, expert_gate, expert_up, expert_down, cap):
    f32 = jnp.float32
    bf16 = jnp.bfloat16
    seqs, width = ffn_in.shape
    top = routes.shape[1]
    local_experts = expert_gate.shape[0]
    experts_all = local_experts * lax.axis_size("ep")
    flat = routes.reshape(-1)
    hits = (flat[:, None] == jnp.arange(experts_all, dtype=jnp.int32)[None, :]).astype(jnp.int32)
    earlier = jnp.cumsum(hits, axis=0) - hits
    slot = jnp.sum(earlier * hits, axis=1)
    place = (flat * cap + slot).reshape(seqs, top)
    picker = jnp.any(
        jnp.arange(experts_all * cap, dtype=jnp.int32)[:, None, None] == place[None, :, :], axis=2
    ).astype(bf16)
    outbound = (
        jnp.dot(picker, ffn_in, preferred_element_type=f32)
        .astype(bf16)
        .reshape(experts_all, cap, width)
    )
    arrived = lax.all_to_all(outbound, "ep", split_axis=0, concat_axis=0, tiled=True)
    items = arrived.shape[1]
    rows = arrived.reshape(-1, local_experts, items, width)
    gate = jnp.einsum("secd,edf->secf", rows, expert_gate, preferred_element_type=f32)
    up = jnp.einsum("secd,edf->secf", rows, expert_up, preferred_element_type=f32)
    act = (jax.nn.silu(gate) * up).astype(bf16)
    part = jnp.einsum("secf,efd->secd", act, expert_down, preferred_element_type=f32).reshape(
        -1, items, width
    )
    summed = lax.psum_scatter(
        part.astype(jnp.bfloat16), "tp", scatter_dimension=2, tiled=True
    ).astype(jnp.float32)
    done = summed.astype(bf16)
    returned = lax.all_to_all(done, "ep", split_axis=0, concat_axis=0, tiled=True)
    columns = returned.shape[2]
    chosen = jnp.take(returned.reshape(-1, columns), place.reshape(-1), axis=0).reshape(
        seqs, top, columns
    )
    return jnp.sum(route_weights[:, :, None] * chosen.astype(f32), axis=1)


def solution(mesh):
    return jax.shard_map(
        per_device,
        mesh=mesh,
        in_specs=(
            P("ep", None),
            P("ep", "tp", None, None),
            P("ep", "tp"),
            P(),
            P(None, "tp"),
            P(None, "tp"),
            P(None, "tp"),
            P(None, "tp"),
            P(None, "tp"),
            P("tp"),
            P("tp"),
            P("tp"),
            P("tp", None),
            P(),
            P(),
            P("ep", None),
            P("ep", None),
            P("ep", None, "tp"),
            P("ep", None, "tp"),
            P("ep", "tp", None),
            P("tp"),
        ),
        out_specs=P("ep", "tp"),
        check_vma=False,
    )
```

```python
import jax
import jax.numpy as jnp
from jax import lax
from jax.experimental import pallas as pl
from jax.experimental.pallas import tpu as pltpu
from jax.sharding import PartitionSpec as P


EPS = 1e-06


def rms_scale(values):
    return lax.rsqrt(jnp.mean(values * values, axis=-1, keepdims=True) + EPS)


def per_device(
    tokens,
    memory,
    log_scale,
    mix_gain_in,
    w_query,
    w_key,
    w_value,
    w_igate,
    w_fgate,
    igate_bias,
    fgate_bias,
    head_gain,
    w_output,
    mix_gain_out,
    ffn_gain_in,
    routes,
    route_weights,
    expert_gate,
    expert_up,
    expert_down,
    ffn_gain_out,
):
    f32 = jnp.float32
    bf16 = jnp.bfloat16
    seqs, width = tokens.shape
    lanes = lax.axis_size("tp")
    groups = lax.axis_size("ep")
    local_experts = expert_gate.shape[0]
    experts_all = local_experts * groups
    top = routes.shape[1]
    cap = min(seqs, max(2, 3 * seqs * top // (2 * experts_all)))
    dense = cap == seqs and local_experts == 1 and lanes == 4 and seqs % 16 == 0
    partial_value = cell(
        tokens,
        memory,
        log_scale,
        mix_gain_in,
        w_query,
        w_key,
        w_value,
        w_igate,
        w_fgate,
        igate_bias,
        fgate_bias,
        head_gain,
        w_output,
        dense,
    )
    if dense:
        return every_token(
            partial_value,
            tokens,
            mix_gain_out,
            ffn_gain_in,
            routes,
            route_weights,
            expert_gate,
            expert_up,
            expert_down,
            ffn_gain_out,
        )
    quarter = width // lanes
    own = lax.axis_index("tp") * quarter
    mixed = sum_over(partial_value, "tp")
    resid = (tokens.astype(f32) + mixed * rms_scale(mixed) * mix_gain_out).astype(bf16)
    rf = resid.astype(f32)
    ffn_in = (rf * rms_scale(rf) * ffn_gain_in).astype(bf16)
    routed = slotted(ffn_in, routes, route_weights, expert_gate, expert_up, expert_down, cap)
    resid_part = lax.dynamic_slice_in_dim(rf, own, quarter, 1)
    total = sum_over(jnp.sum(routed * routed, axis=1), "tp")
    scaled = routed * lax.rsqrt(total / width + EPS)[:, None]
    return (resid_part + scaled * ffn_gain_out).astype(bf16)


def exchange(value, axis, step):
    size = lax.axis_size(axis)
    if size & (size - 1) == 0:
        pairs = [(i, i ^ step) for i in range(size)]
    else:
        pairs = [(i, (i + step) % size) for i in range(size)]
    return lax.ppermute(value, axis, pairs)


def sum_over(value, axis):
    total = value.astype(jnp.float32)
    for step in range(1, lax.axis_size(axis)):
        total = total + exchange(value, axis, step).astype(jnp.float32)
    return total


def whole():
    return pl.BlockSpec(memory_space=pltpu.VMEM)


def biases_body(heads, ib, fb, out):
    for h in range(heads):
        out[0:1, h : h + 1] = jnp.full((1, 1), ib[h], jnp.float32)
        out[1:2, h : h + 1] = jnp.full((1, 1), fb[h], jnp.float32)


def biases(igate_bias, fgate_bias):
    heads = igate_bias.shape[0]
    return pl.pallas_call(
        lambda *refs: biases_body(heads, *refs),
        out_shape=jax.ShapeDtypeStruct((2, heads), jnp.float32),
        in_specs=[pl.BlockSpec(memory_space=pltpu.SMEM)] * 2,
        out_specs=whole(),
        compiler_params=pltpu.CompilerParams(vmem_limit_bytes=1 << 20),
        cost_estimate=pl.CostEstimate(flops=11 * 10**8, transcendentals=0, bytes_accessed=4096),
        name="biases",
    )(igate_bias, fgate_bias)


def cell_body(heads, key_dim, value_dim, halves, *refs):
    f32 = jnp.float32
    bf16 = jnp.bfloat16
    (tokens, gain, wi, wf, bias, scale, wq, wk, wv, mem, hg, wo) = refs[:12]
    outs, recall = refs[12:-1], refs[-1]
    seqs = tokens.shape[0]
    xf = tokens[...].astype(f32)
    normed = (xf * rms_scale(xf) * gain[...]).astype(bf16)
    query = jnp.dot(normed, wq[...], preferred_element_type=f32) * key_dim ** (-0.5)
    wide = normed.astype(f32)
    diagonal = lax.broadcasted_iota(jnp.int32, (seqs, seqs), 0) == lax.broadcasted_iota(
        jnp.int32, (seqs, seqs), 1
    )
    carries, fresh = [], []
    for h in range(heads):
        in_pre = jnp.sum(wide * wi[h : h + 1, :].astype(f32), axis=1, keepdims=True) + bias[0:1, h : h + 1]
        forget = jnp.sum(wide * wf[h : h + 1, :].astype(f32), axis=1, keepdims=True) + bias[1:2, h : h + 1]
        forget_log = jnp.minimum(forget, 0.0) - jnp.log1p(jnp.exp(-jnp.abs(forget)))
        column = jnp.sum(jnp.where(diagonal, scale[h : h + 1, :], 0.0), axis=1, keepdims=True)
        carried = forget_log + column
        new_max = jnp.maximum(carried, in_pre)
        carries.append(jnp.exp(carried - new_max))
        fresh.append(jnp.exp(in_pre - new_max))
    keys = jnp.dot(normed, wk[...], preferred_element_type=f32)
    turned = [query[:, h * key_dim : (h + 1) * key_dim].T for h in range(heads)]
    for b in range(seqs):
        for h in range(heads):
            product = turned[h][:, b : b + 1] * mem[b, h]
            recall[h, b : b + 1, :] = jnp.sum(product, axis=0, keepdims=True)
    values = jnp.dot(normed, wv[...], preferred_element_type=f32)
    parts = []
    for h in range(heads):
        ks = slice(h * key_dim, (h + 1) * key_dim)
        vs = slice(h * value_dim, (h + 1) * value_dim)
        match = jnp.sum(query[:, ks] * keys[:, ks], axis=1, keepdims=True)
        read = carries[h] * recall[h] + (fresh[h] * match) * values[:, vs]
        inv = lax.rsqrt(jnp.mean(read * read, axis=1, keepdims=True) + EPS)
        parts.append((read * inv * hg[:, vs]).astype(bf16))
    headout = parts[0] if heads == 1 else jnp.concatenate(parts, axis=1)
    product = jnp.dot(headout, wo[...], preferred_element_type=f32)
    if halves:
        low, high = product[: seqs // 2], product[seqs // 2 :]
        odd = lax.axis_index("tp") % 2 == 1
        outs[0][...] = jnp.where(odd, high, low).astype(bf16)
        outs[1][...] = jnp.where(odd, low, high).astype(bf16)
    else:
        outs[0][...] = product.astype(bf16)


def cell(
    tokens,
    memory,
    log_scale,
    mix_gain_in,
    w_query,
    w_key,
    w_value,
    w_igate,
    w_fgate,
    igate_bias,
    fgate_bias,
    head_gain,
    w_output,
    halves,
):
    f32 = jnp.float32
    bf16 = jnp.bfloat16
    seqs, width = tokens.shape
    heads, key_dim, value_dim = memory.shape[1:]
    body = lambda *refs: cell_body(heads, key_dim, value_dim, halves, *refs)
    operands = [
        tokens,
        mix_gain_in.reshape(1, width),
        w_igate.T,
        w_fgate.T,
        biases(igate_bias, fgate_bias),
        log_scale.T,
        w_query,
        w_key,
        w_value,
        memory,
        head_gain.reshape(1, heads * value_dim),
        w_output,
    ]
    shape = jax.ShapeDtypeStruct((seqs // 2 if halves else seqs, w_output.shape[1]), bf16)
    result = pl.pallas_call(
        body,
        out_shape=[shape] * (2 if halves else 1),
        in_specs=[whole()] * len(operands),
        out_specs=[whole()] * (2 if halves else 1),
        scratch_shapes=[pltpu.VMEM((heads, seqs, value_dim), f32)],
        compiler_params=pltpu.CompilerParams(vmem_limit_bytes=12 << 20),
        name="cell",
    )(*operands)
    return result if halves else result[0]


def after_mix_body(parts, tokens, gain_out, gain_in, resid, spread):
    f32 = jnp.float32
    half = tokens.shape[0] // 2
    mixed = parts[0][...].astype(f32)
    for part in parts[1:]:
        mixed = mixed + part[...].astype(f32)
    odd = lax.axis_index("tp") % 2 == 1
    xf = tokens[...].astype(f32)
    xf = jnp.where(odd, xf[half:], xf[:half])
    kept = (xf + mixed * rms_scale(mixed) * gain_out[...]).astype(jnp.bfloat16)
    resid[...] = kept
    rf = kept.astype(f32)
    ffn_in = (rf * rms_scale(rf) * gain_in[...]).astype(jnp.bfloat16)
    for g in range(spread.shape[0]):
        spread[g] = ffn_in


def after_mix(parts, tokens, gain_out, gain_in, groups):
    seqs, width = tokens.shape
    count = len(parts)
    return pl.pallas_call(
        lambda *refs: after_mix_body(refs[:count], *refs[count:]),
        out_shape=(
            jax.ShapeDtypeStruct((seqs // 2, width), jnp.bfloat16),
            jax.ShapeDtypeStruct((groups, seqs // 2, width), jnp.bfloat16),
        ),
        in_specs=[whole()] * (count + 3),
        out_specs=(whole(), whole()),
        compiler_params=pltpu.CompilerParams(vmem_limit_bytes=8 << 20),
        name="after_mix",
    )(*parts, tokens, gain_out.reshape(1, width), gain_in.reshape(1, width))


def expert_body(rows, gate_w, up_w, down_w, gate_n, up_n, down_n, out):
    f32 = jnp.float32
    groups, half, width = rows.shape
    ffn_in = rows[...].reshape(groups * half, width)
    total = None
    for gates, ups, downs in ((gate_w, up_w, down_w), (gate_n, up_n, down_n)):
        gate = jnp.dot(ffn_in, gates[...], preferred_element_type=f32)
        up = jnp.dot(ffn_in, ups[...], preferred_element_type=f32)
        act = (gate * jax.nn.sigmoid(gate) * up).astype(jnp.bfloat16)
        part = jnp.dot(act, downs[...], preferred_element_type=f32)
        total = part if total is None else total + part
    out[...] = total.astype(jnp.bfloat16).reshape(groups, half, width)


def expert(rows, own, neighbour):
    return pl.pallas_call(
        expert_body,
        out_shape=jax.ShapeDtypeStruct(rows.shape, jnp.bfloat16),
        in_specs=[whole()] * 7,
        out_specs=whole(),
        compiler_params=pltpu.CompilerParams(vmem_limit_bytes=16 << 20),
        name="expert",
    )(rows, *own, *neighbour)


def share_body(back, weights, resid, share, both):
    f32 = jnp.float32
    groups, half, _ = back.shape
    odd = lax.axis_index("tp") % 2 == 1
    turned = weights[...].T
    mine = jnp.where(odd, turned[half:], turned[:half])
    total = mine[:, 0:1] * back[0].astype(f32)
    for e in range(1, groups):
        total = total + mine[:, e : e + 1] * back[e].astype(f32)
    rounded = total.astype(jnp.bfloat16)
    share[...] = rounded
    both[0] = rounded
    both[1] = resid[...]


def combine(back, weights, resid):
    _, half, width = back.shape
    return pl.pallas_call(
        share_body,
        out_shape=(
            jax.ShapeDtypeStruct((half, width), jnp.bfloat16),
            jax.ShapeDtypeStruct((2, half, width), jnp.bfloat16),
        ),
        in_specs=[whole()] * 3,
        out_specs=(whole(), whole()),
        compiler_params=pltpu.CompilerParams(vmem_limit_bytes=8 << 20),
        name="share",
    )(back, weights, resid)


def last_body(share, both, other_y, other_far, resid, gain, out, picks):
    f32 = jnp.float32
    quarter = out.shape[1]
    kept = share[...].astype(f32) + other_y[...].astype(f32)
    other = both[0].astype(f32) + other_far[...].astype(f32)
    picks[0] = kept * rms_scale(kept)
    picks[1] = other * rms_scale(other)
    picks[2] = resid[...].astype(f32)
    picks[3] = both[1].astype(f32)
    lane = lax.axis_index("tp")
    odd = lane % 2 == 1
    places = pl.ds(pl.multiple_of(lane * quarter, quarter), quarter)
    mine = picks[2, :, places] + picks[0, :, places] * gain[...]
    theirs = picks[3, :, places] + picks[1, :, places] * gain[...]
    low, high = jnp.where(odd, theirs, mine), jnp.where(odd, mine, theirs)
    out[...] = jnp.concatenate([low, high], axis=0).astype(jnp.bfloat16)


def last(share, both, other_y, other_far, resid, gain):
    half, width = share.shape
    quarter = gain.shape[0]
    return pl.pallas_call(
        last_body,
        out_shape=jax.ShapeDtypeStruct((2 * half, quarter), jnp.bfloat16),
        in_specs=[whole()] * 6,
        out_specs=whole(),
        scratch_shapes=[pltpu.VMEM((4, half, width), jnp.float32)],
        compiler_params=pltpu.CompilerParams(vmem_limit_bytes=8 << 20),
        name="last",
    )(share, both, other_y, other_far, resid, gain.reshape(1, quarter))


def every_token(
    halves,
    tokens,
    mix_gain_out,
    ffn_gain_in,
    routes,
    route_weights,
    expert_gate,
    expert_up,
    expert_down,
    ffn_gain_out,
):
    groups = lax.axis_size("ep")
    mine, theirs = halves
    parts = [mine]
    for step in (2, 3, 1):
        parts.append(exchange(theirs if step % 2 else mine, "tp", step))
    shards = (expert_gate[0], expert_up[0], expert_down[0])
    *waited, _ = lax.optimization_barrier((*shards, mine))
    neighbour = [exchange(shard, "tp", 1) for shard in waited]
    resid, spread = after_mix(parts, tokens, mix_gain_out, ffn_gain_in, groups)
    named = routes[:, :, None] == jnp.arange(groups, dtype=jnp.int32)[None, None, :]
    weights = jnp.sum(jnp.where(named, route_weights[:, :, None], 0.0), axis=1).T
    spread, weights, gain_out = lax.optimization_barrier((spread, weights, ffn_gain_out))
    rows = lax.all_to_all(spread, "ep", split_axis=0, concat_axis=0, tiled=True)
    blocks = expert(rows, shards, neighbour)
    blocks, weights, resid, gain_out = lax.optimization_barrier((blocks, weights, resid, gain_out))
    back = lax.all_to_all(blocks, "ep", split_axis=0, concat_axis=0, tiled=True)
    share, both = combine(back, weights, resid)
    sums = {}
    for step in (3, 2, 1):
        sums[step] = exchange(both if step == 1 else share, "tp", step)
    return last(share, sums[1], sums[2], sums[3], resid, gain_out)


def slotted(ffn_in, routes, route_weights, expert_gate, expert_up, expert_down, cap):
    f32 = jnp.float32
    bf16 = jnp.bfloat16
    seqs, width = ffn_in.shape
    top = routes.shape[1]
    local_experts = expert_gate.shape[0]
    experts_all = local_experts * lax.axis_size("ep")
    flat = routes.reshape(-1)
    hits = (flat[:, None] == jnp.arange(experts_all, dtype=jnp.int32)[None, :]).astype(jnp.int32)
    earlier = jnp.cumsum(hits, axis=0) - hits
    slot = jnp.sum(earlier * hits, axis=1)
    place = (flat * cap + slot).reshape(seqs, top)
    picker = jnp.any(
        jnp.arange(experts_all * cap, dtype=jnp.int32)[:, None, None] == place[None, :, :], axis=2
    ).astype(bf16)
    outbound = (
        jnp.dot(picker, ffn_in, preferred_element_type=f32)
        .astype(bf16)
        .reshape(experts_all, cap, width)
    )
    arrived = lax.all_to_all(outbound, "ep", split_axis=0, concat_axis=0, tiled=True)
    items = arrived.shape[1]
    rows = arrived.reshape(-1, local_experts, items, width)
    gate = jnp.einsum("secd,edf->secf", rows, expert_gate, preferred_element_type=f32)
    up = jnp.einsum("secd,edf->secf", rows, expert_up, preferred_element_type=f32)
    act = (jax.nn.silu(gate) * up).astype(bf16)
    part = jnp.einsum("secf,efd->secd", act, expert_down, preferred_element_type=f32).reshape(
        -1, items, width
    )
    summed = lax.psum_scatter(
        part.astype(jnp.bfloat16), "tp", scatter_dimension=2, tiled=True
    ).astype(jnp.float32)
    done = summed.astype(bf16)
    returned = lax.all_to_all(done, "ep", split_axis=0, concat_axis=0, tiled=True)
    columns = returned.shape[2]
    chosen = jnp.take(returned.reshape(-1, columns), place.reshape(-1), axis=0).reshape(
        seqs, top, columns
    )
    return jnp.sum(route_weights[:, :, None] * chosen.astype(f32), axis=1)


def solution(mesh):
    return jax.shard_map(
        per_device,
        mesh=mesh,
        in_specs=(
            P("ep", None),
            P("ep", "tp", None, None),
            P("ep", "tp"),
            P(),
            P(None, "tp"),
            P(None, "tp"),
            P(None, "tp"),
            P(None, "tp"),
            P(None, "tp"),
            P("tp"),
            P("tp"),
            P("tp"),
            P("tp", None),
            P(),
            P(),
            P("ep", None),
            P("ep", None),
            P("ep", None, "tp"),
            P("ep", None, "tp"),
            P("ep", "tp", None),
            P("tp"),
        ),
        out_specs=P("ep", "tp"),
        check_vma=False,
    )
```

```python
import jax
import jax.numpy as jnp
from jax import lax
from jax.experimental import pallas as pl
from jax.experimental.pallas import tpu as pltpu
from jax.sharding import PartitionSpec as P


EPS = 1e-06


def rms_scale(values):
    return lax.rsqrt(jnp.mean(values * values, axis=-1, keepdims=True) + EPS)


def per_device(
    tokens,
    memory,
    log_scale,
    mix_gain_in,
    w_query,
    w_key,
    w_value,
    w_igate,
    w_fgate,
    igate_bias,
    fgate_bias,
    head_gain,
    w_output,
    mix_gain_out,
    ffn_gain_in,
    routes,
    route_weights,
    expert_gate,
    expert_up,
    expert_down,
    ffn_gain_out,
):
    f32 = jnp.float32
    bf16 = jnp.bfloat16
    seqs, width = tokens.shape
    lanes = lax.axis_size("tp")
    groups = lax.axis_size("ep")
    local_experts = expert_gate.shape[0]
    experts_all = local_experts * groups
    top = routes.shape[1]
    cap = min(seqs, max(2, 3 * seqs * top // (2 * experts_all)))
    paired = lanes % 2 == 0 and lanes & (lanes - 1) == 0 and seqs % 16 == 0
    dense = cap == seqs and local_experts == 1 and paired
    partial_value = cell(
        tokens,
        memory,
        log_scale,
        mix_gain_in,
        w_query,
        w_key,
        w_value,
        w_igate,
        w_fgate,
        igate_bias,
        fgate_bias,
        head_gain,
        w_output,
        dense,
    )
    if dense:
        return every_token(
            partial_value,
            tokens,
            mix_gain_out,
            ffn_gain_in,
            routes,
            route_weights,
            expert_gate,
            expert_up,
            expert_down,
            ffn_gain_out,
        )
    quarter = width // lanes
    own = lax.axis_index("tp") * quarter
    mixed = sum_over(partial_value, "tp")
    resid = (tokens.astype(f32) + mixed * rms_scale(mixed) * mix_gain_out).astype(bf16)
    rf = resid.astype(f32)
    ffn_in = (rf * rms_scale(rf) * ffn_gain_in).astype(bf16)
    routed = slotted(ffn_in, routes, route_weights, expert_gate, expert_up, expert_down, cap)
    resid_part = lax.dynamic_slice_in_dim(rf, own, quarter, 1)
    total = sum_over(jnp.sum(routed * routed, axis=1), "tp")
    scaled = routed * lax.rsqrt(total / width + EPS)[:, None]
    return (resid_part + scaled * ffn_gain_out).astype(bf16)


def exchange(value, axis, step):
    size = lax.axis_size(axis)
    if size & (size - 1) == 0:
        pairs = [(i, i ^ step) for i in range(size)]
    else:
        pairs = [(i, (i + step) % size) for i in range(size)]
    return lax.ppermute(value, axis, pairs)


def sum_over(value, axis):
    total = value.astype(jnp.float32)
    for step in range(1, lax.axis_size(axis)):
        total = total + exchange(value, axis, step).astype(jnp.float32)
    return total


def whole():
    return pl.BlockSpec(memory_space=pltpu.VMEM)


def biases_body(heads, ib, fb, out):
    for h in range(heads):
        out[0:1, h : h + 1] = jnp.full((1, 1), ib[h], jnp.float32)
        out[1:2, h : h + 1] = jnp.full((1, 1), fb[h], jnp.float32)


def biases(igate_bias, fgate_bias):
    heads = igate_bias.shape[0]
    return pl.pallas_call(
        lambda *refs: biases_body(heads, *refs),
        out_shape=jax.ShapeDtypeStruct((2, heads), jnp.float32),
        in_specs=[pl.BlockSpec(memory_space=pltpu.SMEM)] * 2,
        out_specs=whole(),
        compiler_params=pltpu.CompilerParams(vmem_limit_bytes=1 << 20),
        cost_estimate=pl.CostEstimate(flops=11 * 10**8, transcendentals=0, bytes_accessed=4096),
        name="biases",
    )(igate_bias, fgate_bias)


def cell_body(heads, key_dim, value_dim, halves, *refs):
    f32 = jnp.float32
    bf16 = jnp.bfloat16
    (tokens, gain, wi, wf, bias, scale, wq, wk, wv, mem, hg, wo) = refs[:12]
    outs, recall = refs[12:-1], refs[-1]
    seqs = tokens.shape[0]
    xf = tokens[...].astype(f32)
    normed = (xf * rms_scale(xf) * gain[...]).astype(bf16)
    query = jnp.dot(normed, wq[...], preferred_element_type=f32) * key_dim ** (-0.5)
    wide = normed.astype(f32)
    diagonal = lax.broadcasted_iota(jnp.int32, (seqs, seqs), 0) == lax.broadcasted_iota(
        jnp.int32, (seqs, seqs), 1
    )
    carries, fresh = [], []
    for h in range(heads):
        in_pre = jnp.sum(wide * wi[h : h + 1, :].astype(f32), axis=1, keepdims=True) + bias[0:1, h : h + 1]
        forget = jnp.sum(wide * wf[h : h + 1, :].astype(f32), axis=1, keepdims=True) + bias[1:2, h : h + 1]
        forget_log = jnp.minimum(forget, 0.0) - jnp.log1p(jnp.exp(-jnp.abs(forget)))
        column = jnp.sum(jnp.where(diagonal, scale[h : h + 1, :], 0.0), axis=1, keepdims=True)
        carried = forget_log + column
        new_max = jnp.maximum(carried, in_pre)
        carries.append(jnp.exp(carried - new_max))
        fresh.append(jnp.exp(in_pre - new_max))
    keys = jnp.dot(normed, wk[...], preferred_element_type=f32)
    turned = [query[:, h * key_dim : (h + 1) * key_dim].T for h in range(heads)]
    for b in range(seqs):
        for h in range(heads):
            product = turned[h][:, b : b + 1] * mem[b, h]
            recall[h, b : b + 1, :] = jnp.sum(product, axis=0, keepdims=True)
    values = jnp.dot(normed, wv[...], preferred_element_type=f32)
    parts = []
    for h in range(heads):
        ks = slice(h * key_dim, (h + 1) * key_dim)
        vs = slice(h * value_dim, (h + 1) * value_dim)
        match = jnp.sum(query[:, ks] * keys[:, ks], axis=1, keepdims=True)
        read = carries[h] * recall[h] + (fresh[h] * match) * values[:, vs]
        inv = lax.rsqrt(jnp.mean(read * read, axis=1, keepdims=True) + EPS)
        parts.append((read * inv * hg[:, vs]).astype(bf16))
    headout = parts[0] if heads == 1 else jnp.concatenate(parts, axis=1)
    product = jnp.dot(headout, wo[...], preferred_element_type=f32)
    if halves:
        low, high = product[: seqs // 2], product[seqs // 2 :]
        odd = lax.axis_index("tp") % 2 == 1
        outs[0][...] = jnp.where(odd, high, low).astype(bf16)
        outs[1][...] = jnp.where(odd, low, high).astype(bf16)
    else:
        outs[0][...] = product.astype(bf16)


def cell(
    tokens,
    memory,
    log_scale,
    mix_gain_in,
    w_query,
    w_key,
    w_value,
    w_igate,
    w_fgate,
    igate_bias,
    fgate_bias,
    head_gain,
    w_output,
    halves,
):
    f32 = jnp.float32
    bf16 = jnp.bfloat16
    seqs, width = tokens.shape
    heads, key_dim, value_dim = memory.shape[1:]
    body = lambda *refs: cell_body(heads, key_dim, value_dim, halves, *refs)
    operands = [
        tokens,
        mix_gain_in.reshape(1, width),
        w_igate.T,
        w_fgate.T,
        biases(igate_bias, fgate_bias),
        log_scale.T,
        w_query,
        w_key,
        w_value,
        memory,
        head_gain.reshape(1, heads * value_dim),
        w_output,
    ]
    shape = jax.ShapeDtypeStruct((seqs // 2 if halves else seqs, w_output.shape[1]), bf16)
    result = pl.pallas_call(
        body,
        out_shape=[shape] * (2 if halves else 1),
        in_specs=[whole()] * len(operands),
        out_specs=[whole()] * (2 if halves else 1),
        scratch_shapes=[pltpu.VMEM((heads, seqs, value_dim), f32)],
        compiler_params=pltpu.CompilerParams(vmem_limit_bytes=12 << 20),
        name="cell",
    )(*operands)
    return result if halves else result[0]


def after_mix_body(parts, tokens, gain_out, gain_in, resid, spread):
    f32 = jnp.float32
    half = tokens.shape[0] // 2
    mixed = parts[0][...].astype(f32)
    for part in parts[1:]:
        mixed = mixed + part[...].astype(f32)
    odd = lax.axis_index("tp") % 2 == 1
    xf = tokens[...].astype(f32)
    xf = jnp.where(odd, xf[half:], xf[:half])
    kept = (xf + mixed * rms_scale(mixed) * gain_out[...]).astype(jnp.bfloat16)
    resid[...] = kept
    rf = kept.astype(f32)
    ffn_in = (rf * rms_scale(rf) * gain_in[...]).astype(jnp.bfloat16)
    for g in range(spread.shape[0]):
        spread[g] = ffn_in


def after_mix(parts, tokens, gain_out, gain_in, groups):
    seqs, width = tokens.shape
    count = len(parts)
    return pl.pallas_call(
        lambda *refs: after_mix_body(refs[:count], *refs[count:]),
        out_shape=(
            jax.ShapeDtypeStruct((seqs // 2, width), jnp.bfloat16),
            jax.ShapeDtypeStruct((groups, seqs // 2, width), jnp.bfloat16),
        ),
        in_specs=[whole()] * (count + 3),
        out_specs=(whole(), whole()),
        compiler_params=pltpu.CompilerParams(vmem_limit_bytes=8 << 20),
        name="after_mix",
    )(*parts, tokens, gain_out.reshape(1, width), gain_in.reshape(1, width))


def expert_body(rows, gate_w, up_w, down_w, gate_n, up_n, down_n, out):
    f32 = jnp.float32
    groups, half, width = rows.shape
    ffn_in = rows[...].reshape(groups * half, width)
    total = None
    for gates, ups, downs in ((gate_w, up_w, down_w), (gate_n, up_n, down_n)):
        gate = jnp.dot(ffn_in, gates[...], preferred_element_type=f32)
        up = jnp.dot(ffn_in, ups[...], preferred_element_type=f32)
        act = (gate * jax.nn.sigmoid(gate) * up).astype(jnp.bfloat16)
        part = jnp.dot(act, downs[...], preferred_element_type=f32)
        total = part if total is None else total + part
    out[...] = total.astype(jnp.bfloat16).reshape(groups, half, width)


def expert(rows, own, neighbour):
    return pl.pallas_call(
        expert_body,
        out_shape=jax.ShapeDtypeStruct(rows.shape, jnp.bfloat16),
        in_specs=[whole()] * 7,
        out_specs=whole(),
        compiler_params=pltpu.CompilerParams(vmem_limit_bytes=16 << 20),
        name="expert",
    )(rows, *own, *neighbour)


def share_body(back, weights, resid, share, both):
    f32 = jnp.float32
    groups, half, _ = back.shape
    odd = lax.axis_index("tp") % 2 == 1
    turned = weights[...].T
    mine = jnp.where(odd, turned[half:], turned[:half])
    total = mine[:, 0:1] * back[0].astype(f32)
    for e in range(1, groups):
        total = total + mine[:, e : e + 1] * back[e].astype(f32)
    rounded = total.astype(jnp.bfloat16)
    share[...] = rounded
    both[0] = rounded
    both[1] = resid[...]


def combine(back, weights, resid):
    _, half, width = back.shape
    return pl.pallas_call(
        share_body,
        out_shape=(
            jax.ShapeDtypeStruct((half, width), jnp.bfloat16),
            jax.ShapeDtypeStruct((2, half, width), jnp.bfloat16),
        ),
        in_specs=[whole()] * 3,
        out_specs=(whole(), whole()),
        compiler_params=pltpu.CompilerParams(vmem_limit_bytes=8 << 20),
        name="share",
    )(back, weights, resid)


def last_body(count, *refs):
    f32 = jnp.float32
    sames, others = refs[:count], refs[count : 2 * count - 1]
    both, resid, gain, out, picks = refs[2 * count - 1 :]
    quarter = out.shape[1]
    kept = sames[0][...].astype(f32)
    for part in sames[1:]:
        kept = kept + part[...].astype(f32)
    other = both[0].astype(f32)
    for part in others:
        other = other + part[...].astype(f32)
    picks[0] = kept * rms_scale(kept)
    picks[1] = other * rms_scale(other)
    picks[2] = resid[...].astype(f32)
    picks[3] = both[1].astype(f32)
    lane = lax.axis_index("tp")
    odd = lane % 2 == 1
    places = pl.ds(pl.multiple_of(lane * quarter, quarter), quarter)
    mine = picks[2, :, places] + picks[0, :, places] * gain[...]
    theirs = picks[3, :, places] + picks[1, :, places] * gain[...]
    low, high = jnp.where(odd, theirs, mine), jnp.where(odd, mine, theirs)
    out[...] = jnp.concatenate([low, high], axis=0).astype(jnp.bfloat16)


def last(same, both, other, resid, gain):
    half, width = resid.shape
    quarter = gain.shape[0]
    operands = [*same, *other, both, resid, gain.reshape(1, quarter)]
    return pl.pallas_call(
        lambda *refs: last_body(len(same), *refs),
        out_shape=jax.ShapeDtypeStruct((2 * half, quarter), jnp.bfloat16),
        in_specs=[whole()] * len(operands),
        out_specs=whole(),
        scratch_shapes=[pltpu.VMEM((4, half, width), jnp.float32)],
        compiler_params=pltpu.CompilerParams(vmem_limit_bytes=8 << 20),
        name="last",
    )(*operands)


def odds_first(lanes):
    return [*range(3, lanes, 2), *range(2, lanes, 2), 1]


def every_token(
    halves,
    tokens,
    mix_gain_out,
    ffn_gain_in,
    routes,
    route_weights,
    expert_gate,
    expert_up,
    expert_down,
    ffn_gain_out,
):
    groups = lax.axis_size("ep")
    lanes = lax.axis_size("tp")
    mine, theirs = halves
    parts = [mine]
    for step in odds_first(lanes):
        parts.append(exchange(theirs if step % 2 else mine, "tp", step))
    shards = (expert_gate[0], expert_up[0], expert_down[0])
    *waited, _ = lax.optimization_barrier((*shards, mine))
    neighbour = [exchange(shard, "tp", 1) for shard in waited]
    resid, spread = after_mix(parts, tokens, mix_gain_out, ffn_gain_in, groups)
    named = routes[:, :, None] == jnp.arange(groups, dtype=jnp.int32)[None, None, :]
    weights = jnp.sum(jnp.where(named, route_weights[:, :, None], 0.0), axis=1).T
    spread, weights, gain_out = lax.optimization_barrier((spread, weights, ffn_gain_out))
    rows = lax.all_to_all(spread, "ep", split_axis=0, concat_axis=0, tiled=True)
    blocks = expert(rows, shards, neighbour)
    blocks, weights, resid, gain_out = lax.optimization_barrier((blocks, weights, resid, gain_out))
    back = lax.all_to_all(blocks, "ep", split_axis=0, concat_axis=0, tiled=True)
    share, both = combine(back, weights, resid)
    sums = {}
    for step in odds_first(lanes):
        sums[step] = exchange(both if step == 1 else share, "tp", step)
    same = [share] + [sums[step] for step in range(2, lanes, 2)]
    other = [sums[step] for step in range(3, lanes, 2)]
    return last(same, sums[1], other, resid, gain_out)


def slotted(ffn_in, routes, route_weights, expert_gate, expert_up, expert_down, cap):
    f32 = jnp.float32
    bf16 = jnp.bfloat16
    seqs, width = ffn_in.shape
    top = routes.shape[1]
    local_experts = expert_gate.shape[0]
    experts_all = local_experts * lax.axis_size("ep")
    flat = routes.reshape(-1)
    hits = (flat[:, None] == jnp.arange(experts_all, dtype=jnp.int32)[None, :]).astype(jnp.int32)
    earlier = jnp.cumsum(hits, axis=0) - hits
    slot = jnp.sum(earlier * hits, axis=1)
    place = (flat * cap + slot).reshape(seqs, top)
    picker = jnp.any(
        jnp.arange(experts_all * cap, dtype=jnp.int32)[:, None, None] == place[None, :, :], axis=2
    ).astype(bf16)
    outbound = (
        jnp.dot(picker, ffn_in, preferred_element_type=f32)
        .astype(bf16)
        .reshape(experts_all, cap, width)
    )
    arrived = lax.all_to_all(outbound, "ep", split_axis=0, concat_axis=0, tiled=True)
    items = arrived.shape[1]
    rows = arrived.reshape(-1, local_experts, items, width)
    gate = jnp.einsum("secd,edf->secf", rows, expert_gate, preferred_element_type=f32)
    up = jnp.einsum("secd,edf->secf", rows, expert_up, preferred_element_type=f32)
    act = (jax.nn.silu(gate) * up).astype(bf16)
    part = jnp.einsum("secf,efd->secd", act, expert_down, preferred_element_type=f32).reshape(
        -1, items, width
    )
    summed = lax.psum_scatter(
        part.astype(jnp.bfloat16), "tp", scatter_dimension=2, tiled=True
    ).astype(jnp.float32)
    done = summed.astype(bf16)
    returned = lax.all_to_all(done, "ep", split_axis=0, concat_axis=0, tiled=True)
    columns = returned.shape[2]
    chosen = jnp.take(returned.reshape(-1, columns), place.reshape(-1), axis=0).reshape(
        seqs, top, columns
    )
    return jnp.sum(route_weights[:, :, None] * chosen.astype(f32), axis=1)


def solution(mesh):
    return jax.shard_map(
        per_device,
        mesh=mesh,
        in_specs=(
            P("ep", None),
            P("ep", "tp", None, None),
            P("ep", "tp"),
            P(),
            P(None, "tp"),
            P(None, "tp"),
            P(None, "tp"),
            P(None, "tp"),
            P(None, "tp"),
            P("tp"),
            P("tp"),
            P("tp"),
            P("tp", None),
            P(),
            P(),
            P("ep", None),
            P("ep", None),
            P("ep", None, "tp"),
            P("ep", None, "tp"),
            P("ep", "tp", None),
            P("tp"),
        ),
        out_specs=P("ep", "tp"),
        check_vma=False,
    )
```

```python
import jax
import jax.numpy as jnp
from jax import lax
from jax.experimental import pallas as pl
from jax.experimental.pallas import tpu as pltpu
from jax.sharding import PartitionSpec as P


EPS = 1e-06


def rms_scale(values):
    return lax.rsqrt(jnp.mean(values * values, axis=-1, keepdims=True) + EPS)


def per_device(
    tokens,
    memory,
    log_scale,
    mix_gain_in,
    w_query,
    w_key,
    w_value,
    w_igate,
    w_fgate,
    igate_bias,
    fgate_bias,
    head_gain,
    w_output,
    mix_gain_out,
    ffn_gain_in,
    routes,
    route_weights,
    expert_gate,
    expert_up,
    expert_down,
    ffn_gain_out,
):
    f32 = jnp.float32
    bf16 = jnp.bfloat16
    seqs, width = tokens.shape
    lanes = lax.axis_size("tp")
    groups = lax.axis_size("ep")
    local_experts = expert_gate.shape[0]
    experts_all = local_experts * groups
    top = routes.shape[1]
    cap = min(seqs, max(2, 3 * seqs * top // (2 * experts_all)))
    paired = lanes % 2 == 0 and lanes & (lanes - 1) == 0 and seqs % 16 == 0
    dense = cap == seqs and local_experts == 1 and paired
    partial_value = cell(
        tokens,
        memory,
        log_scale,
        mix_gain_in,
        w_query,
        w_key,
        w_value,
        w_igate,
        w_fgate,
        igate_bias,
        fgate_bias,
        head_gain,
        w_output,
        dense,
    )
    if dense:
        return every_token(
            partial_value,
            tokens,
            mix_gain_out,
            ffn_gain_in,
            routes,
            route_weights,
            expert_gate,
            expert_up,
            expert_down,
            ffn_gain_out,
        )
    quarter = width // lanes
    own = lax.axis_index("tp") * quarter
    mixed = sum_over(partial_value, "tp")
    resid = (tokens.astype(f32) + mixed * rms_scale(mixed) * mix_gain_out).astype(bf16)
    rf = resid.astype(f32)
    ffn_in = (rf * rms_scale(rf) * ffn_gain_in).astype(bf16)
    routed = slotted(ffn_in, routes, route_weights, expert_gate, expert_up, expert_down, cap)
    resid_part = lax.dynamic_slice_in_dim(rf, own, quarter, 1)
    total = sum_over(jnp.sum(routed * routed, axis=1), "tp")
    scaled = routed * lax.rsqrt(total / width + EPS)[:, None]
    return (resid_part + scaled * ffn_gain_out).astype(bf16)


def exchange(value, axis, step):
    size = lax.axis_size(axis)
    if size & (size - 1) == 0:
        pairs = [(i, i ^ step) for i in range(size)]
    else:
        pairs = [(i, (i + step) % size) for i in range(size)]
    return lax.ppermute(value, axis, pairs)


def sum_over(value, axis):
    total = value.astype(jnp.float32)
    for step in range(1, lax.axis_size(axis)):
        total = total + exchange(value, axis, step).astype(jnp.float32)
    return total


def whole():
    return pl.BlockSpec(memory_space=pltpu.VMEM)


def biases_body(heads, ib, fb, out):
    for h in range(heads):
        out[0:1, h : h + 1] = jnp.full((1, 1), ib[h], jnp.float32)
        out[1:2, h : h + 1] = jnp.full((1, 1), fb[h], jnp.float32)


def biases(igate_bias, fgate_bias):
    heads = igate_bias.shape[0]
    return pl.pallas_call(
        lambda *refs: biases_body(heads, *refs),
        out_shape=jax.ShapeDtypeStruct((2, heads), jnp.float32),
        in_specs=[pl.BlockSpec(memory_space=pltpu.SMEM)] * 2,
        out_specs=whole(),
        compiler_params=pltpu.CompilerParams(vmem_limit_bytes=1 << 20),
        cost_estimate=pl.CostEstimate(flops=8 * 10**8, transcendentals=0, bytes_accessed=4096),
        name="biases",
    )(igate_bias, fgate_bias)


def cell_body(heads, key_dim, value_dim, halves, *refs):
    f32 = jnp.float32
    bf16 = jnp.bfloat16
    (tokens, gain, wi, wf, bias, scale, wq, wk, wv_h, mem, hg, wo_h) = refs[:12]
    outs, (recall, wv, wo, sems) = refs[12:-4], refs[-4:]
    value_copy = pltpu.make_async_copy(wv_h, wv, sems.at[0])
    output_copy = pltpu.make_async_copy(wo_h, wo, sems.at[1])
    value_copy.start()
    output_copy.start()
    seqs = tokens.shape[0]
    xf = tokens[...].astype(f32)
    normed = (xf * rms_scale(xf) * gain[...]).astype(bf16)
    query = jnp.dot(normed, wq[...], preferred_element_type=f32) * key_dim ** (-0.5)
    wide = normed.astype(f32)
    diagonal = lax.broadcasted_iota(jnp.int32, (seqs, seqs), 0) == lax.broadcasted_iota(
        jnp.int32, (seqs, seqs), 1
    )
    carries, fresh = [], []
    for h in range(heads):
        in_pre = jnp.sum(wide * wi[h : h + 1, :].astype(f32), axis=1, keepdims=True) + bias[0:1, h : h + 1]
        forget = jnp.sum(wide * wf[h : h + 1, :].astype(f32), axis=1, keepdims=True) + bias[1:2, h : h + 1]
        forget_log = jnp.minimum(forget, 0.0) - jnp.log1p(jnp.exp(-jnp.abs(forget)))
        column = jnp.sum(jnp.where(diagonal, scale[h : h + 1, :], 0.0), axis=1, keepdims=True)
        carried = forget_log + column
        new_max = jnp.maximum(carried, in_pre)
        carries.append(jnp.exp(carried - new_max))
        fresh.append(jnp.exp(in_pre - new_max))
    keys = jnp.dot(normed, wk[...], preferred_element_type=f32)
    turned = [query[:, h * key_dim : (h + 1) * key_dim].T for h in range(heads)]
    for b in range(seqs):
        for h in range(heads):
            product = turned[h][:, b : b + 1] * mem[b, h]
            recall[h, b : b + 1, :] = jnp.sum(product, axis=0, keepdims=True)
    value_copy.wait()
    values = jnp.dot(normed, wv[...], preferred_element_type=f32)
    parts = []
    for h in range(heads):
        ks = slice(h * key_dim, (h + 1) * key_dim)
        vs = slice(h * value_dim, (h + 1) * value_dim)
        match = jnp.sum(query[:, ks] * keys[:, ks], axis=1, keepdims=True)
        read = carries[h] * recall[h] + (fresh[h] * match) * values[:, vs]
        inv = lax.rsqrt(jnp.mean(read * read, axis=1, keepdims=True) + EPS)
        parts.append((read * inv * hg[:, vs]).astype(bf16))
    output_copy.wait()
    headout = parts[0] if heads == 1 else jnp.concatenate(parts, axis=1)
    product = jnp.dot(headout, wo[...], preferred_element_type=f32)
    if halves:
        low, high = product[: seqs // 2], product[seqs // 2 :]
        odd = lax.axis_index("tp") % 2 == 1
        outs[0][...] = jnp.where(odd, high, low).astype(bf16)
        outs[1][...] = jnp.where(odd, low, high).astype(bf16)
    else:
        outs[0][...] = product.astype(bf16)


def cell(
    tokens,
    memory,
    log_scale,
    mix_gain_in,
    w_query,
    w_key,
    w_value,
    w_igate,
    w_fgate,
    igate_bias,
    fgate_bias,
    head_gain,
    w_output,
    halves,
):
    f32 = jnp.float32
    bf16 = jnp.bfloat16
    seqs, width = tokens.shape
    heads, key_dim, value_dim = memory.shape[1:]
    hbm = pl.BlockSpec(memory_space=pltpu.HBM)
    body = lambda *refs: cell_body(heads, key_dim, value_dim, halves, *refs)
    operands = [
        tokens,
        mix_gain_in.reshape(1, width),
        w_igate.T,
        w_fgate.T,
        biases(igate_bias, fgate_bias),
        log_scale.T,
        w_query,
        w_key,
        w_value,
        memory,
        head_gain.reshape(1, heads * value_dim),
        w_output,
    ]
    shape = jax.ShapeDtypeStruct((seqs // 2 if halves else seqs, w_output.shape[1]), bf16)
    late = (8, 11)
    for i in late:
        operands[i] = pltpu.with_memory_space_constraint(operands[i], pltpu.HBM)
    result = pl.pallas_call(
        body,
        out_shape=[shape] * (2 if halves else 1),
        in_specs=[hbm if i in late else whole() for i in range(len(operands))],
        out_specs=[whole()] * (2 if halves else 1),
        scratch_shapes=[
            pltpu.VMEM((heads, seqs, value_dim), f32),
            pltpu.VMEM(w_value.shape, w_value.dtype),
            pltpu.VMEM(w_output.shape, w_output.dtype),
            pltpu.SemaphoreType.DMA((2,)),
        ],
        compiler_params=pltpu.CompilerParams(vmem_limit_bytes=12 << 20),
        name="cell",
    )(*operands)
    return result if halves else result[0]


def after_mix_body(parts, tokens, gain_out, gain_in, resid, spread):
    f32 = jnp.float32
    half = tokens.shape[0] // 2
    mixed = parts[0][...].astype(f32)
    for part in parts[1:]:
        mixed = mixed + part[...].astype(f32)
    odd = lax.axis_index("tp") % 2 == 1
    xf = tokens[...].astype(f32)
    xf = jnp.where(odd, xf[half:], xf[:half])
    kept = (xf + mixed * rms_scale(mixed) * gain_out[...]).astype(jnp.bfloat16)
    resid[...] = kept
    rf = kept.astype(f32)
    ffn_in = (rf * rms_scale(rf) * gain_in[...]).astype(jnp.bfloat16)
    for g in range(spread.shape[0]):
        spread[g] = ffn_in


def after_mix(parts, tokens, gain_out, gain_in, groups):
    seqs, width = tokens.shape
    count = len(parts)
    return pl.pallas_call(
        lambda *refs: after_mix_body(refs[:count], *refs[count:]),
        out_shape=(
            jax.ShapeDtypeStruct((seqs // 2, width), jnp.bfloat16),
            jax.ShapeDtypeStruct((groups, seqs // 2, width), jnp.bfloat16),
        ),
        in_specs=[whole()] * (count + 3),
        out_specs=(whole(), whole()),
        compiler_params=pltpu.CompilerParams(vmem_limit_bytes=8 << 20),
        name="after_mix",
    )(*parts, tokens, gain_out.reshape(1, width), gain_in.reshape(1, width))


def expert_body(rows, gate_w, up_w, down_w, gate_n, up_n, down_n, out):
    f32 = jnp.float32
    groups, half, width = rows.shape
    ffn_in = rows[...].reshape(groups * half, width)
    total = None
    for gates, ups, downs in ((gate_w, up_w, down_w), (gate_n, up_n, down_n)):
        gate = jnp.dot(ffn_in, gates[...], preferred_element_type=f32)
        up = jnp.dot(ffn_in, ups[...], preferred_element_type=f32)
        act = (gate * jax.nn.sigmoid(gate) * up).astype(jnp.bfloat16)
        part = jnp.dot(act, downs[...], preferred_element_type=f32)
        total = part if total is None else total + part
    out[...] = total.astype(jnp.bfloat16).reshape(groups, half, width)


def expert(rows, own, neighbour):
    return pl.pallas_call(
        expert_body,
        out_shape=jax.ShapeDtypeStruct(rows.shape, jnp.bfloat16),
        in_specs=[whole()] * 7,
        out_specs=whole(),
        compiler_params=pltpu.CompilerParams(vmem_limit_bytes=16 << 20),
        name="expert",
    )(rows, *own, *neighbour)


def share_body(back, weights, resid, share, both):
    f32 = jnp.float32
    groups, half, _ = back.shape
    odd = lax.axis_index("tp") % 2 == 1
    turned = weights[...].T
    mine = jnp.where(odd, turned[half:], turned[:half])
    total = mine[:, 0:1] * back[0].astype(f32)
    for e in range(1, groups):
        total = total + mine[:, e : e + 1] * back[e].astype(f32)
    rounded = total.astype(jnp.bfloat16)
    share[...] = rounded
    both[0] = rounded
    both[1] = resid[...]


def combine(back, weights, resid):
    _, half, width = back.shape
    return pl.pallas_call(
        share_body,
        out_shape=(
            jax.ShapeDtypeStruct((half, width), jnp.bfloat16),
            jax.ShapeDtypeStruct((2, half, width), jnp.bfloat16),
        ),
        in_specs=[whole()] * 3,
        out_specs=(whole(), whole()),
        compiler_params=pltpu.CompilerParams(vmem_limit_bytes=8 << 20),
        name="share",
    )(back, weights, resid)


def last_body(count, *refs):
    f32 = jnp.float32
    sames, others = refs[:count], refs[count : 2 * count - 1]
    both, resid, gain, out, picks = refs[2 * count - 1 :]
    quarter = out.shape[1]
    kept = sames[0][...].astype(f32)
    for part in sames[1:]:
        kept = kept + part[...].astype(f32)
    other = both[0].astype(f32)
    for part in others:
        other = other + part[...].astype(f32)
    picks[0] = kept * rms_scale(kept)
    picks[1] = other * rms_scale(other)
    picks[2] = resid[...].astype(f32)
    picks[3] = both[1].astype(f32)
    lane = lax.axis_index("tp")
    odd = lane % 2 == 1
    places = pl.ds(pl.multiple_of(lane * quarter, quarter), quarter)
    mine = picks[2, :, places] + picks[0, :, places] * gain[...]
    theirs = picks[3, :, places] + picks[1, :, places] * gain[...]
    low, high = jnp.where(odd, theirs, mine), jnp.where(odd, mine, theirs)
    out[...] = jnp.concatenate([low, high], axis=0).astype(jnp.bfloat16)


def last(same, both, other, resid, gain):
    half, width = resid.shape
    quarter = gain.shape[0]
    operands = [*same, *other, both, resid, gain.reshape(1, quarter)]
    return pl.pallas_call(
        lambda *refs: last_body(len(same), *refs),
        out_shape=jax.ShapeDtypeStruct((2 * half, quarter), jnp.bfloat16),
        in_specs=[whole()] * len(operands),
        out_specs=whole(),
        scratch_shapes=[pltpu.VMEM((4, half, width), jnp.float32)],
        compiler_params=pltpu.CompilerParams(vmem_limit_bytes=8 << 20),
        name="last",
    )(*operands)


def odds_first(lanes):
    return [*range(3, lanes, 2), *range(2, lanes, 2), 1]


def every_token(
    halves,
    tokens,
    mix_gain_out,
    ffn_gain_in,
    routes,
    route_weights,
    expert_gate,
    expert_up,
    expert_down,
    ffn_gain_out,
):
    groups = lax.axis_size("ep")
    lanes = lax.axis_size("tp")
    mine, theirs = halves
    parts = [mine]
    for step in odds_first(lanes):
        parts.append(exchange(theirs if step % 2 else mine, "tp", step))
    shards = (expert_gate[0], expert_up[0], expert_down[0])
    *waited, _ = lax.optimization_barrier((*shards, mine))
    neighbour = [exchange(shard, "tp", 1) for shard in waited]
    resid, spread = after_mix(parts, tokens, mix_gain_out, ffn_gain_in, groups)
    named = routes[:, :, None] == jnp.arange(groups, dtype=jnp.int32)[None, None, :]
    weights = jnp.sum(jnp.where(named, route_weights[:, :, None], 0.0), axis=1).T
    spread, weights, gain_out = lax.optimization_barrier((spread, weights, ffn_gain_out))
    rows = lax.all_to_all(spread, "ep", split_axis=0, concat_axis=0, tiled=True)
    blocks = expert(rows, shards, neighbour)
    blocks, weights, resid, gain_out = lax.optimization_barrier((blocks, weights, resid, gain_out))
    back = lax.all_to_all(blocks, "ep", split_axis=0, concat_axis=0, tiled=True)
    share, both = combine(back, weights, resid)
    sums = {}
    for step in odds_first(lanes):
        sums[step] = exchange(both if step == 1 else share, "tp", step)
    same = [share] + [sums[step] for step in range(2, lanes, 2)]
    other = [sums[step] for step in range(3, lanes, 2)]
    return last(same, sums[1], other, resid, gain_out)


def slotted(ffn_in, routes, route_weights, expert_gate, expert_up, expert_down, cap):
    f32 = jnp.float32
    bf16 = jnp.bfloat16
    seqs, width = ffn_in.shape
    top = routes.shape[1]
    local_experts = expert_gate.shape[0]
    experts_all = local_experts * lax.axis_size("ep")
    flat = routes.reshape(-1)
    hits = (flat[:, None] == jnp.arange(experts_all, dtype=jnp.int32)[None, :]).astype(jnp.int32)
    earlier = jnp.cumsum(hits, axis=0) - hits
    slot = jnp.sum(earlier * hits, axis=1)
    place = (flat * cap + slot).reshape(seqs, top)
    picker = jnp.any(
        jnp.arange(experts_all * cap, dtype=jnp.int32)[:, None, None] == place[None, :, :], axis=2
    ).astype(bf16)
    outbound = (
        jnp.dot(picker, ffn_in, preferred_element_type=f32)
        .astype(bf16)
        .reshape(experts_all, cap, width)
    )
    arrived = lax.all_to_all(outbound, "ep", split_axis=0, concat_axis=0, tiled=True)
    items = arrived.shape[1]
    rows = arrived.reshape(-1, local_experts, items, width)
    gate = jnp.einsum("secd,edf->secf", rows, expert_gate, preferred_element_type=f32)
    up = jnp.einsum("secd,edf->secf", rows, expert_up, preferred_element_type=f32)
    act = (jax.nn.silu(gate) * up).astype(bf16)
    part = jnp.einsum("secf,efd->secd", act, expert_down, preferred_element_type=f32).reshape(
        -1, items, width
    )
    summed = lax.psum_scatter(
        part.astype(jnp.bfloat16), "tp", scatter_dimension=2, tiled=True
    ).astype(jnp.float32)
    done = summed.astype(bf16)
    returned = lax.all_to_all(done, "ep", split_axis=0, concat_axis=0, tiled=True)
    columns = returned.shape[2]
    chosen = jnp.take(returned.reshape(-1, columns), place.reshape(-1), axis=0).reshape(
        seqs, top, columns
    )
    return jnp.sum(route_weights[:, :, None] * chosen.astype(f32), axis=1)


def solution(mesh):
    return jax.shard_map(
        per_device,
        mesh=mesh,
        in_specs=(
            P("ep", None),
            P("ep", "tp", None, None),
            P("ep", "tp"),
            P(),
            P(None, "tp"),
            P(None, "tp"),
            P(None, "tp"),
            P(None, "tp"),
            P(None, "tp"),
            P("tp"),
            P("tp"),
            P("tp"),
            P("tp", None),
            P(),
            P(),
            P("ep", None),
            P("ep", None),
            P("ep", None, "tp"),
            P("ep", None, "tp"),
            P("ep", "tp", None),
            P("tp"),
        ),
        out_specs=P("ep", "tp"),
        check_vma=False,
    )
```

```python
import jax
import jax.numpy as jnp
from jax import lax
from jax.experimental import pallas as pl
from jax.experimental.pallas import tpu as pltpu
from jax.sharding import PartitionSpec as P


EPS = 1e-06


def rms_scale(values):
    return lax.rsqrt(jnp.mean(values * values, axis=-1, keepdims=True) + EPS)


def per_device(
    tokens,
    memory,
    log_scale,
    mix_gain_in,
    w_query,
    w_key,
    w_value,
    w_igate,
    w_fgate,
    igate_bias,
    fgate_bias,
    head_gain,
    w_output,
    mix_gain_out,
    ffn_gain_in,
    routes,
    route_weights,
    expert_gate,
    expert_up,
    expert_down,
    ffn_gain_out,
):
    f32 = jnp.float32
    bf16 = jnp.bfloat16
    seqs, width = tokens.shape
    lanes = lax.axis_size("tp")
    groups = lax.axis_size("ep")
    local_experts = expert_gate.shape[0]
    experts_all = local_experts * groups
    top = routes.shape[1]
    cap = min(seqs, max(2, 3 * seqs * top // (2 * experts_all)))
    paired = lanes % 2 == 0 and lanes & (lanes - 1) == 0 and seqs % 16 == 0
    dense = cap == seqs and local_experts == 1 and paired
    partial_value = cell(
        tokens,
        memory,
        log_scale,
        mix_gain_in,
        w_query,
        w_key,
        w_value,
        w_igate,
        w_fgate,
        igate_bias,
        fgate_bias,
        head_gain,
        w_output,
        dense,
    )
    if dense:
        return every_token(
            partial_value,
            tokens,
            mix_gain_out,
            ffn_gain_in,
            routes,
            route_weights,
            expert_gate,
            expert_up,
            expert_down,
            ffn_gain_out,
        )
    quarter = width // lanes
    own = lax.axis_index("tp") * quarter
    mixed = sum_over(partial_value, "tp")
    resid = (tokens.astype(f32) + mixed * rms_scale(mixed) * mix_gain_out).astype(bf16)
    rf = resid.astype(f32)
    ffn_in = (rf * rms_scale(rf) * ffn_gain_in).astype(bf16)
    routed = slotted(ffn_in, routes, route_weights, expert_gate, expert_up, expert_down, cap)
    resid_part = lax.dynamic_slice_in_dim(rf, own, quarter, 1)
    total = sum_over(jnp.sum(routed * routed, axis=1), "tp")
    scaled = routed * lax.rsqrt(total / width + EPS)[:, None]
    return (resid_part + scaled * ffn_gain_out).astype(bf16)


def exchange(value, axis, step):
    size = lax.axis_size(axis)
    if size & (size - 1) == 0:
        pairs = [(i, i ^ step) for i in range(size)]
    else:
        pairs = [(i, (i + step) % size) for i in range(size)]
    return lax.ppermute(value, axis, pairs)


def sum_over(value, axis):
    total = value.astype(jnp.float32)
    for step in range(1, lax.axis_size(axis)):
        total = total + exchange(value, axis, step).astype(jnp.float32)
    return total


def whole():
    return pl.BlockSpec(memory_space=pltpu.VMEM)


def biases_body(heads, ib, fb, out):
    for h in range(heads):
        out[0:1, h : h + 1] = jnp.full((1, 1), ib[h], jnp.float32)
        out[1:2, h : h + 1] = jnp.full((1, 1), fb[h], jnp.float32)


def biases(igate_bias, fgate_bias):
    heads = igate_bias.shape[0]
    return pl.pallas_call(
        lambda *refs: biases_body(heads, *refs),
        out_shape=jax.ShapeDtypeStruct((2, heads), jnp.float32),
        in_specs=[pl.BlockSpec(memory_space=pltpu.SMEM)] * 2,
        out_specs=whole(),
        compiler_params=pltpu.CompilerParams(vmem_limit_bytes=1 << 20),
        cost_estimate=pl.CostEstimate(flops=11 * 10**8, transcendentals=0, bytes_accessed=4096),
        name="biases",
    )(igate_bias, fgate_bias)


def cell_body(heads, key_dim, value_dim, halves, *refs):
    f32 = jnp.float32
    bf16 = jnp.bfloat16
    (tokens, gain, wi, wf, bias, scale, wq, wk, wv, mem, hg, wo) = refs[:12]
    outs, recall = refs[12:-1], refs[-1]
    seqs = tokens.shape[0]
    xf = tokens[...].astype(f32)
    normed = (xf * rms_scale(xf) * gain[...]).astype(bf16)
    query = jnp.dot(normed, wq[...], preferred_element_type=f32) * key_dim ** (-0.5)
    wide = normed.astype(f32)
    diagonal = lax.broadcasted_iota(jnp.int32, (seqs, seqs), 0) == lax.broadcasted_iota(
        jnp.int32, (seqs, seqs), 1
    )
    carries, fresh = [], []
    for h in range(heads):
        in_pre = jnp.sum(wide * wi[h : h + 1, :].astype(f32), axis=1, keepdims=True) + bias[0:1, h : h + 1]
        forget = jnp.sum(wide * wf[h : h + 1, :].astype(f32), axis=1, keepdims=True) + bias[1:2, h : h + 1]
        forget_log = jnp.minimum(forget, 0.0) - jnp.log1p(jnp.exp(-jnp.abs(forget)))
        column = jnp.sum(jnp.where(diagonal, scale[h : h + 1, :], 0.0), axis=1, keepdims=True)
        carried = forget_log + column
        new_max = jnp.maximum(carried, in_pre)
        carries.append(jnp.exp(carried - new_max))
        fresh.append(jnp.exp(in_pre - new_max))
    keys = jnp.dot(normed, wk[...], preferred_element_type=f32)
    turned = [query[:, h * key_dim : (h + 1) * key_dim].T for h in range(heads)]
    for b in range(seqs):
        for h in range(heads):
            product = turned[h][:, b : b + 1] * mem[b, h]
            recall[h, b : b + 1, :] = jnp.sum(product, axis=0, keepdims=True)
    values = jnp.dot(normed, wv[...], preferred_element_type=f32)
    parts = []
    for h in range(heads):
        ks = slice(h * key_dim, (h + 1) * key_dim)
        vs = slice(h * value_dim, (h + 1) * value_dim)
        match = jnp.sum(query[:, ks] * keys[:, ks], axis=1, keepdims=True)
        read = carries[h] * recall[h] + (fresh[h] * match) * values[:, vs]
        inv = lax.rsqrt(jnp.mean(read * read, axis=1, keepdims=True) + EPS)
        parts.append((read * inv * hg[:, vs]).astype(bf16))
    headout = parts[0] if heads == 1 else jnp.concatenate(parts, axis=1)
    product = jnp.dot(headout, wo[...], preferred_element_type=f32)
    if halves:
        low, high = product[: seqs // 2], product[seqs // 2 :]
        odd = lax.axis_index("tp") % 2 == 1
        outs[0][...] = jnp.where(odd, high, low).astype(bf16)
        outs[1][...] = jnp.where(odd, low, high).astype(bf16)
    else:
        outs[0][...] = product.astype(bf16)


def cell(
    tokens,
    memory,
    log_scale,
    mix_gain_in,
    w_query,
    w_key,
    w_value,
    w_igate,
    w_fgate,
    igate_bias,
    fgate_bias,
    head_gain,
    w_output,
    halves,
):
    f32 = jnp.float32
    bf16 = jnp.bfloat16
    seqs, width = tokens.shape
    heads, key_dim, value_dim = memory.shape[1:]
    body = lambda *refs: cell_body(heads, key_dim, value_dim, halves, *refs)
    operands = [
        tokens,
        mix_gain_in.reshape(1, width),
        w_igate.T,
        w_fgate.T,
        biases(igate_bias, fgate_bias),
        log_scale.T,
        w_query,
        w_key,
        w_value,
        memory,
        head_gain.reshape(1, heads * value_dim),
        w_output,
    ]
    shape = jax.ShapeDtypeStruct((seqs // 2 if halves else seqs, w_output.shape[1]), bf16)
    result = pl.pallas_call(
        body,
        out_shape=[shape] * (2 if halves else 1),
        in_specs=[whole()] * len(operands),
        out_specs=[whole()] * (2 if halves else 1),
        scratch_shapes=[pltpu.VMEM((heads, seqs, value_dim), f32)],
        compiler_params=pltpu.CompilerParams(vmem_limit_bytes=12 << 20),
        name="cell",
    )(*operands)
    return result if halves else result[0]


def after_mix_body(parts, tokens, gain_out, gain_in, resid, spread):
    f32 = jnp.float32
    half = tokens.shape[0] // 2
    mixed = parts[0][...].astype(f32)
    for part in parts[1:]:
        mixed = mixed + part[...].astype(f32)
    odd = lax.axis_index("tp") % 2 == 1
    xf = tokens[...].astype(f32)
    xf = jnp.where(odd, xf[half:], xf[:half])
    kept = (xf + mixed * rms_scale(mixed) * gain_out[...]).astype(jnp.bfloat16)
    resid[...] = kept
    rf = kept.astype(f32)
    ffn_in = (rf * rms_scale(rf) * gain_in[...]).astype(jnp.bfloat16)
    for g in range(spread.shape[0]):
        spread[g] = ffn_in


def after_mix(parts, tokens, gain_out, gain_in, groups):
    seqs, width = tokens.shape
    count = len(parts)
    return pl.pallas_call(
        lambda *refs: after_mix_body(refs[:count], *refs[count:]),
        out_shape=(
            jax.ShapeDtypeStruct((seqs // 2, width), jnp.bfloat16),
            jax.ShapeDtypeStruct((groups, seqs // 2, width), jnp.bfloat16),
        ),
        in_specs=[whole()] * (count + 3),
        out_specs=(whole(), whole()),
        compiler_params=pltpu.CompilerParams(vmem_limit_bytes=8 << 20),
        name="after_mix",
    )(*parts, tokens, gain_out.reshape(1, width), gain_in.reshape(1, width))


def expert_body(rows, gate_w, up_w, down_w, gate_n, up_n, down_n, out):
    f32 = jnp.float32
    groups, half, width = rows.shape
    ffn_in = rows[...].reshape(groups * half, width)
    pairs = []
    for gates, ups in ((gate_w, up_w), (gate_n, up_n)):
        gate = jnp.dot(ffn_in, gates[...], preferred_element_type=f32)
        pairs.append((gate, jnp.dot(ffn_in, ups[...], preferred_element_type=f32)))
    acts = [(gate * jax.nn.sigmoid(gate) * up).astype(jnp.bfloat16) for gate, up in pairs]
    total = jnp.dot(acts[0], down_w[...], preferred_element_type=f32)
    total = total + jnp.dot(acts[1], down_n[...], preferred_element_type=f32)
    out[...] = total.astype(jnp.bfloat16).reshape(groups, half, width)


def expert(rows, own, neighbour):
    return pl.pallas_call(
        expert_body,
        out_shape=jax.ShapeDtypeStruct(rows.shape, jnp.bfloat16),
        in_specs=[whole()] * 7,
        out_specs=whole(),
        compiler_params=pltpu.CompilerParams(vmem_limit_bytes=16 << 20),
        name="expert",
    )(rows, *own, *neighbour)


def share_body(back, weights, resid, share, both):
    f32 = jnp.float32
    groups, half, _ = back.shape
    odd = lax.axis_index("tp") % 2 == 1
    turned = weights[...].T
    mine = jnp.where(odd, turned[half:], turned[:half])
    total = mine[:, 0:1] * back[0].astype(f32)
    for e in range(1, groups):
        total = total + mine[:, e : e + 1] * back[e].astype(f32)
    rounded = total.astype(jnp.bfloat16)
    share[...] = rounded
    both[0] = rounded
    both[1] = resid[...]


def combine(back, weights, resid):
    _, half, width = back.shape
    return pl.pallas_call(
        share_body,
        out_shape=(
            jax.ShapeDtypeStruct((half, width), jnp.bfloat16),
            jax.ShapeDtypeStruct((2, half, width), jnp.bfloat16),
        ),
        in_specs=[whole()] * 3,
        out_specs=(whole(), whole()),
        compiler_params=pltpu.CompilerParams(vmem_limit_bytes=8 << 20),
        name="share",
    )(back, weights, resid)


def last_body(count, *refs):
    f32 = jnp.float32
    sames, others = refs[:count], refs[count : 2 * count - 1]
    both, resid, gain, out, picks = refs[2 * count - 1 :]
    quarter = out.shape[1]
    kept = sames[0][...].astype(f32)
    for part in sames[1:]:
        kept = kept + part[...].astype(f32)
    other = both[0].astype(f32)
    for part in others:
        other = other + part[...].astype(f32)
    picks[0] = kept * rms_scale(kept)
    picks[1] = other * rms_scale(other)
    picks[2] = resid[...].astype(f32)
    picks[3] = both[1].astype(f32)
    lane = lax.axis_index("tp")
    odd = lane % 2 == 1
    places = pl.ds(pl.multiple_of(lane * quarter, quarter), quarter)
    mine = picks[2, :, places] + picks[0, :, places] * gain[...]
    theirs = picks[3, :, places] + picks[1, :, places] * gain[...]
    low, high = jnp.where(odd, theirs, mine), jnp.where(odd, mine, theirs)
    out[...] = jnp.concatenate([low, high], axis=0).astype(jnp.bfloat16)


def last(same, both, other, resid, gain):
    half, width = resid.shape
    quarter = gain.shape[0]
    operands = [*same, *other, both, resid, gain.reshape(1, quarter)]
    return pl.pallas_call(
        lambda *refs: last_body(len(same), *refs),
        out_shape=jax.ShapeDtypeStruct((2 * half, quarter), jnp.bfloat16),
        in_specs=[whole()] * len(operands),
        out_specs=whole(),
        scratch_shapes=[pltpu.VMEM((4, half, width), jnp.float32)],
        compiler_params=pltpu.CompilerParams(vmem_limit_bytes=8 << 20),
        name="last",
    )(*operands)


def odds_first(lanes):
    return [*range(3, lanes, 2), *range(2, lanes, 2), 1]


def every_token(
    halves,
    tokens,
    mix_gain_out,
    ffn_gain_in,
    routes,
    route_weights,
    expert_gate,
    expert_up,
    expert_down,
    ffn_gain_out,
):
    groups = lax.axis_size("ep")
    lanes = lax.axis_size("tp")
    mine, theirs = halves
    parts = [mine]
    for step in odds_first(lanes):
        parts.append(exchange(theirs if step % 2 else mine, "tp", step))
    shards = (expert_gate[0], expert_up[0], expert_down[0])
    *waited, _ = lax.optimization_barrier((*shards, mine))
    neighbour = [exchange(shard, "tp", 1) for shard in waited]
    resid, spread = after_mix(parts, tokens, mix_gain_out, ffn_gain_in, groups)
    named = routes[:, :, None] == jnp.arange(groups, dtype=jnp.int32)[None, None, :]
    weights = jnp.sum(jnp.where(named, route_weights[:, :, None], 0.0), axis=1).T
    spread, weights, gain_out = lax.optimization_barrier((spread, weights, ffn_gain_out))
    rows = lax.all_to_all(spread, "ep", split_axis=0, concat_axis=0, tiled=True)
    blocks = expert(rows, shards, neighbour)
    blocks, weights, resid, gain_out = lax.optimization_barrier((blocks, weights, resid, gain_out))
    back = lax.all_to_all(blocks, "ep", split_axis=0, concat_axis=0, tiled=True)
    share, both = combine(back, weights, resid)
    sums = {}
    for step in odds_first(lanes):
        sums[step] = exchange(both if step == 1 else share, "tp", step)
    same = [share] + [sums[step] for step in range(2, lanes, 2)]
    other = [sums[step] for step in range(3, lanes, 2)]
    return last(same, sums[1], other, resid, gain_out)


def slotted(ffn_in, routes, route_weights, expert_gate, expert_up, expert_down, cap):
    f32 = jnp.float32
    bf16 = jnp.bfloat16
    seqs, width = ffn_in.shape
    top = routes.shape[1]
    local_experts = expert_gate.shape[0]
    experts_all = local_experts * lax.axis_size("ep")
    flat = routes.reshape(-1)
    hits = (flat[:, None] == jnp.arange(experts_all, dtype=jnp.int32)[None, :]).astype(jnp.int32)
    earlier = jnp.cumsum(hits, axis=0) - hits
    slot = jnp.sum(earlier * hits, axis=1)
    place = (flat * cap + slot).reshape(seqs, top)
    picker = jnp.any(
        jnp.arange(experts_all * cap, dtype=jnp.int32)[:, None, None] == place[None, :, :], axis=2
    ).astype(bf16)
    outbound = (
        jnp.dot(picker, ffn_in, preferred_element_type=f32)
        .astype(bf16)
        .reshape(experts_all, cap, width)
    )
    arrived = lax.all_to_all(outbound, "ep", split_axis=0, concat_axis=0, tiled=True)
    items = arrived.shape[1]
    rows = arrived.reshape(-1, local_experts, items, width)
    gate = jnp.einsum("secd,edf->secf", rows, expert_gate, preferred_element_type=f32)
    up = jnp.einsum("secd,edf->secf", rows, expert_up, preferred_element_type=f32)
    act = (jax.nn.silu(gate) * up).astype(bf16)
    part = jnp.einsum("secf,efd->secd", act, expert_down, preferred_element_type=f32).reshape(
        -1, items, width
    )
    summed = lax.psum_scatter(
        part.astype(jnp.bfloat16), "tp", scatter_dimension=2, tiled=True
    ).astype(jnp.float32)
    done = summed.astype(bf16)
    returned = lax.all_to_all(done, "ep", split_axis=0, concat_axis=0, tiled=True)
    columns = returned.shape[2]
    chosen = jnp.take(returned.reshape(-1, columns), place.reshape(-1), axis=0).reshape(
        seqs, top, columns
    )
    return jnp.sum(route_weights[:, :, None] * chosen.astype(f32), axis=1)


def solution(mesh):
    return jax.shard_map(
        per_device,
        mesh=mesh,
        in_specs=(
            P("ep", None),
            P("ep", "tp", None, None),
            P("ep", "tp"),
            P(),
            P(None, "tp"),
            P(None, "tp"),
            P(None, "tp"),
            P(None, "tp"),
            P(None, "tp"),
            P("tp"),
            P("tp"),
            P("tp"),
            P("tp", None),
            P(),
            P(),
            P("ep", None),
            P("ep", None),
            P("ep", None, "tp"),
            P("ep", None, "tp"),
            P("ep", "tp", None),
            P("tp"),
        ),
        out_specs=P("ep", "tp"),
        check_vma=False,
    )
```
